32 devices in a mesh: sp: 4 (over y, x), tp: 8 (over z, core).
Axes of the slice: x: 2, y: 2, z: 4, core: 2. Of those that a mesh axis runs over, the one named last changes fastest.
Arguments:
- tokens: bfloat16 [2, 512, 4096], P(None, 'sp', 'tp'), may hold values from -6 to 6
- key_matrix: bfloat16 [4096, 4096], P(None, 'tp'), may hold values from -0.09375 to 0.09375
- value_matrix: bfloat16 [4096, 4096], P(None, 'tp'), may hold values from -0.375 to 0.375
- gate_matrix: bfloat16 [4096, 64], replicated, may hold values from -0.09375 to 0.09375
- head_decay_rate: float32 [32], P('tp'), may hold values from 0 to 1, as said below
- extra_log_decay: float32 [2, 32, 512], P(None, 'tp', 'sp'), may hold values from -3 to 0, as said below
- next_token_query: bfloat16 [2, 4096], P(None, 'tp'), may hold values from -6 to 6
- next_token_key: bfloat16 [2, 4096], P(None, 'tp'), may hold values from -6 to 6
- next_token_value: bfloat16 [2, 32, 128], P(None, 'tp', 'sp'), may hold values from -6 to 6
- next_write_strength: float32 [2, 32], P(None, 'tp'), may hold values from 0.05 to 1
- read_norm_gain: float32 [128], P('sp'), may hold values from 0.1 to 1.9
Outputs:
- state_cache: bfloat16 [2, 32, 128, 128], P(None, 'tp', None, 'sp')
- first_read: bfloat16 [2, 32, 128], P(None, 'tp', 'sp')
The draws below stay inside these ranges and needn't reach their ends.
Inputs may be any that keep to these rules, and one draw needn't show every extreme that they name: `head_decay_rate`: positive. `extra_log_decay`: never positive.
All inputs are finite; a program needn't handle non-finite values.
Results may differ from the reference program's by a relative error of at most 0.013.
Values may be sent and summed in bfloat16 or wider, within the bound.
A program may use at most 64 MiB of HBM per device.

```python
import jax
import jax.numpy as jnp
from jax import lax

D = 4096
HEAD_COUNT = 32
DK = 128
DV = 128
PROMPT_COUNT = 2
POS_DEV = 128
BLOCK = 64
PROMPT_LENGTH = 512


def draw_head_decay_rate(key, part):
    chooser, fast_key, slow_key = jax.random.split(jax.random.fold_in(key, 11), 3)
    fast_share = 0.5
    fast_mask = jax.random.uniform(chooser, (HEAD_COUNT,), jnp.float32) < fast_share
    fast_rate = jnp.exp(jax.random.uniform(fast_key, (HEAD_COUNT,), jnp.float32, jnp.log(0.02), jnp.log(0.05)))
    slow_rate = jnp.exp(jax.random.uniform(slow_key, (HEAD_COUNT,), jnp.float32, jnp.log(0.05 / PROMPT_LENGTH), jnp.log(0.4 / PROMPT_LENGTH)))
    return jnp.where(fast_mask, fast_rate, slow_rate).astype(jnp.float32)


def draw_extra_log_decay(key, part):
    block_key, location_seed, magnitude_seed = jax.random.split(jax.random.fold_in(key, 23), 3)
    lowest_rate = 0.05
    highest_rate = 0.6
    block_total = PROMPT_LENGTH // POS_DEV
    block_rate = jnp.exp(jax.random.uniform(block_key, (PROMPT_COUNT, HEAD_COUNT, block_total), jnp.float32, jnp.log(lowest_rate / PROMPT_LENGTH), jnp.log(highest_rate / PROMPT_LENGTH)))
    position_decay = jnp.repeat(block_rate, POS_DEV, axis=2)
    spike_positions = jax.random.randint(location_seed, (PROMPT_COUNT, HEAD_COUNT, 2), 0, PROMPT_LENGTH)
    spike_magnitude = jnp.log(jax.random.uniform(magnitude_seed, (PROMPT_COUNT, HEAD_COUNT, 2), jnp.float32, 0.5, 0.8))
    spike_locations = jnp.arange(PROMPT_LENGTH, dtype=jnp.int32)
    decay_spikes = jnp.sum(jnp.where(spike_locations[None, None, None, :] == spike_positions[..., None], spike_magnitude[..., None], 0.0), axis=2)
    return (decay_spikes - position_decay).astype(jnp.float32)


def level_of(own_key, dims, shards, smallest, top_value):
    gain, own = 1.0, jax.random.fold_in(own_key, 6)
    for position, parts in shards:
        heights = jnp.exp(jax.random.uniform(jax.random.fold_in(own, position), (parts,), jnp.float32, smallest / len(shards), top_value / len(shards)))
        gain = gain * jnp.repeat(heights, dims[position] // parts).reshape([-1 if axis == position else 1 for axis in range(len(dims))])
    return gain


def bell_draw(own_key, shape, width, most, cuts=(), held_as=jnp.bfloat16):
    values = width * jax.random.normal(own_key, shape, jnp.float32)
    if cuts:
        values = values * level_of(own_key, shape, cuts, -0.22, 0.18)
    return jnp.clip(values, -most, most).astype(held_as)


def setup_inputs(seed: int = 0) -> dict:
    splits = jax.random.split(jax.random.key(seed), 12)
    return {
        "tokens": bell_draw(splits[0], (PROMPT_COUNT, PROMPT_LENGTH, D), 1.0, 6.0, ((1, 4), (2, 8))),
        "key_matrix": bell_draw(splits[1], (D, HEAD_COUNT * DK), D ** -0.5, 0.09375, ((1, 8),)),
        "value_matrix": bell_draw(splits[2], (D, HEAD_COUNT * DV), (D // 16) ** -0.5, 0.375, ((1, 8),)),
        "gate_matrix": bell_draw(splits[3], (D, 2 * HEAD_COUNT), D ** -0.5, 0.09375),
        "head_decay_rate": draw_head_decay_rate(jax.random.fold_in(splits[11], 71), 0),
        "extra_log_decay": draw_extra_log_decay(jax.random.fold_in(splits[11], 71), 0),
        "next_token_query": bell_draw(splits[6], (PROMPT_COUNT, HEAD_COUNT * DK), 1.0, 6.0, ((1, 8),)),
        "next_token_key": bell_draw(splits[7], (PROMPT_COUNT, HEAD_COUNT * DK), 1.0, 6.0, ((1, 8),)),
        "next_token_value": bell_draw(splits[8], (PROMPT_COUNT, HEAD_COUNT, DV), 1.0, 6.0, ((1, 8), (2, 4))),
        "next_write_strength": jnp.clip(0.05 + 0.95 * jax.random.uniform(splits[9], (PROMPT_COUNT, HEAD_COUNT), jnp.float32) ** level_of(splits[9], (PROMPT_COUNT, HEAD_COUNT), ((1, 8),), -0.2, 0.2), 0.05, 1.0),
        "read_norm_gain": jnp.clip(1.0 + 0.18 * jax.random.normal(splits[10], (DV,), jnp.float32), 0.1, 1.9),
    }


exact_mode = lax.Precision.HIGHEST
strength_offset = 5.0

def unit_rows(matrix):
    return matrix * lax.rsqrt(lax.optimization_barrier(jnp.sum(matrix * matrix, axis=-1, keepdims=True)) + 1e-06)

def nilpotent_inverse(mixing):
    extent = mixing.shape[-1]
    result = jnp.zeros_like(mixing) + jnp.eye(extent, dtype=jnp.float32)
    powered = -mixing
    covered = 1
    while covered < extent:
        result = result + jnp.einsum('...ij,...jk->...ik', result, powered, precision=exact_mode)
        powered = jnp.einsum('...ij,...jk->...ik', powered, powered, precision=exact_mode)
        covered = covered * 2
    return result

def block_terms(unit_keys, values, decay_logarithm, strength):
    extent = unit_keys.shape[-2]
    lower = jnp.tril(jnp.ones((extent, extent), jnp.bool_))
    strict = jnp.tril(jnp.ones((extent, extent), jnp.bool_), -1)
    running = jnp.cumsum(decay_logarithm, axis=-1)
    spread = running[..., :, None] - running[..., None, :]
    within = jnp.where(lower, jnp.exp(jnp.where(lower, spread, 0.0)), 0.0)
    scaled = unit_keys * strength[..., None]
    mixing = jnp.where(strict, jnp.einsum('...id,...jd->...ij', scaled, unit_keys, precision=exact_mode) * within, 0.0)
    inverse = nilpotent_inverse(mixing)
    writes = jnp.einsum('...ij,...je->...ie', inverse, values * strength[..., None], precision=exact_mode)
    erases = jnp.einsum('...ij,...jd->...id', inverse, scaled * jnp.exp(running)[..., None], precision=exact_mode)
    final_log = running[..., -1]
    carried = unit_keys * jnp.exp(final_log[..., None] - running)[..., None]
    return (writes, erases, carried, final_log)

def split_blocks(array, block_count):
    shaped = array.reshape(array.shape[:2] + (block_count, array.shape[2] // block_count) + array.shape[3:])
    return jnp.moveaxis(shaped, 2, 0)

def reference(tokens, key_matrix, value_matrix, gate_matrix, head_decay_rate, extra_log_decay, next_token_query, next_token_key, next_token_value, next_write_strength, read_norm_gain):
    key_proj = jnp.dot(tokens, key_matrix, preferred_element_type=jnp.float32).astype(jnp.bfloat16)
    value_proj = jnp.dot(tokens, value_matrix, preferred_element_type=jnp.float32).astype(jnp.bfloat16)
    gate_pre = jnp.dot(tokens, gate_matrix, preferred_element_type=jnp.float32)
    key_float = lax.optimization_barrier(key_proj).astype(jnp.float32)
    value_float = lax.optimization_barrier(value_proj).astype(jnp.float32)
    unit_keys = unit_rows(key_float.reshape(PROMPT_COUNT, PROMPT_LENGTH, HEAD_COUNT, DK).transpose(0, 2, 1, 3))
    values = value_float.reshape(PROMPT_COUNT, PROMPT_LENGTH, HEAD_COUNT, DV).transpose(0, 2, 1, 3)
    gate_projected = gate_pre.transpose(0, 2, 1)
    decay_logarithm = -head_decay_rate[None, :, None] * jax.nn.softplus(gate_projected[:, :HEAD_COUNT]) + extra_log_decay
    strength = jax.nn.sigmoid(gate_projected[:, HEAD_COUNT:] - strength_offset)
    block_count = PROMPT_LENGTH // BLOCK
    block_parts = block_terms(split_blocks(unit_keys, block_count), split_blocks(values, block_count), split_blocks(decay_logarithm, block_count), split_blocks(strength, block_count))

    def advance(current, block_part):
        writes, erases, carried, final_log = block_part
        fresh = writes - jnp.einsum('shcd,shde->shce', erases, current, precision=exact_mode)
        current = current * jnp.exp(final_log)[..., None, None] + jnp.einsum('shcd,shce->shde', carried, fresh, precision=exact_mode)
        return (current, None)
    start_state = jnp.zeros((PROMPT_COUNT, HEAD_COUNT, DK, DV), jnp.float32)
    state, _ = lax.scan(advance, start_state, block_parts)
    query_rows = next_token_query.astype(jnp.float32).reshape(PROMPT_COUNT, HEAD_COUNT, DK)
    unit_new = unit_rows(next_token_key.astype(jnp.float32).reshape(PROMPT_COUNT, HEAD_COUNT, DK))
    value_rows = next_token_value.astype(jnp.float32)
    key_read = jnp.einsum('shd,shde->she', unit_new, state, precision=exact_mode)
    query_read = jnp.einsum('shd,shde->she', query_rows, state, precision=exact_mode)
    intersection = lax.optimization_barrier(jnp.sum(query_rows * unit_new, axis=-1))
    read_raw = query_read + (next_write_strength * intersection)[..., None] * (value_rows - key_read)
    first_read = read_raw * lax.rsqrt(lax.optimization_barrier(jnp.mean(read_raw * read_raw, axis=-1, keepdims=True)) + 1e-06) * read_norm_gain
    return (state.astype(jnp.bfloat16), first_read.astype(jnp.bfloat16))
```

```python
import functools

import jax
import jax.numpy as jnp
from jax import lax
from jax.experimental import pallas as pl
from jax.experimental.pallas import tpu as pltpu
from jax.sharding import PartitionSpec as P

DV = 128
CORES = 2
MESH = pl.DeviceIdType.MESH


exact_mode = lax.Precision.HIGHEST
strength_offset = 5.0


def unit_rows(matrix):
    return matrix * lax.rsqrt(jnp.sum(matrix * matrix, axis=-1, keepdims=True) + 1e-06)


def nilpotent_inverse(mixing):
    extent = mixing.shape[-1]
    result = jnp.zeros_like(mixing) + jnp.eye(extent, dtype=jnp.float32)
    powered = -mixing
    covered = 1
    while covered < extent:
        product = lax.optimization_barrier(
            jnp.einsum("...ij,...jk->...ik", result, powered, precision=exact_mode)
        )
        result = result + product
        powered = jnp.einsum("...ij,...jk->...ik", powered, powered, precision=exact_mode)
        covered = covered * 2
    return result


def block_terms(unit_keys, values, decay_logarithm, strength):
    extent = unit_keys.shape[-2]
    lower = jnp.tril(jnp.ones((extent, extent), jnp.bool_))
    strict = jnp.tril(jnp.ones((extent, extent), jnp.bool_), -1)
    running = jnp.cumsum(decay_logarithm, axis=-1)
    spread = running[..., :, None] - running[..., None, :]
    within = jnp.where(lower, jnp.exp(jnp.where(lower, spread, 0.0)), 0.0)
    scaled = unit_keys * strength[..., None]
    mixing = jnp.where(
        strict,
        jnp.einsum("...id,...jd->...ij", scaled, unit_keys, precision=exact_mode) * within,
        0.0,
    )
    inverse = nilpotent_inverse(mixing)
    writes = jnp.einsum(
        "...ij,...je->...ie", inverse, values * strength[..., None], precision=exact_mode
    )
    erases = jnp.einsum(
        "...ij,...jd->...id", inverse, scaled * jnp.exp(running)[..., None], precision=exact_mode
    )
    final_log = running[..., -1]
    carried = unit_keys * jnp.exp(final_log[..., None] - running)[..., None]
    return (writes, erases, carried, final_log)


def split_blocks(array, block_count):
    shaped = array.reshape(
        array.shape[:2] + (block_count, array.shape[2] // block_count) + array.shape[3:]
    )
    return jnp.moveaxis(shaped, 2, 0)


def local_general(
    tokens,
    key_matrix,
    value_matrix,
    gate_matrix,
    head_decay_rate,
    extra_log_decay,
    next_token_query,
    next_token_key,
    next_token_value,
    next_write_strength,
    read_norm_gain,
):
    sequences, positions, _ = tokens.shape
    local_heads = head_decay_rate.shape[0]
    key_width = key_matrix.shape[1] // local_heads
    value_width = value_matrix.shape[1] // local_heads
    all_heads = gate_matrix.shape[1] // 2
    group_size = lax.axis_size("sp")
    column_share = value_width // group_size
    first_head = lax.axis_index("tp") * local_heads
    decay_cols = lax.dynamic_slice_in_dim(gate_matrix, first_head, local_heads, 1)
    strength_cols = lax.dynamic_slice_in_dim(gate_matrix, all_heads + first_head, local_heads, 1)
    gate_cols = jnp.concatenate([decay_cols, strength_cols], axis=1)
    row_count = sequences * positions
    incoming = lax.all_gather(tokens, "tp", axis=2, tiled=True)
    span_width = incoming.shape[2]
    flat_rows = incoming.reshape(row_count, span_width)
    products = lax.optimization_barrier(
        (
            jnp.dot(flat_rows, key_matrix, preferred_element_type=jnp.float32),
            jnp.dot(flat_rows, value_matrix, preferred_element_type=jnp.float32),
            jnp.dot(flat_rows, gate_cols, preferred_element_type=jnp.float32),
        )
    )
    key_sum = products[0]
    value_sum = products[1]
    gate_pre = products[2]
    key_float = lax.optimization_barrier(key_sum.astype(jnp.bfloat16)).astype(jnp.float32)
    value_float = lax.optimization_barrier(value_sum.astype(jnp.bfloat16)).astype(jnp.float32)
    unit_keys = unit_rows(
        key_float.reshape(sequences, positions, local_heads, key_width).transpose(0, 2, 1, 3)
    )
    values = value_float.reshape(sequences, positions, local_heads, value_width).transpose(
        0, 2, 1, 3
    )
    gate_projected = gate_pre.reshape(sequences, positions, 2 * local_heads).transpose(0, 2, 1)
    decay_logarithm = (
        -head_decay_rate[None, :, None] * jax.nn.softplus(gate_projected[:, :local_heads])
        + extra_log_decay
    )
    strength = jax.nn.sigmoid(gate_projected[:, local_heads:] - strength_offset)
    block_count = positions // min(64, positions)
    block_parts = block_terms(
        split_blocks(unit_keys, block_count),
        split_blocks(values, block_count),
        split_blocks(decay_logarithm, block_count),
        split_blocks(strength, block_count),
    )
    identity = jnp.zeros((sequences, local_heads, key_width, key_width), jnp.float32) + jnp.eye(
        key_width, dtype=jnp.float32
    )
    start_map = jnp.concatenate(
        [identity, jnp.zeros((sequences, local_heads, key_width, value_width), jnp.float32)],
        axis=-1,
    )

    def advance(current, block_part):
        writes, erases, carried, final_log = block_part
        padded = jnp.concatenate(
            [jnp.zeros(writes.shape[:-1] + (key_width,), jnp.float32), writes], axis=-1
        )
        removed = lax.optimization_barrier(
            jnp.einsum("shcd,shde->shce", erases, current, precision=exact_mode)
        )
        fresh = padded - removed
        added = lax.optimization_barrier(
            jnp.einsum("shcd,shce->shde", carried, fresh, precision=exact_mode)
        )
        current = current * jnp.exp(final_log)[..., None, None] + added
        return (current, None)

    local_map, _ = lax.scan(advance, start_map, block_parts)
    carry_map = local_map[..., :key_width]
    write_map = local_map[..., key_width:]
    carry_copies = jnp.broadcast_to(carry_map[None], (group_size,) + carry_map.shape)
    write_parts = jnp.moveaxis(
        write_map.reshape(sequences, local_heads, key_width, group_size, column_share), 3, 0
    )
    carries = lax.all_to_all(carry_copies, "sp", split_axis=0, concat_axis=0, tiled=True)
    write_cols = lax.all_to_all(write_parts, "sp", split_axis=0, concat_axis=0, tiled=True)

    def fold_step(current, block_map):
        moved = lax.optimization_barrier(
            jnp.einsum("shij,shje->shie", block_map[0], current, precision=exact_mode)
        )
        return (moved + block_map[1], None)

    begin_state = jnp.zeros(write_cols.shape[1:], jnp.float32)
    folded, _ = lax.scan(fold_step, begin_state, (carries, write_cols))
    query_rows = next_token_query.astype(jnp.float32).reshape(sequences, local_heads, key_width)
    unit_new = unit_rows(
        next_token_key.astype(jnp.float32).reshape(sequences, local_heads, key_width)
    )
    value_rows = next_token_value.astype(jnp.float32)
    key_read = jnp.einsum("shd,shde->she", unit_new, folded, precision=exact_mode)
    query_read = jnp.einsum("shd,shde->she", query_rows, folded, precision=exact_mode)
    intersection = jnp.sum(query_rows * unit_new, axis=-1)
    read_raw = query_read + (next_write_strength * intersection)[..., None] * (
        value_rows - key_read
    )
    square_total = lax.psum(jnp.sum(read_raw * read_raw, axis=-1, keepdims=True), "sp")
    first_read = read_raw * lax.rsqrt(square_total / DV + 1e-06) * read_norm_gain
    return (folded.astype(jnp.bfloat16), first_read.astype(jnp.bfloat16))


def exact_dot(left, right, contract=((1,), (0,))):
    return lax.dot_general(
        left, right, (contract, ((), ())), precision=exact_mode, preferred_element_type=jnp.float32
    )


def short_dot(left, right, contract=((1,), (0,))):
    return lax.dot_general(
        left.astype(jnp.bfloat16),
        right.astype(jnp.bfloat16),
        (contract, ((), ())),
        preferred_element_type=jnp.float32,
    )


def softplus(x):
    return jnp.maximum(x, 0.0) + jnp.log1p(jnp.exp(-jnp.abs(x)))


def grid_mask(rows, cols, rule):
    row = lax.broadcasted_iota(jnp.int32, (rows, cols), 0)
    col = lax.broadcasted_iota(jnp.int32, (rows, cols), 1)
    return rule(row, col)


def fused_kernel(
    sp_size,
    tp_size,
    rate_ref,
    next_strength_ref,
    tokens_ref,
    key_ref,
    value_ref,
    gate_hbm,
    extra_hbm,
    query_hbm,
    new_key_hbm,
    new_value_hbm,
    gain_hbm,
    state_ref,
    read_ref,
    gathered,
    key_w,
    value_w,
    gate_ref,
    extra_ref,
    query_ref,
    new_key_ref,
    new_value_ref,
    gain_ref,
    key_acc,
    value_acc,
    gate_acc,
    kv_out,
    kv_in,
    side_out,
    side_in,
    state_out,
    state_in,
    row_out,
    row_in,
    load_sem,
    weight_sem,
    gather_recv,
    gather_send,
    swap_recv,
    swap_send,
    swap_local,
    last_recv,
    last_send,
    last_local,
):
    sequences, positions, depth = tokens_ref.shape
    local_heads = extra_ref.shape[1]
    key_width = key_acc.shape[1] // local_heads
    value_width = value_acc.shape[1] // local_heads
    share = value_width // sp_size
    all_heads = gate_ref.shape[0] // 2
    chips = tp_size // CORES
    me = lax.axis_index("sp")
    spot = lax.axis_index("tp")
    chip = spot // CORES
    core = spot % CORES
    partner = chip * CORES + (1 - core)

    loads = [
        pltpu.make_async_copy(tokens_ref.at[s], gathered.at[spot, s], load_sem.at[s])
        for s in range(sequences)
    ]
    for load in loads:
        load.start()

    barrier = pltpu.get_barrier_semaphore()
    pl.semaphore_signal(barrier, inc=1, device_id={"tp": partner}, device_id_type=MESH)

    @pl.when(chip > 0)
    def _():
        pl.semaphore_signal(barrier, inc=1, device_id={"tp": spot - CORES}, device_id_type=MESH)

    @pl.when(chip < chips - 1)
    def _():
        pl.semaphore_signal(barrier, inc=1, device_id={"tp": spot + CORES}, device_id_type=MESH)

    for offset in range(1, sp_size):
        pl.semaphore_signal(
            barrier, inc=1, device_id={"sp": (me + offset) % sp_size}, device_id_type=MESH
        )
    weights = [
        pltpu.make_async_copy(key_ref, key_w, weight_sem.at[0]),
        pltpu.make_async_copy(value_ref, value_w, weight_sem.at[1]),
        pltpu.make_async_copy(gate_hbm, gate_ref, weight_sem.at[2]),
        pltpu.make_async_copy(extra_hbm, extra_ref, weight_sem.at[3]),
        pltpu.make_async_copy(query_hbm, query_ref, weight_sem.at[4]),
        pltpu.make_async_copy(new_key_hbm, new_key_ref, weight_sem.at[5]),
        pltpu.make_async_copy(new_value_hbm, new_value_ref, weight_sem.at[6]),
        pltpu.make_async_copy(gain_hbm, gain_ref, weight_sem.at[7]),
    ]
    for weight in weights:
        weight.start()
    key_acc[...] = jnp.zeros_like(key_acc)
    value_acc[...] = jnp.zeros_like(value_acc)
    gate_acc[...] = jnp.zeros_like(gate_acc)
    side_out[...] = jnp.zeros_like(side_out)
    row_out[...] = jnp.zeros_like(row_out)
    for load in loads:
        load.wait()
    near = jnp.where(chip > 0, 1, 0) + jnp.where(chip < chips - 1, 1, 0)
    pl.semaphore_wait(barrier, near + sp_size)

    def piece(origin, s, way, target):
        return pltpu.make_async_remote_copy(
            src_ref=gathered.at[origin, s],
            dst_ref=gathered.at[origin, s],
            send_sem=gather_send.at[origin, s, way],
            recv_sem=gather_recv.at[origin, s],
            device_id={"tp": target},
            device_id_type=MESH,
        )

    def take(block, s):
        rows = gathered[block, s]
        cut = slice(s * positions, (s + 1) * positions)
        span = pl.ds(pl.multiple_of(block * depth, depth), depth)
        key_acc[cut] += jnp.dot(rows, key_w[span, :], preferred_element_type=jnp.float32)
        value_acc[cut] += jnp.dot(rows, value_w[span, :], preferred_element_type=jnp.float32)
        gate_acc[cut] += lax.dot_general(
            rows,
            gate_ref[:, span],
            (((1,), (1,)), ((), ())),
            preferred_element_type=jnp.float32,
        )

    first = spot * local_heads
    chooser = grid_mask(
        2 * local_heads,
        2 * all_heads,
        lambda r, c: c == jnp.where(r < local_heads, first + r, all_heads + first + r - local_heads),
    ).astype(jnp.float32)
    placer = grid_mask(share, value_width, lambda r, c: c == me * share + r).astype(jnp.float32)

    def swap(s, target, origin):
        return [
            pltpu.make_async_remote_copy(
                src_ref=source.at[target, s],
                dst_ref=sink.at[origin, s],
                send_sem=swap_send.at[n, s, target],
                recv_sem=swap_recv.at[n, s, origin],
                device_id={"sp": target},
                device_id_type=MESH,
            )
            for n, (source, sink) in enumerate(((side_out, side_in), (kv_out, kv_in)))
        ]

    def kept(s):
        return [
            pltpu.make_async_copy(kv_out.at[me, s], kv_in.at[me, s], swap_local.at[0, s]),
            pltpu.make_async_copy(side_out.at[me, s], side_in.at[me, s], swap_local.at[1, s]),
        ]

    def hand_out(s):
        cut = slice(s * positions, (s + 1) * positions)
        gates = exact_dot(chooser, gate_acc[cut], ((1,), (1,)))
        new_value = exact_dot(new_value_ref[s].astype(jnp.float32), placer)
        extra = extra_ref[s]
        for h in range(local_heads):
            kv_out[h, s, 0] = key_acc[cut, h * key_width : (h + 1) * key_width].astype(jnp.bfloat16)
            kv_out[h, s, 1] = value_acc[cut, h * value_width : (h + 1) * value_width].astype(
                jnp.bfloat16
            )
            side_out[h, s, 0:1, :] = (
                -rate_ref[h] * softplus(gates[h : h + 1]) + extra[h : h + 1, :]
            )
            side_out[h, s, 1:2, :] = jax.nn.sigmoid(
                gates[local_heads + h : local_heads + h + 1] - strength_offset
            )
            side_out[h, s, 2:3, :] = new_value[h : h + 1, :]
        for n in range(2):
            for offset in range(1, sp_size):
                swap(s, (me + offset) % sp_size, me)[n].start()
        for copy in kept(s):
            copy.start()

    for s in range(sequences):

        @pl.when(chip < chips - 1)
        def _(s=s):
            piece(spot, s, 0, spot + CORES).start()

        @pl.when(chip > 0)
        def _(s=s):
            piece(spot, s, 1, spot - CORES).start()

        piece(spot, s, 2, partner).start()
    for weight in weights:
        weight.wait()
    for s in range(sequences):
        take(spot, s)
        piece(partner, s, 2, partner).wait_recv()
        take(partner, s)

    for distance in range(1, chips):
        for s in range(sequences):
            for way, step in ((0, -1), (1, 1)):
                origin_chip = chip + step * distance
                origin = origin_chip * CORES + core
                present = (origin_chip >= 0) & (origin_chip < chips)
                onward = chip - step

                @pl.when(present)
                def _(s=s, way=way, origin=origin, onward=onward):
                    piece(origin, s, way, partner).wait_recv()

                    @pl.when((onward >= 0) & (onward < chips))
                    def _():
                        piece(origin, s, way, onward * CORES + core).start()

                    piece(origin, s, 2, partner).start()

            def absorb(index, carry, distance=distance, s=s):
                side = index // CORES
                which = index % CORES
                origin_chip = chip + (2 * side - 1) * distance
                present = (origin_chip >= 0) & (origin_chip < chips)

                @pl.when(present & (which == 0))
                def _():
                    take(origin_chip * CORES + core, s)

                @pl.when(present & (which == 1))
                def _():
                    block = origin_chip * CORES + 1 - core
                    piece(block, s, 2, partner).wait_recv()
                    take(block, s)

                return carry

            lax.fori_loop(0, 2 * CORES, absorb, 0)
            if distance == chips - 1:
                hand_out(s)

    side_rows = side_in.shape[2]
    upto = grid_mask(positions, positions, lambda r, c: r <= c).astype(jnp.float32)
    eye = grid_mask(positions, positions, lambda r, c: r == c).astype(jnp.float32)
    lower = grid_mask(positions, positions, lambda r, c: r >= c)
    strict = grid_mask(positions, positions, lambda r, c: r > c)
    lanes = pl.ds(pl.multiple_of(me * key_width, key_width), key_width)
    queries = query_ref[:, lanes].astype(jnp.float32)
    new_keys = new_key_ref[:, lanes].astype(jnp.float32)
    new_keys = new_keys * lax.rsqrt(jnp.sum(new_keys * new_keys, axis=-1, keepdims=True) + 1e-06)
    meets = jnp.sum(queries * new_keys, axis=-1, keepdims=True)

    def final(n, s, source, sink, target, origin):
        return pltpu.make_async_remote_copy(
            src_ref=source,
            dst_ref=sink.at[origin, s],
            send_sem=last_send.at[n, s, target],
            recv_sem=last_recv.at[n, s, origin],
            device_id={"sp": target},
            device_id_type=MESH,
        )

    def stay(s):
        return [
            pltpu.make_async_copy(state_out.at[me, s], state_in.at[me, s], last_local.at[0, s]),
            pltpu.make_async_copy(row_out.at[s], row_in.at[me, s], last_local.at[1, s]),
        ]

    for s in range(sequences):
        for copy in kept(s):
            copy.wait()
        for offset in range(1, sp_size):
            source = (me + offset) % sp_size
            swap(s, source, source)[0].wait_recv()
        side = side_in[:, s].reshape(sp_size * side_rows, positions)
        running_row = exact_dot(side, upto)
        running_col = exact_dot(upto, side, ((0,), (1,)))
        side_col = exact_dot(eye, side, ((1,), (1,)))
        for offset in range(1, sp_size):
            source = (me + offset) % sp_size
            swap(s, source, source)[1].wait_recv()
        parts = []
        for b in range(sp_size):
            line = b * side_rows
            row = running_row[line : line + 1, :]
            col = running_col[:, line : line + 1]
            strength = side_col[:, line + 1 : line + 2]
            final_log = row[:, positions - 1 : positions]
            keys = kv_in[b, s, 0].astype(jnp.float32)
            keys = keys * lax.rsqrt(jnp.sum(keys * keys, axis=-1, keepdims=True) + 1e-06)
            within = jnp.where(lower, jnp.exp(jnp.where(lower, col - row, 0.0)), 0.0)
            scaled = keys * strength
            power = jnp.where(strict, -short_dot(scaled, keys, ((1,), (1,))) * within, 0.0)
            targets = jnp.concatenate(
                [kv_in[b, s, 1].astype(jnp.float32) * strength, scaled * jnp.exp(col)], axis=1
            ).astype(jnp.bfloat16)
            carried = (keys * jnp.exp(final_log - col)).T.astype(jnp.bfloat16)
            parts.append([eye + power, power, targets, carried, jnp.exp(final_log)])
        for part in parts:
            part[1] = short_dot(part[1], part[1])
        covered = 2
        while covered < positions:
            for part in parts:
                if covered * 2 < positions:
                    both = short_dot(part[1], jnp.concatenate([part[0], part[1]], axis=1))
                    part[0] = part[0] + both[:, :positions]
                    part[1] = both[:, positions:]
                else:
                    part[0] = part[0] + short_dot(part[1], part[0])
            covered = covered * 2
        for part in parts:
            part[2] = short_dot(part[0], part[2])
        state = None
        for _, _, solved, carried, shrink in parts:
            fresh = solved[:, :value_width]
            if state is None:
                state = short_dot(carried, fresh)
            else:
                fresh = fresh - short_dot(solved[:, value_width:], state)
                state = state * shrink + short_dot(carried, fresh)

        turned = state.T.astype(jnp.bfloat16)
        for j in range(sp_size):
            state_out[j, s] = turned[j * share : (j + 1) * share, :]
        for offset in range(1, sp_size):
            target = (me + offset) % sp_size
            final(0, s, state_out.at[target, s], state_in, target, me).start()
        wide = (8, key_width)
        first_row = grid_mask(*wide, lambda r, c: r == 0)
        probes = jnp.where(
            first_row,
            jnp.broadcast_to(queries[s : s + 1], wide),
            jnp.broadcast_to(new_keys[s : s + 1], wide),
        )
        reads = exact_dot(probes, state)
        query_read, key_read = reads[0:1], reads[1:2]
        new_value = jnp.sum(side_in[:, s, 2, :], axis=0, keepdims=True)
        raw = query_read + (next_strength_ref[s, me] * meets[s : s + 1]) * (new_value - key_read)
        row_out[s, 0:1, :] = raw * lax.rsqrt(
            jnp.sum(raw * raw, axis=-1, keepdims=True) / value_width + 1e-06
        )
        for offset in range(1, sp_size):
            target = (me + offset) % sp_size
            final(1, s, row_out.at[s], row_in, target, me).start()
        for copy in stay(s):
            copy.start()

    picker = grid_mask(value_width, share, lambda r, c: r == me * share + c).astype(jnp.float32)
    row_lines = row_in.shape[2]
    for s in range(sequences):
        for copy in stay(s):
            copy.wait()
        for offset in range(1, sp_size):
            source = (me + offset) % sp_size
            final(0, s, state_in.at[source, s], state_in, source, source).wait_recv()
            final(1, s, row_in.at[source, s], row_in, source, source).wait_recv()
        rows = exact_dot(row_in[:, s].reshape(sp_size * row_lines, value_width), picker)
        rows = rows * gain_ref[...].reshape(1, share)
        read_ref[s] = jnp.concatenate(
            [rows[i * row_lines : i * row_lines + 1] for i in range(sp_size)], axis=0
        ).astype(jnp.bfloat16)
        for i in range(sp_size):
            state_ref[s, i] = state_in[i, s]

    for s in range(sequences):
        for offset in range(1, sp_size):
            target = (me + offset) % sp_size
            for copy in swap(s, target, me):
                copy.wait_send()
            final(0, s, state_out.at[target, s], state_in, target, me).wait_send()
            final(1, s, row_out.at[s], row_in, target, me).wait_send()
    for distance in range(chips):
        for way, step in ((0, -1), (1, 1)):
            if distance == 0 and way == 1:
                continue
            origin_chip = chip + step * distance
            origin = origin_chip * CORES + core

            @pl.when((origin_chip >= 0) & (origin_chip < chips))
            def _(origin=origin):
                for s in range(sequences):
                    piece(origin, s, 2, partner).wait_send()

            for other, onward in ((0, chip + 1), (1, chip - 1)):
                if distance and other != way:
                    continue

                @pl.when(
                    (origin_chip >= 0)
                    & (origin_chip < chips)
                    & (onward >= 0)
                    & (onward < chips)
                )
                def _(origin=origin, other=other, onward=onward):
                    for s in range(sequences):
                        piece(origin, s, other, onward * CORES + core).wait_send()


def place_kernel(state_ref, read_ref, state_hbm, read_hbm, sem):
    copies = [
        pltpu.make_async_copy(state_ref, state_hbm, sem.at[0]),
        pltpu.make_async_copy(read_ref, read_hbm, sem.at[1]),
    ]
    for copy in copies:
        copy.start()
    for copy in copies:
        copy.wait()


def local_fused(
    tokens,
    key_matrix,
    value_matrix,
    gate_matrix,
    head_decay_rate,
    extra_log_decay,
    next_token_query,
    next_token_key,
    next_token_value,
    next_write_strength,
    read_norm_gain,
):
    sequences, positions, depth = tokens.shape
    local_heads = head_decay_rate.shape[0]
    sp_size = lax.axis_size("sp")
    tp_size = lax.axis_size("tp")
    key_total = key_matrix.shape[1]
    value_total = value_matrix.shape[1]
    key_width = key_total // local_heads
    value_width = value_total // local_heads
    share = value_width // sp_size
    rows = sequences * positions
    vmem = pl.BlockSpec(memory_space=pltpu.VMEM)
    smem = pl.BlockSpec(memory_space=pltpu.SMEM)
    anywhere = pl.BlockSpec(memory_space=pl.ANY)
    dma = pltpu.SemaphoreType.DMA
    turned, read = pl.pallas_call(
        functools.partial(fused_kernel, sp_size, tp_size),
        out_shape=(
            pltpu.VMEM((sequences, local_heads, share, key_width), jnp.bfloat16),
            pltpu.VMEM((sequences, local_heads, share), jnp.bfloat16),
        ),
        in_specs=[smem, smem] + [anywhere] * 9,
        out_specs=(vmem, vmem),
        scratch_shapes=[
            pltpu.VMEM((tp_size, sequences, positions, depth), jnp.bfloat16),
            pltpu.VMEM(key_matrix.shape, jnp.bfloat16),
            pltpu.VMEM(value_matrix.shape, jnp.bfloat16),
            pltpu.VMEM(gate_matrix.shape[::-1], jnp.bfloat16),
            pltpu.VMEM(extra_log_decay.shape, jnp.float32),
            pltpu.VMEM(next_token_query.shape, jnp.bfloat16),
            pltpu.VMEM(next_token_key.shape, jnp.bfloat16),
            pltpu.VMEM(next_token_value.shape, jnp.bfloat16),
            pltpu.VMEM(read_norm_gain.shape, jnp.float32),
            pltpu.VMEM((rows, key_total), jnp.float32),
            pltpu.VMEM((rows, value_total), jnp.float32),
            pltpu.VMEM((rows, gate_matrix.shape[1]), jnp.float32),
            pltpu.VMEM((sp_size, sequences, 2, positions, key_width), jnp.bfloat16),
            pltpu.VMEM((sp_size, sequences, 2, positions, key_width), jnp.bfloat16),
            pltpu.VMEM((sp_size, sequences, 8, positions), jnp.float32),
            pltpu.VMEM((sp_size, sequences, 8, positions), jnp.float32),
            pltpu.VMEM((sp_size, sequences, share, key_width), jnp.bfloat16),
            pltpu.VMEM((sp_size, sequences, share, key_width), jnp.bfloat16),
            pltpu.VMEM((sequences, 8, value_width), jnp.float32),
            pltpu.VMEM((sp_size, sequences, 8, value_width), jnp.float32),
            dma((sequences,)),
            dma((8,)),
            dma((tp_size, sequences)),
            dma((tp_size, sequences, 3)),
            dma((2, sequences, sp_size)),
            dma((2, sequences, sp_size)),
            dma((2, sequences)),
            dma((2, sequences, sp_size)),
            dma((2, sequences, sp_size)),
            dma((2, sequences)),
        ],
        compiler_params=pltpu.CompilerParams(
            collective_id=0, has_side_effects=True
        ),
    )(
        head_decay_rate,
        next_write_strength,
        tokens,
        key_matrix,
        value_matrix,
        gate_matrix.T,
        extra_log_decay,
        next_token_query,
        next_token_key,
        next_token_value,
        read_norm_gain,
    )
    turned, read = pl.pallas_call(
        place_kernel,
        out_shape=tuple(jax.ShapeDtypeStruct(a.shape, a.dtype) for a in (turned, read)),
        in_specs=[vmem, vmem],
        out_specs=(anywhere, anywhere),
        scratch_shapes=[dma((2,))],
    )(*(pltpu.with_memory_space_constraint(a, pltpu.VMEM) for a in (turned, read)))
    return jnp.swapaxes(turned, 2, 3), read


def local(*arguments):
    tokens, key_matrix, value_matrix = arguments[:3]
    sequences, positions, _ = tokens.shape
    local_heads = arguments[4].shape[0]
    sp_size = lax.axis_size("sp")
    fits = (
        local_heads == sp_size
        and sequences == 2
        and lax.axis_size("tp") % CORES == 0
        and lax.axis_size("tp") > CORES
        and positions == key_matrix.shape[1] // local_heads
        and positions == value_matrix.shape[1] // local_heads
        and positions % 128 == 0
    )
    return local_fused(*arguments) if fits else local_general(*arguments)


def solution(mesh):
    in_specs = (
        P(None, "sp", "tp"),
        P(None, "tp"),
        P(None, "tp"),
        P(),
        P("tp"),
        P(None, "tp", "sp"),
        P(None, "tp"),
        P(None, "tp"),
        P(None, "tp", "sp"),
        P(None, "tp"),
        P("sp"),
    )
    out_specs = (P(None, "tp", None, "sp"), P(None, "tp", "sp"))
    return jax.shard_map(local, mesh=mesh, in_specs=in_specs, out_specs=out_specs, check_vma=False)
```

```python
import functools

import jax
import jax.numpy as jnp
from jax import lax
from jax.experimental import pallas as pl
from jax.experimental.pallas import tpu as pltpu
from jax.sharding import PartitionSpec as P

DV = 128
CORES = 2
MESH = pl.DeviceIdType.MESH


exact_mode = lax.Precision.HIGHEST
strength_offset = 5.0


def unit_rows(matrix):
    return matrix * lax.rsqrt(jnp.sum(matrix * matrix, axis=-1, keepdims=True) + 1e-06)


def nilpotent_inverse(mixing):
    extent = mixing.shape[-1]
    result = jnp.zeros_like(mixing) + jnp.eye(extent, dtype=jnp.float32)
    powered = -mixing
    covered = 1
    while covered < extent:
        product = lax.optimization_barrier(
            jnp.einsum("...ij,...jk->...ik", result, powered, precision=exact_mode)
        )
        result = result + product
        powered = jnp.einsum("...ij,...jk->...ik", powered, powered, precision=exact_mode)
        covered = covered * 2
    return result


def block_terms(unit_keys, values, decay_logarithm, strength):
    extent = unit_keys.shape[-2]
    lower = jnp.tril(jnp.ones((extent, extent), jnp.bool_))
    strict = jnp.tril(jnp.ones((extent, extent), jnp.bool_), -1)
    running = jnp.cumsum(decay_logarithm, axis=-1)
    spread = running[..., :, None] - running[..., None, :]
    within = jnp.where(lower, jnp.exp(jnp.where(lower, spread, 0.0)), 0.0)
    scaled = unit_keys * strength[..., None]
    mixing = jnp.where(
        strict,
        jnp.einsum("...id,...jd->...ij", scaled, unit_keys, precision=exact_mode) * within,
        0.0,
    )
    inverse = nilpotent_inverse(mixing)
    writes = jnp.einsum(
        "...ij,...je->...ie", inverse, values * strength[..., None], precision=exact_mode
    )
    erases = jnp.einsum(
        "...ij,...jd->...id", inverse, scaled * jnp.exp(running)[..., None], precision=exact_mode
    )
    final_log = running[..., -1]
    carried = unit_keys * jnp.exp(final_log[..., None] - running)[..., None]
    return (writes, erases, carried, final_log)


def split_blocks(array, block_count):
    shaped = array.reshape(
        array.shape[:2] + (block_count, array.shape[2] // block_count) + array.shape[3:]
    )
    return jnp.moveaxis(shaped, 2, 0)


def local_general(
    tokens,
    key_matrix,
    value_matrix,
    gate_matrix,
    head_decay_rate,
    extra_log_decay,
    next_token_query,
    next_token_key,
    next_token_value,
    next_write_strength,
    read_norm_gain,
):
    sequences, positions, _ = tokens.shape
    local_heads = head_decay_rate.shape[0]
    key_width = key_matrix.shape[1] // local_heads
    value_width = value_matrix.shape[1] // local_heads
    all_heads = gate_matrix.shape[1] // 2
    group_size = lax.axis_size("sp")
    column_share = value_width // group_size
    first_head = lax.axis_index("tp") * local_heads
    decay_cols = lax.dynamic_slice_in_dim(gate_matrix, first_head, local_heads, 1)
    strength_cols = lax.dynamic_slice_in_dim(gate_matrix, all_heads + first_head, local_heads, 1)
    gate_cols = jnp.concatenate([decay_cols, strength_cols], axis=1)
    row_count = sequences * positions
    incoming = lax.all_gather(tokens, "tp", axis=2, tiled=True)
    span_width = incoming.shape[2]
    flat_rows = incoming.reshape(row_count, span_width)
    products = lax.optimization_barrier(
        (
            jnp.dot(flat_rows, key_matrix, preferred_element_type=jnp.float32),
            jnp.dot(flat_rows, value_matrix, preferred_element_type=jnp.float32),
            jnp.dot(flat_rows, gate_cols, preferred_element_type=jnp.float32),
        )
    )
    key_sum = products[0]
    value_sum = products[1]
    gate_pre = products[2]
    key_float = lax.optimization_barrier(key_sum.astype(jnp.bfloat16)).astype(jnp.float32)
    value_float = lax.optimization_barrier(value_sum.astype(jnp.bfloat16)).astype(jnp.float32)
    unit_keys = unit_rows(
        key_float.reshape(sequences, positions, local_heads, key_width).transpose(0, 2, 1, 3)
    )
    values = value_float.reshape(sequences, positions, local_heads, value_width).transpose(
        0, 2, 1, 3
    )
    gate_projected = gate_pre.reshape(sequences, positions, 2 * local_heads).transpose(0, 2, 1)
    decay_logarithm = (
        -head_decay_rate[None, :, None] * jax.nn.softplus(gate_projected[:, :local_heads])
        + extra_log_decay
    )
    strength = jax.nn.sigmoid(gate_projected[:, local_heads:] - strength_offset)
    block_count = positions // min(64, positions)
    block_parts = block_terms(
        split_blocks(unit_keys, block_count),
        split_blocks(values, block_count),
        split_blocks(decay_logarithm, block_count),
        split_blocks(strength, block_count),
    )
    identity = jnp.zeros((sequences, local_heads, key_width, key_width), jnp.float32) + jnp.eye(
        key_width, dtype=jnp.float32
    )
    start_map = jnp.concatenate(
        [identity, jnp.zeros((sequences, local_heads, key_width, value_width), jnp.float32)],
        axis=-1,
    )

    def advance(current, block_part):
        writes, erases, carried, final_log = block_part
        padded = jnp.concatenate(
            [jnp.zeros(writes.shape[:-1] + (key_width,), jnp.float32), writes], axis=-1
        )
        removed = lax.optimization_barrier(
            jnp.einsum("shcd,shde->shce", erases, current, precision=exact_mode)
        )
        fresh = padded - removed
        added = lax.optimization_barrier(
            jnp.einsum("shcd,shce->shde", carried, fresh, precision=exact_mode)
        )
        current = current * jnp.exp(final_log)[..., None, None] + added
        return (current, None)

    local_map, _ = lax.scan(advance, start_map, block_parts)
    carry_map = local_map[..., :key_width]
    write_map = local_map[..., key_width:]
    carry_copies = jnp.broadcast_to(carry_map[None], (group_size,) + carry_map.shape)
    write_parts = jnp.moveaxis(
        write_map.reshape(sequences, local_heads, key_width, group_size, column_share), 3, 0
    )
    carries = lax.all_to_all(carry_copies, "sp", split_axis=0, concat_axis=0, tiled=True)
    write_cols = lax.all_to_all(write_parts, "sp", split_axis=0, concat_axis=0, tiled=True)

    def fold_step(current, block_map):
        moved = lax.optimization_barrier(
            jnp.einsum("shij,shje->shie", block_map[0], current, precision=exact_mode)
        )
        return (moved + block_map[1], None)

    begin_state = jnp.zeros(write_cols.shape[1:], jnp.float32)
    folded, _ = lax.scan(fold_step, begin_state, (carries, write_cols))
    query_rows = next_token_query.astype(jnp.float32).reshape(sequences, local_heads, key_width)
    unit_new = unit_rows(
        next_token_key.astype(jnp.float32).reshape(sequences, local_heads, key_width)
    )
    value_rows = next_token_value.astype(jnp.float32)
    key_read = jnp.einsum("shd,shde->she", unit_new, folded, precision=exact_mode)
    query_read = jnp.einsum("shd,shde->she", query_rows, folded, precision=exact_mode)
    intersection = jnp.sum(query_rows * unit_new, axis=-1)
    read_raw = query_read + (next_write_strength * intersection)[..., None] * (
        value_rows - key_read
    )
    square_total = lax.psum(jnp.sum(read_raw * read_raw, axis=-1, keepdims=True), "sp")
    first_read = read_raw * lax.rsqrt(square_total / DV + 1e-06) * read_norm_gain
    return (folded.astype(jnp.bfloat16), first_read.astype(jnp.bfloat16))


def short_dot(left, right, contract=((1,), (0,))):
    return lax.dot_general(
        left.astype(jnp.bfloat16),
        right.astype(jnp.bfloat16),
        (contract, ((), ())),
        preferred_element_type=jnp.float32,
    )


def three_terms(x):
    first = x.astype(jnp.bfloat16)
    rest = x - first.astype(jnp.float32)
    second = rest.astype(jnp.bfloat16)
    third = (rest - second.astype(jnp.float32)).astype(jnp.bfloat16)
    return first, second, third


def softplus(x):
    return jnp.maximum(x, 0.0) + jnp.log1p(jnp.exp(-jnp.abs(x)))


def grid_mask(rows, cols, rule):
    row = lax.broadcasted_iota(jnp.int32, (rows, cols), 0)
    col = lax.broadcasted_iota(jnp.int32, (rows, cols), 1)
    return rule(row, col)


def compose(late, early):
    late_map, late_write, late_keep = late
    early_map, early_write, early_keep = early
    width = early_map.shape[1]
    moved = short_dot(late_map, jnp.concatenate([early_map, early_write], axis=1))
    return (
        late_keep * early_map + early_keep * late_map - moved[:, :width],
        late_keep * early_write + late_write - moved[:, width:],
        late_keep * early_keep,
    )


def compose_write(late, early_write):
    late_map, late_write, late_keep = late
    return late_keep * early_write + late_write - short_dot(late_map, early_write)


def fused_kernel(
    sp_size,
    tp_size,
    rate_ref,
    next_strength_ref,
    tokens_ref,
    key_ref,
    value_ref,
    gate_hbm,
    extra_hbm,
    query_hbm,
    new_key_hbm,
    new_value_hbm,
    gain_hbm,
    state_ref,
    read_ref,
    gathered,
    key_w,
    value_w,
    gate_ref,
    gate_own,
    extra_ref,
    query_ref,
    new_key_ref,
    new_value_ref,
    gain_ref,
    key_acc,
    value_acc,
    gate_acc,
    key_out,
    key_in,
    value_out,
    value_in,
    side_out,
    side_in,
    state_out,
    row_out,
    row_in,
    load_sem,
    weight_sem,
    gather_recv,
    gather_send,
    swap_recv,
    swap_send,
    last_recv,
    last_send,
    above_sem,
    peers_sem,
):
    sequences, positions, depth = tokens_ref.shape
    local_heads = extra_ref.shape[1]
    key_width = key_acc.shape[1] // local_heads
    value_width = value_acc.shape[1] // local_heads
    share = value_width // sp_size
    all_heads = gate_ref.shape[0] // 2
    chips = tp_size // CORES
    me = lax.axis_index("sp")
    spot = lax.axis_index("tp")
    chip = spot // CORES
    core = spot % CORES
    partner = chip * CORES + (1 - core)
    half = positions // 2
    units = [(s, part * half, half) for s in range(sequences) for part in range(2)]
    last_unit = len(units) - 1
    batches = [(0, 0, positions, (0, 1)), (1, 0, half, (2,)), (1, half, half, (3,))]
    others = [sp_size - 1 - me, me + 1 - 2 * (me % 2), (me + 2) % sp_size]

    loads = [
        pltpu.make_async_copy(tokens_ref.at[s], gathered.at[spot, s], load_sem.at[s])
        for s in range(sequences)
    ]
    for load in loads:
        load.start()

    barrier = pltpu.get_barrier_semaphore()
    pl.semaphore_signal(barrier, inc=1, device_id={"tp": partner}, device_id_type=MESH)

    @pl.when(chip < chips - 1)
    def _():
        pl.semaphore_signal(barrier, inc=1, device_id={"tp": spot + CORES}, device_id_type=MESH)

    for other in range(1, sp_size):

        @pl.when(me < other)
        def _(other=other):
            pl.semaphore_signal(barrier, inc=1, device_id={"sp": other}, device_id_type=MESH)

    weights = [
        pltpu.make_async_copy(key_ref, key_w, weight_sem.at[0]),
        pltpu.make_async_copy(value_ref, value_w, weight_sem.at[1]),
        pltpu.make_async_copy(gate_hbm, gate_ref, weight_sem.at[2]),
        pltpu.make_async_copy(extra_hbm, extra_ref, weight_sem.at[3]),
        pltpu.make_async_copy(query_hbm, query_ref, weight_sem.at[4]),
        pltpu.make_async_copy(new_key_hbm, new_key_ref, weight_sem.at[5]),
        pltpu.make_async_copy(new_value_hbm, new_value_ref, weight_sem.at[6]),
        pltpu.make_async_copy(gain_hbm, gain_ref, weight_sem.at[7]),
    ]
    for weight in weights:
        weight.start()
    pl.semaphore_wait(barrier, jnp.where(chip > 0, 1, 0) + 1 + me)

    @pl.when(chip > 0)
    def _():
        pl.semaphore_signal(above_sem, inc=1, device_id={"tp": spot - CORES}, device_id_type=MESH)

    for other in range(sp_size - 1):

        @pl.when(other < me)
        def _(other=other):
            pl.semaphore_signal(peers_sem, inc=1, device_id={"sp": other}, device_id_type=MESH)

    def piece(origin, u, way, target):
        s, low, count = units[u]
        block = gathered.at[origin, s, pl.ds(low, count)]
        return pltpu.make_async_remote_copy(
            src_ref=block,
            dst_ref=block,
            send_sem=gather_send.at[origin, u, way],
            recv_sem=gather_recv.at[origin, u],
            device_id={"tp": target},
            device_id_type=MESH,
        )

    for load in loads:
        load.wait()

    for u in range(len(units)):

        @pl.when((chip > 0) if u < last_unit else (chip == chips - 1))
        def _(u=u):
            piece(spot, u, 1, spot - CORES).start()

        piece(spot, u, 2, partner).start()

    @pl.when(chip < chips - 1)
    def _():
        pl.semaphore_wait(above_sem, 1)

    for u in range(len(units)):

        @pl.when((chip < chips - 1) if u < last_unit else (chip == 0))
        def _(u=u):
            piece(spot, u, 0, spot + CORES).start()

    key_acc[...] = jnp.zeros_like(key_acc)
    value_acc[...] = jnp.zeros_like(value_acc)
    gate_acc[...] = jnp.zeros_like(gate_acc)
    side_out[...] = jnp.zeros_like(side_out)

    def add_in(rows, span, batch):
        s, low, count, parts = batches[batch]
        cut = slice(s * positions + low, s * positions + low + count)
        key_acc[cut] += jnp.dot(rows, key_w[span, :], preferred_element_type=jnp.float32)
        value_acc[cut] += jnp.dot(rows, value_w[span, :], preferred_element_type=jnp.float32)
        gates = lax.dot_general(
            gate_own[:, span],
            rows,
            (((1,), (1,)), ((), ())),
            preferred_element_type=jnp.float32,
        )
        gate_acc[s, :, low : low + count] += gates

    def take_one(block, batch):
        s, low, count, _ = batches[batch]
        span = pl.ds(pl.multiple_of(block * depth, depth), depth)
        add_in(gathered[block, s, low : low + count], span, batch)

    def take_chip(origin_chip, batch):
        s, low, count, _ = batches[batch]
        width = CORES * depth
        span = pl.ds(pl.multiple_of(origin_chip * width, width), width)
        rows = jnp.concatenate(
            [gathered[origin_chip * CORES + c, s, low : low + count] for c in range(CORES)], axis=1
        )
        add_in(rows, span, batch)

    first = spot * local_heads

    def prepare():
        for weight in weights:
            weight.wait()
        chooser = grid_mask(
            2 * local_heads,
            2 * all_heads,
            lambda r, c: c
            == jnp.where(r < local_heads, first + r, all_heads + first + r - local_heads),
        ).astype(jnp.float32)
        gate_own[...] = short_dot(chooser, gate_ref[...]).astype(jnp.bfloat16)
        placer = grid_mask(share, value_width, lambda r, c: c == me * share + r)
        for s in range(sequences):
            new_value = short_dot(new_value_ref[s], placer.astype(jnp.float32))
            for h in range(local_heads):
                side_out[h, s, 2:3, :] = new_value[h : h + 1, :]

    def own(batch):
        for u in batches[batch][3]:
            piece(partner, u, 2, partner).wait_recv()
        take_chip(chip, batch)

    def relay(distance, u):
        for way, step in ((0, -1), (1, 1)):
            origin_chip = chip + step * distance
            origin = origin_chip * CORES + core
            present = (origin_chip >= 0) & (origin_chip < chips)
            onward = chip - step
            beyond = (onward >= 0) & (onward < chips)

            @pl.when(present)
            def _(way=way, origin_chip=origin_chip, origin=origin, onward=onward, beyond=beyond):
                piece(origin, u, way, partner).wait_recv()

                @pl.when(beyond)
                def _():
                    piece(origin, u, way, onward * CORES + core).start()

                piece(origin, u, 2, partner).start()
                if u == 1:

                    @pl.when(beyond & (origin_chip == (0 if way == 0 else chips - 1)))
                    def _():
                        piece(spot, last_unit, way, onward * CORES + core).start()

    def absorb(distance, batch):
        def one_side(side, carry):
            origin_chip = chip + (2 * side - 1) * distance

            @pl.when((origin_chip >= 0) & (origin_chip < chips))
            def _():
                for u in batches[batch][3]:
                    piece(origin_chip * CORES + 1 - core, u, 2, partner).wait_recv()
                take_chip(origin_chip, batch)

            return carry

        lax.fori_loop(0, 2, one_side, 0)

    def absorb_lane(distance, batch, lane):
        def one_side(side, carry):
            origin_chip = chip + (2 * side - 1) * distance

            @pl.when((origin_chip >= 0) & (origin_chip < chips))
            def _():
                block = origin_chip * CORES + (core if lane == 0 else 1 - core)
                if lane:
                    for u in batches[batch][3]:
                        piece(block, u, 2, partner).wait_recv()
                take_one(block, batch)

            return carry

        lax.fori_loop(0, 2, one_side, 0)

    def swap(n, slot, target, origin):
        s, low, count, _ = batches[slot]
        if n == 0:
            source, sink = side_out.at[target, slot], side_in.at[origin, slot]
        else:
            source, sink = ((key_out, key_in), (value_out, value_in))[n - 1]
            source = source.at[target, s, pl.ds(low, count)]
            sink = sink.at[origin, s, pl.ds(low, count)]
        return pltpu.make_async_remote_copy(
            src_ref=source,
            dst_ref=sink,
            send_sem=swap_send.at[n, slot, target],
            recv_sem=swap_recv.at[n, slot, origin],
            device_id={"sp": target},
            device_id_type=MESH,
        )

    def hand_out(slot):
        s, low, count, _ = batches[slot]
        cut = slice(s * positions + low, s * positions + low + count)
        gates = gate_acc[s, :, low : low + count]
        extra = extra_ref[s, :, low : low + count]
        for h in range(local_heads):
            side_out[h, slot, 0:1, low : low + count] = (
                -rate_ref[h] * softplus(gates[h : h + 1]) + extra[h : h + 1, :]
            )
            side_out[h, slot, 1:2, low : low + count] = jax.nn.sigmoid(
                gates[local_heads + h : local_heads + h + 1] - strength_offset
            )
        for other in others:
            swap(0, slot, other, me).start()
        for h in range(local_heads):
            key_out[h, s, low : low + count] = key_acc[
                cut, h * key_width : (h + 1) * key_width
            ].astype(jnp.bfloat16)
        for other in others:
            swap(1, slot, other, me).start()
        for h in range(local_heads):
            value_out[h, s, low : low + count] = value_acc[
                cut, h * value_width : (h + 1) * value_width
            ].astype(jnp.bfloat16)
        for other in others:
            swap(2, slot, other, me).start()
        side_in[me, slot] = side_out[me, slot]
        key_in[me, s, low : low + count] = key_out[me, s, low : low + count]
        value_in[me, s, low : low + count] = value_out[me, s, low : low + count]

    far = chips - 1
    last_batch = len(batches) - 1
    steps = {1: [(1, 0), (1, 1), (1, 2)]} if far > 1 else {}
    for distance in range(2, far):
        steps[distance] = [(distance, 0), (distance, 1), (distance, 2)]
    work = [(own, (0,)), (own, (1,)), (own, (2,))]
    prepared = False
    for distance in range(1, far):
        for event in steps[distance]:
            relay(*event)
            if not prepared:
                prepare()
                prepared = True
            if work:
                act, operands = work.pop(0)
                act(*operands)
            if event[1] == 1:
                work.insert(0, (absorb, (distance, 0)))
            if event[1] == 2:
                work.append((absorb, (distance, 1)))
    if not prepared:
        prepare()
    for act, operands in [w for w in work if w[0] is own]:
        act(*operands)
    work = [w for w in work if w[0] is absorb]
    relay(far, 0)
    for act, operands in [w for w in work if w[1][1] == 0]:
        act(*operands)
    work = [w for w in work if w[1][1] != 0]
    relay(far, 1)
    absorb(far, 0)

    @pl.when(me < sp_size - 1)
    def _():
        pl.semaphore_wait(peers_sem, sp_size - 1 - me)

    hand_out(0)
    if far > 1:
        relay(1, last_unit)
    for act, operands in work:
        act(*operands)
    relay(far, 2)
    if far > 1:
        absorb(1, last_batch)
    absorb(far, 1)
    hand_out(1)
    pending = None
    for distance in range(2, far):
        relay(distance, last_unit)
        if pending is not None:
            absorb(*pending)
        pending = (distance, last_batch)
    relay(far, last_unit)
    if pending is not None:
        absorb(*pending)
    absorb_lane(far, last_batch, 0)
    absorb_lane(far, last_batch, 1)
    hand_out(2)

    for u in range(len(units)):
        piece(spot, u, 2, partner).wait_send()

        @pl.when(chip < chips - 1)
        def _(u=u):
            piece(spot, u, 0, spot + CORES).wait_send()

        @pl.when(chip > 0)
        def _(u=u):
            piece(spot, u, 1, spot - CORES).wait_send()

        for distance in range(1, chips):
            for way, step in ((0, -1), (1, 1)):
                origin_chip = chip + step * distance
                origin = origin_chip * CORES + core
                onward = chip - step
                present = (origin_chip >= 0) & (origin_chip < chips)

                @pl.when(present)
                def _(u=u, origin=origin):
                    piece(origin, u, 2, partner).wait_send()

                @pl.when(present & (onward >= 0) & (onward < chips))
                def _(u=u, origin=origin, way=way, onward=onward):
                    piece(origin, u, way, onward * CORES + core).wait_send()

    side_rows = side_in.shape[2]
    upto = grid_mask(positions, positions, lambda r, c: r <= c).astype(jnp.float32)
    down = jnp.concatenate(
        [
            grid_mask(positions, positions, lambda r, c: c <= r).astype(jnp.float32),
            grid_mask(positions, positions, lambda r, c: c == r).astype(jnp.float32),
        ],
        axis=0,
    )
    lanes = pl.ds(pl.multiple_of(me * key_width, key_width), key_width)
    queries = query_ref[:, lanes].astype(jnp.float32)
    new_keys = new_key_ref[:, lanes].astype(jnp.float32)
    new_keys = new_keys * lax.rsqrt(jnp.sum(new_keys * new_keys, axis=-1, keepdims=True) + 1e-06)
    meets = jnp.sum(queries * new_keys, axis=-1, keepdims=True)

    def block_maps(s, slots):
        count = positions
        eye = grid_mask(count, count, lambda r, c: r == c).astype(jnp.float32)
        lower = grid_mask(count, count, lambda r, c: r >= c)
        strict = grid_mask(count, count, lambda r, c: r > c)
        for slot in slots:
            for other in others:
                swap(0, slot, other, other).wait_recv()
        side = three_terms(
            sum(side_in[:, slot].reshape(sp_size * side_rows, positions) for slot in slots)
        )
        running_row = sum(short_dot(term, upto) for term in side)
        columns = sum(short_dot(down, term, ((1,), (1,))) for term in side)
        for slot in slots:
            for other in others:
                swap(1, slot, other, other).wait_recv()
        parts = []
        for b in range(sp_size):
            line = b * side_rows
            row = running_row[line : line + 1, :]
            col = columns[:positions, line : line + 1]
            strength = columns[positions:, line + 1 : line + 2]
            final_log = row[:, count - 1 : count]
            keys = key_in[b, s].astype(jnp.float32)
            keys = keys * lax.rsqrt(jnp.sum(keys * keys, axis=-1, keepdims=True) + 1e-06)
            within = jnp.where(lower, jnp.exp(jnp.where(lower, col - row, 0.0)), 0.0)
            scaled = keys * strength
            power = jnp.where(strict, -short_dot(scaled, keys, ((1,), (1,))) * within, 0.0)
            erased = scaled * jnp.exp(col)
            carried = (keys * jnp.exp(final_log - col)).T.astype(jnp.bfloat16)
            parts.append([eye + power, power, strength, erased, carried, jnp.exp(final_log)])
        for part in parts:
            part[1] = short_dot(part[1], part[1])
        covered = 2
        while covered < count:
            for part in parts:
                if covered * 2 < count:
                    both = short_dot(part[1], jnp.concatenate([part[0], part[1]], axis=1))
                    part[0] = part[0] + both[:, :count]
                    part[1] = both[:, count:]
                else:
                    part[0] = part[0] + short_dot(part[1], part[0])
            covered = covered * 2
        for slot in slots:
            for other in others:
                swap(2, slot, other, other).wait_recv()
        solved = []
        for b, part in enumerate(parts):
            values = value_in[b, s].astype(jnp.float32) * part[2]
            solved.append(short_dot(part[0], jnp.concatenate([part[3], values], axis=1)))
        maps = []
        for part, both in zip(parts, solved):
            both = short_dot(part[4], both)
            maps.append((both[:, :key_width], both[:, key_width:], part[5]))
        return maps

    def final(n, s, target, origin):
        source, sink = (
            (state_out.at[target, s], state_ref.at[s, origin]),
            (row_out.at[target, s], row_in.at[origin, s]),
        )[n]
        return pltpu.make_async_remote_copy(
            src_ref=source,
            dst_ref=sink,
            send_sem=last_send.at[n, s, target],
            recv_sem=last_recv.at[n, s, origin],
            device_id={"sp": target},
            device_id_type=MESH,
        )

    def finish(s, maps):
        while len(maps) > 2:
            maps = [compose(maps[i + 1], maps[i]) for i in range(0, len(maps), 2)]
        state = compose_write(maps[1], maps[0][1])
        wide = (8, key_width)
        first_row = grid_mask(*wide, lambda r, c: r == 0)
        probes = jnp.where(
            first_row,
            jnp.broadcast_to(queries[s : s + 1], wide),
            jnp.broadcast_to(new_keys[s : s + 1], wide),
        )
        probe_terms, state_terms = three_terms(probes)[:2], three_terms(state)[:2]
        reads = (
            short_dot(probe_terms[0], state_terms[0])
            + short_dot(probe_terms[0], state_terms[1])
            + short_dot(probe_terms[1], state_terms[0])
        )
        turned = state.T.astype(jnp.bfloat16)
        for j in range(sp_size):
            state_out[j, s] = turned[j * share : (j + 1) * share, :]
        for other in others:
            final(0, s, other, me).start()
        query_read, key_read = reads[0:1], reads[1:2]
        new_value = jnp.sum(side_in[:, s, 2, :], axis=0, keepdims=True)
        raw = query_read + (next_strength_ref[s, me] * meets[s : s + 1]) * (new_value - key_read)
        raw = raw * lax.rsqrt(jnp.sum(raw * raw, axis=-1, keepdims=True) / value_width + 1e-06)
        for j in range(sp_size):
            turn = j * share
            row_out[j, s, 0:1, :] = (
                jnp.concatenate([raw[:, turn:], raw[:, :turn]], axis=1) if j else raw
            )
        for other in others:
            final(1, s, other, me).start()
        state_ref[s, me] = state_out[me, s]
        row_in[me, s] = row_out[me, s]

    row_out[...] = jnp.zeros_like(row_out)
    finish(0, block_maps(0, (0,)))
    finish(1, block_maps(1, (1, 2)))

    for slot in range(len(batches)):
        for n in range(3):
            for other in others:
                swap(n, slot, other, me).wait_send()
    for s in range(sequences):
        for n in range(2):
            for other in others:
                final(n, s, other, me).wait_send()
    for s in range(sequences):
        for other in others:
            final(1, s, other, other).wait_recv()
        rows = jnp.concatenate([row_in[i, s, 0:1, :share] for i in range(sp_size)], axis=0)
        read_ref[s] = (rows * gain_ref[...].reshape(1, share)).astype(jnp.bfloat16)
    for s in range(sequences):
        for other in others:
            final(0, s, other, other).wait_recv()


def place_kernel(state_ref, read_ref, state_hbm, read_hbm, sem):
    copies = [
        pltpu.make_async_copy(state_ref, state_hbm, sem.at[0]),
        pltpu.make_async_copy(read_ref, read_hbm, sem.at[1]),
    ]
    for copy in copies:
        copy.start()
    for copy in copies:
        copy.wait()


def local_fused(
    tokens,
    key_matrix,
    value_matrix,
    gate_matrix,
    head_decay_rate,
    extra_log_decay,
    next_token_query,
    next_token_key,
    next_token_value,
    next_write_strength,
    read_norm_gain,
):
    sequences, positions, depth = tokens.shape
    local_heads = head_decay_rate.shape[0]
    sp_size = lax.axis_size("sp")
    tp_size = lax.axis_size("tp")
    key_total = key_matrix.shape[1]
    value_total = value_matrix.shape[1]
    key_width = key_total // local_heads
    value_width = value_total // local_heads
    share = value_width // sp_size
    rows = sequences * positions
    units = 2 * sequences
    slots = sequences + 1
    vmem = pl.BlockSpec(memory_space=pltpu.VMEM)
    smem = pl.BlockSpec(memory_space=pltpu.SMEM)
    anywhere = pl.BlockSpec(memory_space=pl.ANY)
    dma = pltpu.SemaphoreType.DMA
    held = (sp_size, sequences, positions)
    turned, read = pl.pallas_call(
        functools.partial(fused_kernel, sp_size, tp_size),
        out_shape=(
            pltpu.VMEM((sequences, local_heads, share, key_width), jnp.bfloat16),
            pltpu.VMEM((sequences, local_heads, share), jnp.bfloat16),
        ),
        in_specs=[smem, smem] + [anywhere] * 9,
        out_specs=(vmem, vmem),
        scratch_shapes=[
            pltpu.VMEM((tp_size, sequences, positions, depth), jnp.bfloat16),
            pltpu.VMEM(key_matrix.shape, jnp.bfloat16),
            pltpu.VMEM(value_matrix.shape, jnp.bfloat16),
            pltpu.VMEM(gate_matrix.shape[::-1], jnp.bfloat16),
            pltpu.VMEM((2 * local_heads, gate_matrix.shape[0]), jnp.bfloat16),
            pltpu.VMEM(extra_log_decay.shape, jnp.float32),
            pltpu.VMEM(next_token_query.shape, jnp.bfloat16),
            pltpu.VMEM(next_token_key.shape, jnp.bfloat16),
            pltpu.VMEM(next_token_value.shape, jnp.bfloat16),
            pltpu.VMEM(read_norm_gain.shape, jnp.float32),
            pltpu.VMEM((rows, key_total), jnp.float32),
            pltpu.VMEM((rows, value_total), jnp.float32),
            pltpu.VMEM((sequences, 2 * local_heads, positions), jnp.float32),
            pltpu.VMEM((*held, key_width), jnp.bfloat16),
            pltpu.VMEM((*held, key_width), jnp.bfloat16),
            pltpu.VMEM((*held, value_width), jnp.bfloat16),
            pltpu.VMEM((*held, value_width), jnp.bfloat16),
            pltpu.VMEM((sp_size, slots, 8, positions), jnp.float32),
            pltpu.VMEM((sp_size, slots, 8, positions), jnp.float32),
            pltpu.VMEM((sp_size, sequences, share, key_width), jnp.bfloat16),
            pltpu.VMEM((sp_size, sequences, 8, value_width), jnp.float32),
            pltpu.VMEM((sp_size, sequences, 8, value_width), jnp.float32),
            dma((sequences,)),
            dma((8,)),
            dma((tp_size, units)),
            dma((tp_size, units, 3)),
            dma((3, slots, sp_size)),
            dma((3, slots, sp_size)),
            dma((2, sequences, sp_size)),
            dma((2, sequences, sp_size)),
            pltpu.SemaphoreType.REGULAR,
            pltpu.SemaphoreType.REGULAR,
        ],
        compiler_params=pltpu.CompilerParams(
            collective_id=0, has_side_effects=True
        ),
    )(
        head_decay_rate,
        next_write_strength,
        tokens,
        key_matrix,
        value_matrix,
        gate_matrix.T,
        extra_log_decay,
        next_token_query,
        next_token_key,
        next_token_value,
        read_norm_gain,
    )
    turned, read = pl.pallas_call(
        place_kernel,
        out_shape=tuple(jax.ShapeDtypeStruct(a.shape, a.dtype) for a in (turned, read)),
        in_specs=[vmem, vmem],
        out_specs=(anywhere, anywhere),
        scratch_shapes=[dma((2,))],
    )(*(pltpu.with_memory_space_constraint(a, pltpu.VMEM) for a in (turned, read)))
    return jnp.swapaxes(turned, 2, 3), read


def local(*arguments):
    tokens, key_matrix, value_matrix = arguments[:3]
    sequences, positions, _ = tokens.shape
    local_heads = arguments[4].shape[0]
    sp_size = lax.axis_size("sp")
    fits = (
        local_heads == sp_size
        and sp_size == 4
        and sequences == 2
        and 2 * local_heads == 8
        and lax.axis_size("tp") % CORES == 0
        and lax.axis_size("tp") > CORES
        and positions == key_matrix.shape[1] // local_heads
        and positions == value_matrix.shape[1] // local_heads
        and positions % 128 == 0
    )
    return local_fused(*arguments) if fits else local_general(*arguments)


def solution(mesh):
    in_specs = (
        P(None, "sp", "tp"),
        P(None, "tp"),
        P(None, "tp"),
        P(),
        P("tp"),
        P(None, "tp", "sp"),
        P(None, "tp"),
        P(None, "tp"),
        P(None, "tp", "sp"),
        P(None, "tp"),
        P("sp"),
    )
    out_specs = (P(None, "tp", None, "sp"), P(None, "tp", "sp"))
    return jax.shard_map(local, mesh=mesh, in_specs=in_specs, out_specs=out_specs, check_vma=False)
```

```python
import functools

import jax
import jax.numpy as jnp
from jax import lax
from jax.experimental import pallas as pl
from jax.experimental.pallas import tpu as pltpu
from jax.sharding import PartitionSpec as P

DV = 128
CORES = 2
MESH = pl.DeviceIdType.MESH


exact_mode = lax.Precision.HIGHEST
strength_offset = 5.0


def unit_rows(matrix):
    return matrix * lax.rsqrt(jnp.sum(matrix * matrix, axis=-1, keepdims=True) + 1e-06)


def nilpotent_inverse(mixing):
    extent = mixing.shape[-1]
    result = jnp.zeros_like(mixing) + jnp.eye(extent, dtype=jnp.float32)
    powered = -mixing
    covered = 1
    while covered < extent:
        product = lax.optimization_barrier(
            jnp.einsum("...ij,...jk->...ik", result, powered, precision=exact_mode)
        )
        result = result + product
        powered = jnp.einsum("...ij,...jk->...ik", powered, powered, precision=exact_mode)
        covered = covered * 2
    return result


def block_terms(unit_keys, values, decay_logarithm, strength):
    extent = unit_keys.shape[-2]
    lower = jnp.tril(jnp.ones((extent, extent), jnp.bool_))
    strict = jnp.tril(jnp.ones((extent, extent), jnp.bool_), -1)
    running = jnp.cumsum(decay_logarithm, axis=-1)
    spread = running[..., :, None] - running[..., None, :]
    within = jnp.where(lower, jnp.exp(jnp.where(lower, spread, 0.0)), 0.0)
    scaled = unit_keys * strength[..., None]
    mixing = jnp.where(
        strict,
        jnp.einsum("...id,...jd->...ij", scaled, unit_keys, precision=exact_mode) * within,
        0.0,
    )
    inverse = nilpotent_inverse(mixing)
    writes = jnp.einsum(
        "...ij,...je->...ie", inverse, values * strength[..., None], precision=exact_mode
    )
    erases = jnp.einsum(
        "...ij,...jd->...id", inverse, scaled * jnp.exp(running)[..., None], precision=exact_mode
    )
    final_log = running[..., -1]
    carried = unit_keys * jnp.exp(final_log[..., None] - running)[..., None]
    return (writes, erases, carried, final_log)


def split_blocks(array, block_count):
    shaped = array.reshape(
        array.shape[:2] + (block_count, array.shape[2] // block_count) + array.shape[3:]
    )
    return jnp.moveaxis(shaped, 2, 0)


def local_general(
    tokens,
    key_matrix,
    value_matrix,
    gate_matrix,
    head_decay_rate,
    extra_log_decay,
    next_token_query,
    next_token_key,
    next_token_value,
    next_write_strength,
    read_norm_gain,
):
    sequences, positions, _ = tokens.shape
    local_heads = head_decay_rate.shape[0]
    key_width = key_matrix.shape[1] // local_heads
    value_width = value_matrix.shape[1] // local_heads
    all_heads = gate_matrix.shape[1] // 2
    group_size = lax.axis_size("sp")
    column_share = value_width // group_size
    first_head = lax.axis_index("tp") * local_heads
    decay_cols = lax.dynamic_slice_in_dim(gate_matrix, first_head, local_heads, 1)
    strength_cols = lax.dynamic_slice_in_dim(gate_matrix, all_heads + first_head, local_heads, 1)
    gate_cols = jnp.concatenate([decay_cols, strength_cols], axis=1)
    row_count = sequences * positions
    incoming = lax.all_gather(tokens, "tp", axis=2, tiled=True)
    span_width = incoming.shape[2]
    flat_rows = incoming.reshape(row_count, span_width)
    products = lax.optimization_barrier(
        (
            jnp.dot(flat_rows, key_matrix, preferred_element_type=jnp.float32),
            jnp.dot(flat_rows, value_matrix, preferred_element_type=jnp.float32),
            jnp.dot(flat_rows, gate_cols, preferred_element_type=jnp.float32),
        )
    )
    key_sum = products[0]
    value_sum = products[1]
    gate_pre = products[2]
    key_float = lax.optimization_barrier(key_sum.astype(jnp.bfloat16)).astype(jnp.float32)
    value_float = lax.optimization_barrier(value_sum.astype(jnp.bfloat16)).astype(jnp.float32)
    unit_keys = unit_rows(
        key_float.reshape(sequences, positions, local_heads, key_width).transpose(0, 2, 1, 3)
    )
    values = value_float.reshape(sequences, positions, local_heads, value_width).transpose(
        0, 2, 1, 3
    )
    gate_projected = gate_pre.reshape(sequences, positions, 2 * local_heads).transpose(0, 2, 1)
    decay_logarithm = (
        -head_decay_rate[None, :, None] * jax.nn.softplus(gate_projected[:, :local_heads])
        + extra_log_decay
    )
    strength = jax.nn.sigmoid(gate_projected[:, local_heads:] - strength_offset)
    block_count = positions // min(64, positions)
    block_parts = block_terms(
        split_blocks(unit_keys, block_count),
        split_blocks(values, block_count),
        split_blocks(decay_logarithm, block_count),
        split_blocks(strength, block_count),
    )
    identity = jnp.zeros((sequences, local_heads, key_width, key_width), jnp.float32) + jnp.eye(
        key_width, dtype=jnp.float32
    )
    start_map = jnp.concatenate(
        [identity, jnp.zeros((sequences, local_heads, key_width, value_width), jnp.float32)],
        axis=-1,
    )

    def advance(current, block_part):
        writes, erases, carried, final_log = block_part
        padded = jnp.concatenate(
            [jnp.zeros(writes.shape[:-1] + (key_width,), jnp.float32), writes], axis=-1
        )
        removed = lax.optimization_barrier(
            jnp.einsum("shcd,shde->shce", erases, current, precision=exact_mode)
        )
        fresh = padded - removed
        added = lax.optimization_barrier(
            jnp.einsum("shcd,shce->shde", carried, fresh, precision=exact_mode)
        )
        current = current * jnp.exp(final_log)[..., None, None] + added
        return (current, None)

    local_map, _ = lax.scan(advance, start_map, block_parts)
    carry_map = local_map[..., :key_width]
    write_map = local_map[..., key_width:]
    carry_copies = jnp.broadcast_to(carry_map[None], (group_size,) + carry_map.shape)
    write_parts = jnp.moveaxis(
        write_map.reshape(sequences, local_heads, key_width, group_size, column_share), 3, 0
    )
    carries = lax.all_to_all(carry_copies, "sp", split_axis=0, concat_axis=0, tiled=True)
    write_cols = lax.all_to_all(write_parts, "sp", split_axis=0, concat_axis=0, tiled=True)

    def fold_step(current, block_map):
        moved = lax.optimization_barrier(
            jnp.einsum("shij,shje->shie", block_map[0], current, precision=exact_mode)
        )
        return (moved + block_map[1], None)

    begin_state = jnp.zeros(write_cols.shape[1:], jnp.float32)
    folded, _ = lax.scan(fold_step, begin_state, (carries, write_cols))
    query_rows = next_token_query.astype(jnp.float32).reshape(sequences, local_heads, key_width)
    unit_new = unit_rows(
        next_token_key.astype(jnp.float32).reshape(sequences, local_heads, key_width)
    )
    value_rows = next_token_value.astype(jnp.float32)
    key_read = jnp.einsum("shd,shde->she", unit_new, folded, precision=exact_mode)
    query_read = jnp.einsum("shd,shde->she", query_rows, folded, precision=exact_mode)
    intersection = jnp.sum(query_rows * unit_new, axis=-1)
    read_raw = query_read + (next_write_strength * intersection)[..., None] * (
        value_rows - key_read
    )
    square_total = lax.psum(jnp.sum(read_raw * read_raw, axis=-1, keepdims=True), "sp")
    first_read = read_raw * lax.rsqrt(square_total / DV + 1e-06) * read_norm_gain
    return (folded.astype(jnp.bfloat16), first_read.astype(jnp.bfloat16))


def short_dot(left, right, contract=((1,), (0,))):
    return lax.dot_general(
        left.astype(jnp.bfloat16),
        right.astype(jnp.bfloat16),
        (contract, ((), ())),
        preferred_element_type=jnp.float32,
    )


def three_terms(x):
    first = x.astype(jnp.bfloat16)
    rest = x - first.astype(jnp.float32)
    second = rest.astype(jnp.bfloat16)
    third = (rest - second.astype(jnp.float32)).astype(jnp.bfloat16)
    return first, second, third


def softplus(x):
    return jnp.maximum(x, 0.0) + jnp.log1p(jnp.exp(-jnp.abs(x)))


def grid_mask(rows, cols, rule):
    row = lax.broadcasted_iota(jnp.int32, (rows, cols), 0)
    col = lax.broadcasted_iota(jnp.int32, (rows, cols), 1)
    return rule(row, col)


def compose(late, early):
    late_map, late_write, late_keep = late
    early_map, early_write, early_keep = early
    width = early_map.shape[1]
    moved = short_dot(late_map, jnp.concatenate([early_map, early_write], axis=1))
    return (
        late_keep * early_map + early_keep * late_map - moved[:, :width],
        late_keep * early_write + late_write - moved[:, width:],
        late_keep * early_keep,
    )


def compose_write(late, early_write):
    late_map, late_write, late_keep = late
    return late_keep * early_write + late_write - short_dot(late_map, early_write)


def fused_kernel(
    sp_size,
    tp_size,
    rate_hbm,
    next_strength_hbm,
    tokens_ref,
    key_ref,
    value_ref,
    gate_hbm,
    extra_hbm,
    query_hbm,
    new_key_hbm,
    new_value_hbm,
    gain_hbm,
    state_ref,
    read_ref,
    rate_ref,
    next_strength_ref,
    gathered,
    key_w,
    value_w,
    gate_ref,
    gate_own,
    extra_ref,
    query_ref,
    new_key_ref,
    new_value_ref,
    gain_ref,
    key_acc,
    value_acc,
    gate_acc,
    key_out,
    key_in,
    value_out,
    value_in,
    side_out,
    side_in,
    state_out,
    row_out,
    row_in,
    load_sem,
    weight_sem,
    gather_recv,
    gather_send,
    swap_recv,
    swap_send,
    last_recv,
    last_send,
    above_sem,
    peers_sem,
):
    sequences, positions, depth = tokens_ref.shape
    local_heads = extra_ref.shape[1]
    key_width = key_acc.shape[1] // local_heads
    value_width = value_acc.shape[1] // local_heads
    share = value_width // sp_size
    all_heads = gate_ref.shape[0] // 2
    chips = tp_size // CORES
    me = lax.axis_index("sp")
    spot = lax.axis_index("tp")
    chip = spot // CORES
    core = spot % CORES
    partner = chip * CORES + (1 - core)
    half = positions // 2
    units = [(s, part * half, half) for s in range(sequences) for part in range(2)]
    last_unit = len(units) - 1
    batches = [(0, 0, positions, (0, 1)), (1, 0, half, (2,)), (1, half, half, (3,))]
    others = [sp_size - 1 - me, me + 1 - 2 * (me % 2), (me + 2) % sp_size]

    loads = [
        pltpu.make_async_copy(tokens_ref.at[s], gathered.at[spot, s], load_sem.at[s])
        for s in range(sequences)
    ]
    for load in loads:
        load.start()

    barrier = pltpu.get_barrier_semaphore()
    pl.semaphore_signal(barrier, inc=1, device_id={"tp": partner}, device_id_type=MESH)

    @pl.when(chip < chips - 1)
    def _():
        pl.semaphore_signal(barrier, inc=1, device_id={"tp": spot + CORES}, device_id_type=MESH)

    for other in range(1, sp_size):

        @pl.when(me < other)
        def _(other=other):
            pl.semaphore_signal(barrier, inc=1, device_id={"sp": other}, device_id_type=MESH)

    weights = [
        pltpu.make_async_copy(key_ref, key_w, weight_sem.at[0]),
        pltpu.make_async_copy(value_ref, value_w, weight_sem.at[1]),
        pltpu.make_async_copy(gate_hbm, gate_ref, weight_sem.at[2]),
        pltpu.make_async_copy(extra_hbm, extra_ref, weight_sem.at[3]),
        pltpu.make_async_copy(query_hbm, query_ref, weight_sem.at[4]),
        pltpu.make_async_copy(new_key_hbm, new_key_ref, weight_sem.at[5]),
        pltpu.make_async_copy(new_value_hbm, new_value_ref, weight_sem.at[6]),
        pltpu.make_async_copy(gain_hbm, gain_ref, weight_sem.at[7]),
        pltpu.make_async_copy(rate_hbm, rate_ref, weight_sem.at[8]),
        pltpu.make_async_copy(next_strength_hbm, next_strength_ref, weight_sem.at[9]),
    ]
    for weight in weights:
        weight.start()
    pl.semaphore_wait(barrier, jnp.where(chip > 0, 1, 0) + 1 + me)

    @pl.when(chip > 0)
    def _():
        pl.semaphore_signal(above_sem, inc=1, device_id={"tp": spot - CORES}, device_id_type=MESH)

    for other in range(sp_size - 1):

        @pl.when(other < me)
        def _(other=other):
            pl.semaphore_signal(peers_sem, inc=1, device_id={"sp": other}, device_id_type=MESH)

    def piece(origin, u, way, target):
        s, low, count = units[u]
        block = gathered.at[origin, s, pl.ds(low, count)]
        return pltpu.make_async_remote_copy(
            src_ref=block,
            dst_ref=block,
            send_sem=gather_send.at[origin, u, way],
            recv_sem=gather_recv.at[origin, u],
            device_id={"tp": target},
            device_id_type=MESH,
        )

    for load in loads:
        load.wait()

    def hub(a_chip):
        return jnp.where((a_chip == 0) | (a_chip == chips - 1), 0, 1)

    for u in range(last_unit):

        @pl.when(chip > 0)
        def _(u=u):
            piece(spot, u, 1, spot - CORES).start()

    for u in [last_unit, *range(last_unit)]:
        piece(spot, u, 2, partner).start()

    @pl.when(chip < chips - 1)
    def _():
        pl.semaphore_wait(above_sem, 1)

    for u in range(last_unit):

        @pl.when(chip < chips - 1)
        def _(u=u):
            piece(spot, u, 0, spot + CORES).start()

    def send_last(way):
        onward = chip + (1 if way == 0 else -1)
        for c in range(CORES):
            piece(chip * CORES + c, last_unit, way, onward * CORES + hub(onward)).start()

    @pl.when(core == 1)
    def _():
        piece(partner, last_unit, 2, partner).wait_recv()

        @pl.when(chip == chips - 1)
        def _():
            send_last(1)

        @pl.when(chip == 0)
        def _():
            send_last(0)

    key_acc[...] = jnp.zeros_like(key_acc)
    value_acc[...] = jnp.zeros_like(value_acc)
    gate_acc[...] = jnp.zeros_like(gate_acc)
    side_out[...] = jnp.zeros_like(side_out)

    def add_in(rows, span, batch):
        s, low, count, parts = batches[batch]
        cut = slice(s * positions + low, s * positions + low + count)
        key_acc[cut] += jnp.dot(rows, key_w[span, :], preferred_element_type=jnp.float32)
        value_acc[cut] += jnp.dot(rows, value_w[span, :], preferred_element_type=jnp.float32)
        gates = lax.dot_general(
            gate_own[:, span],
            rows,
            (((1,), (1,)), ((), ())),
            preferred_element_type=jnp.float32,
        )
        gate_acc[s, :, low : low + count] += gates

    def take_one(block, batch):
        s, low, count, _ = batches[batch]
        span = pl.ds(pl.multiple_of(block * depth, depth), depth)
        add_in(gathered[block, s, low : low + count], span, batch)

    def take_chip(origin_chip, batch):
        s, low, count, _ = batches[batch]
        width = CORES * depth
        span = pl.ds(pl.multiple_of(origin_chip * width, width), width)
        rows = jnp.concatenate(
            [gathered[origin_chip * CORES + c, s, low : low + count] for c in range(CORES)], axis=1
        )
        add_in(rows, span, batch)

    first = spot * local_heads

    def prepare():
        for weight in weights:
            weight.wait()
        chooser = grid_mask(
            2 * local_heads,
            2 * all_heads,
            lambda r, c: c
            == jnp.where(r < local_heads, first + r, all_heads + first + r - local_heads),
        ).astype(jnp.float32)
        gate_own[...] = short_dot(chooser, gate_ref[...]).astype(jnp.bfloat16)
        placer = grid_mask(share, value_width, lambda r, c: c == me * share + r)
        for s in range(sequences):
            new_value = short_dot(new_value_ref[s], placer.astype(jnp.float32))
            for h in range(local_heads):
                side_out[h, s, 2:3, :] = new_value[h : h + 1, :]

    def own(batch):
        for u in batches[batch][3]:
            if u == last_unit:

                @pl.when(core == 0)
                def _(u=u):
                    piece(partner, u, 2, partner).wait_recv()

            else:
                piece(partner, u, 2, partner).wait_recv()
        take_chip(chip, batch)

    def relay(distance, u):
        lanes = range(CORES) if u == last_unit else [core]
        for lane in lanes:
            relay_lane(distance, u, lane)

    def relay_lane(distance, u, lane):
        for way, step in ((1, 1), (0, -1)):
            origin_chip = chip + step * distance
            origin = origin_chip * CORES + lane
            present = (origin_chip >= 0) & (origin_chip < chips)
            if u == last_unit:
                present = present & (core == hub(chip))
            onward = chip - step
            beyond = (onward >= 0) & (onward < chips)
            target = onward * CORES + (hub(onward) if u == last_unit else core)

            @pl.when(present)
            def _(way=way, origin_chip=origin_chip, origin=origin, target=target, beyond=beyond):
                piece(origin, u, way, partner).wait_recv()

                @pl.when(beyond)
                def _():
                    piece(origin, u, way, target).start()

                piece(origin, u, 2, partner).start()
                if u == 1:

                    @pl.when(
                        beyond & (core == 1) & (origin_chip == (0 if way == 0 else chips - 1))
                    )
                    def _():
                        send_last(way)

    def both_sides(distance, act):
        def one_side(side, carry):
            origin_chip = chip + (2 * side - 1) * distance

            @pl.when((origin_chip >= 0) & (origin_chip < chips))
            def _():
                act(origin_chip)

            return carry

        lax.fori_loop(0, 2, one_side, 0)

    def absorb(distance, batch):
        def act(origin_chip):
            for u in batches[batch][3]:
                if u == last_unit:

                    @pl.when(core != hub(chip))
                    def _(u=u):
                        for c in range(CORES):
                            piece(origin_chip * CORES + c, u, 2, partner).wait_recv()

                else:
                    piece(origin_chip * CORES + 1 - core, u, 2, partner).wait_recv()
            take_chip(origin_chip, batch)

        both_sides(distance, act)

    def absorb_last_lane(distance, lane):
        relay_lane(distance, last_unit, lane)

        def act(origin_chip):
            block = origin_chip * CORES + lane

            @pl.when(core != hub(chip))
            def _():
                piece(block, last_unit, 2, partner).wait_recv()

            take_one(block, len(batches) - 1)

        both_sides(distance, act)

    def swap(n, slot, target, origin):
        s, low, count, _ = batches[slot]
        if n == 0:
            source, sink = side_out.at[target, slot], side_in.at[origin, slot]
        else:
            source, sink = ((key_out, key_in), (value_out, value_in))[n - 1]
            source = source.at[target, s, pl.ds(low, count)]
            sink = sink.at[origin, s, pl.ds(low, count)]
        return pltpu.make_async_remote_copy(
            src_ref=source,
            dst_ref=sink,
            send_sem=swap_send.at[n, slot, target],
            recv_sem=swap_recv.at[n, slot, origin],
            device_id={"sp": target},
            device_id_type=MESH,
        )

    def hand_out(slot):
        s, low, count, _ = batches[slot]
        cut = slice(s * positions + low, s * positions + low + count)
        gates = gate_acc[s, :, low : low + count]
        extra = extra_ref[s, :, low : low + count]
        for h in range(local_heads):
            side_out[h, slot, 0:1, low : low + count] = (
                -rate_ref[h] * softplus(gates[h : h + 1]) + extra[h : h + 1, :]
            )
            side_out[h, slot, 1:2, low : low + count] = jax.nn.sigmoid(
                gates[local_heads + h : local_heads + h + 1] - strength_offset
            )
        for other in others:
            swap(0, slot, other, me).start()
        for h in range(local_heads):
            key_out[h, s, low : low + count] = key_acc[
                cut, h * key_width : (h + 1) * key_width
            ].astype(jnp.bfloat16)
        for other in others:
            swap(1, slot, other, me).start()
        for h in range(local_heads):
            value_out[h, s, low : low + count] = value_acc[
                cut, h * value_width : (h + 1) * value_width
            ].astype(jnp.bfloat16)
        for other in others:
            swap(2, slot, other, me).start()
        side_in[me, slot] = side_out[me, slot]
        key_in[me, s, low : low + count] = key_out[me, s, low : low + count]
        value_in[me, s, low : low + count] = value_out[me, s, low : low + count]

    far = chips - 1
    last_batch = len(batches) - 1
    steps = {1: [(1, 0), (1, 1), (1, 2)]} if far > 1 else {}
    for distance in range(2, far):
        steps[distance] = [(distance, 0), (distance, 1), (distance, 2)]
    work = [(own, (0,)), (own, (1,)), (own, (2,))]
    prepared = False
    for distance in range(1, far):
        for event in steps[distance]:
            relay(*event)
            if not prepared:
                prepare()
                prepared = True
            if work:
                act, operands = work.pop(0)
                act(*operands)
            if event[1] == 1:
                work.insert(0, (absorb, (distance, 0)))
            if event[1] == 2:
                work.append((absorb, (distance, 1)))
    if not prepared:
        prepare()
    for act, operands in [w for w in work if w[0] is own]:
        act(*operands)
    work = [w for w in work if w[0] is absorb]
    relay(far, 0)
    for act, operands in [w for w in work if w[1][1] == 0]:
        act(*operands)
    work = [w for w in work if w[1][1] != 0]
    relay(far, 1)
    absorb(far, 0)

    @pl.when(me < sp_size - 1)
    def _():
        pl.semaphore_wait(peers_sem, sp_size - 1 - me)

    hand_out(0)
    if far > 1:
        relay(1, last_unit)
    for act, operands in work:
        act(*operands)
    relay(far, 2)
    if far > 1:
        absorb(1, last_batch)
    absorb(far, 1)
    hand_out(1)
    pending = None
    for distance in range(2, far):
        relay(distance, last_unit)
        if pending is not None:
            absorb(*pending)
        pending = (distance, last_batch)
    if pending is not None:
        absorb(*pending)
    for lane in range(CORES):
        absorb_last_lane(far, lane)
    hand_out(2)

    def settle(u, lane):
        last = u == last_unit
        for distance in range(chips):
            for way, step in ((0, -1), (1, 1)):
                origin_chip = chip + step * distance
                origin = origin_chip * CORES + lane
                onward = chip - step
                present = (origin_chip >= 0) & (origin_chip < chips)
                sends = present & (onward >= 0) & (onward < chips)

                if distance or (way == 0 and not last):

                    @pl.when(present & (core == hub(chip)) if last else present)
                    def _(origin=origin):
                        piece(origin, u, 2, partner).wait_send()

                @pl.when(sends & (core == 1) if last else sends)
                def _(origin=origin, way=way, onward=onward):
                    piece(origin, u, way, onward * CORES + core).wait_send()

    for u in range(last_unit):
        settle(u, core)
    piece(spot, last_unit, 2, partner).wait_send()
    for lane in range(CORES):
        settle(last_unit, lane)

    side_rows = side_in.shape[2]
    upto = grid_mask(positions, positions, lambda r, c: r <= c).astype(jnp.float32)
    down = jnp.concatenate(
        [
            grid_mask(positions, positions, lambda r, c: c <= r).astype(jnp.float32),
            grid_mask(positions, positions, lambda r, c: c == r).astype(jnp.float32),
        ],
        axis=0,
    )
    lanes = pl.ds(pl.multiple_of(me * key_width, key_width), key_width)
    queries = query_ref[:, lanes].astype(jnp.float32)
    new_keys = new_key_ref[:, lanes].astype(jnp.float32)
    new_keys = new_keys * lax.rsqrt(jnp.sum(new_keys * new_keys, axis=-1, keepdims=True) + 1e-06)
    meets = jnp.sum(queries * new_keys, axis=-1, keepdims=True)

    def block_maps(s, slots):
        count = positions
        eye = grid_mask(count, count, lambda r, c: r == c).astype(jnp.float32)
        lower = grid_mask(count, count, lambda r, c: r >= c)
        strict = grid_mask(count, count, lambda r, c: r > c)
        for slot in slots:
            for other in others:
                swap(0, slot, other, other).wait_recv()
        for slot in slots:
            for other in others:
                swap(1, slot, other, other).wait_recv()
        side = three_terms(
            sum(side_in[:, slot].reshape(sp_size * side_rows, positions) for slot in slots)
        )
        running_row = sum(short_dot(term, upto) for term in side)
        columns = sum(short_dot(down, term, ((1,), (1,))) for term in side)
        parts = []
        for b in range(sp_size):
            line = b * side_rows
            row = running_row[line : line + 1, :]
            col = columns[:positions, line : line + 1]
            strength = columns[positions:, line + 1 : line + 2]
            final_log = row[:, count - 1 : count]
            keys = key_in[b, s].astype(jnp.float32)
            keys = keys * lax.rsqrt(jnp.sum(keys * keys, axis=-1, keepdims=True) + 1e-06)
            within = jnp.where(lower, jnp.exp(jnp.where(lower, col - row, 0.0)), 0.0)
            scaled = keys * strength
            power = jnp.where(strict, -short_dot(scaled, keys, ((1,), (1,))) * within, 0.0)
            erased = scaled * jnp.exp(col)
            carried = (keys * jnp.exp(final_log - col)).T.astype(jnp.bfloat16)
            parts.append([eye + power, power, strength, erased, carried, jnp.exp(final_log)])
        for part in parts:
            part[1] = short_dot(part[1], part[1])
        covered = 2
        while covered < count:
            for part in parts:
                if covered * 2 < count:
                    both = short_dot(part[1], jnp.concatenate([part[0], part[1]], axis=1))
                    part[0] = part[0] + both[:, :count]
                    part[1] = both[:, count:]
                else:
                    part[0] = part[0] + short_dot(part[1], part[0])
            covered = covered * 2
        for slot in slots:
            for other in others:
                swap(2, slot, other, other).wait_recv()
        solved = []
        for b, part in enumerate(parts):
            values = value_in[b, s].astype(jnp.float32) * part[2]
            solved.append(short_dot(part[0], jnp.concatenate([part[3], values], axis=1)))
        maps = []
        for part, both in zip(parts, solved):
            both = short_dot(part[4], both)
            maps.append((both[:, :key_width], both[:, key_width:], part[5]))
        return maps

    def final(n, s, target, origin):
        source, sink = (
            (state_out.at[target, s], state_ref.at[s, origin]),
            (row_out.at[target, s], row_in.at[origin, s]),
        )[n]
        return pltpu.make_async_remote_copy(
            src_ref=source,
            dst_ref=sink,
            send_sem=last_send.at[n, s, target],
            recv_sem=last_recv.at[n, s, origin],
            device_id={"sp": target},
            device_id_type=MESH,
        )

    def finish(s, maps):
        while len(maps) > 2:
            maps = [compose(maps[i + 1], maps[i]) for i in range(0, len(maps), 2)]
        state = compose_write(maps[1], maps[0][1])
        wide = (8, key_width)
        first_row = grid_mask(*wide, lambda r, c: r == 0)
        probes = jnp.where(
            first_row,
            jnp.broadcast_to(queries[s : s + 1], wide),
            jnp.broadcast_to(new_keys[s : s + 1], wide),
        )
        probe_terms, state_terms = three_terms(probes)[:2], three_terms(state)[:2]
        reads = (
            short_dot(probe_terms[0], state_terms[0])
            + short_dot(probe_terms[0], state_terms[1])
            + short_dot(probe_terms[1], state_terms[0])
        )
        turned = state.T.astype(jnp.bfloat16)
        for j in range(sp_size):
            state_out[j, s] = turned[j * share : (j + 1) * share, :]
        for other in others:
            final(0, s, other, me).start()
        query_read, key_read = reads[0:1], reads[1:2]
        new_value = jnp.sum(side_in[:, s, 2, :], axis=0, keepdims=True)
        raw = query_read + (next_strength_ref[s, me] * meets[s : s + 1]) * (new_value - key_read)
        raw = raw * lax.rsqrt(jnp.sum(raw * raw, axis=-1, keepdims=True) / value_width + 1e-06)
        for j in range(sp_size):
            turn = j * share
            row_out[j, s, 0:1, :] = (
                jnp.concatenate([raw[:, turn:], raw[:, :turn]], axis=1) if j else raw
            )
        for other in others:
            final(1, s, other, me).start()
        state_ref[s, me] = state_out[me, s]
        row_in[me, s] = row_out[me, s]

    row_out[...] = jnp.zeros_like(row_out)
    finish(0, block_maps(0, (0,)))
    finish(1, block_maps(1, (1, 2)))

    for slot in range(len(batches)):
        for n in range(3):
            for other in others:
                swap(n, slot, other, me).wait_send()
    for s in range(sequences):
        for n in range(2):
            for other in others:
                final(n, s, other, me).wait_send()
    for s in range(sequences):
        for other in others:
            final(1, s, other, other).wait_recv()
        rows = jnp.concatenate([row_in[i, s, 0:1, :share] for i in range(sp_size)], axis=0)
        read_ref[s] = (rows * gain_ref[...].reshape(1, share)).astype(jnp.bfloat16)
    for s in range(sequences):
        for other in others:
            final(0, s, other, other).wait_recv()


def place_kernel(state_ref, read_ref, state_hbm, read_hbm, sem):
    copies = [
        pltpu.make_async_copy(state_ref, state_hbm, sem.at[0]),
        pltpu.make_async_copy(read_ref, read_hbm, sem.at[1]),
    ]
    for copy in copies:
        copy.start()
    for copy in copies:
        copy.wait()


def local_fused(
    tokens,
    key_matrix,
    value_matrix,
    gate_matrix,
    head_decay_rate,
    extra_log_decay,
    next_token_query,
    next_token_key,
    next_token_value,
    next_write_strength,
    read_norm_gain,
):
    sequences, positions, depth = tokens.shape
    local_heads = head_decay_rate.shape[0]
    sp_size = lax.axis_size("sp")
    tp_size = lax.axis_size("tp")
    key_total = key_matrix.shape[1]
    value_total = value_matrix.shape[1]
    key_width = key_total // local_heads
    value_width = value_total // local_heads
    share = value_width // sp_size
    rows = sequences * positions
    units = 2 * sequences
    slots = sequences + 1
    vmem = pl.BlockSpec(memory_space=pltpu.VMEM)
    anywhere = pl.BlockSpec(memory_space=pl.ANY)
    dma = pltpu.SemaphoreType.DMA
    held = (sp_size, sequences, positions)
    turned, read = pl.pallas_call(
        functools.partial(fused_kernel, sp_size, tp_size),
        out_shape=(
            pltpu.VMEM((sequences, local_heads, share, key_width), jnp.bfloat16),
            pltpu.VMEM((sequences, local_heads, share), jnp.bfloat16),
        ),
        in_specs=[anywhere] * 11,
        out_specs=(vmem, vmem),
        scratch_shapes=[
            pltpu.SMEM(head_decay_rate.shape, jnp.float32),
            pltpu.SMEM(next_write_strength.shape, jnp.float32),
            pltpu.VMEM((tp_size, sequences, positions, depth), jnp.bfloat16),
            pltpu.VMEM(key_matrix.shape, jnp.bfloat16),
            pltpu.VMEM(value_matrix.shape, jnp.bfloat16),
            pltpu.VMEM(gate_matrix.shape[::-1], jnp.bfloat16),
            pltpu.VMEM((2 * local_heads, gate_matrix.shape[0]), jnp.bfloat16),
            pltpu.VMEM(extra_log_decay.shape, jnp.float32),
            pltpu.VMEM(next_token_query.shape, jnp.bfloat16),
            pltpu.VMEM(next_token_key.shape, jnp.bfloat16),
            pltpu.VMEM(next_token_value.shape, jnp.bfloat16),
            pltpu.VMEM(read_norm_gain.shape, jnp.float32),
            pltpu.VMEM((rows, key_total), jnp.float32),
            pltpu.VMEM((rows, value_total), jnp.float32),
            pltpu.VMEM((sequences, 2 * local_heads, positions), jnp.float32),
            pltpu.VMEM((*held, key_width), jnp.bfloat16),
            pltpu.VMEM((*held, key_width), jnp.bfloat16),
            pltpu.VMEM((*held, value_width), jnp.bfloat16),
            pltpu.VMEM((*held, value_width), jnp.bfloat16),
            pltpu.VMEM((sp_size, slots, 8, positions), jnp.float32),
            pltpu.VMEM((sp_size, slots, 8, positions), jnp.float32),
            pltpu.VMEM((sp_size, sequences, share, key_width), jnp.bfloat16),
            pltpu.VMEM((sp_size, sequences, 8, value_width), jnp.float32),
            pltpu.VMEM((sp_size, sequences, 8, value_width), jnp.float32),
            dma((sequences,)),
            dma((10,)),
            dma((tp_size, units)),
            dma((tp_size, units, 3)),
            dma((3, slots, sp_size)),
            dma((3, slots, sp_size)),
            dma((2, sequences, sp_size)),
            dma((2, sequences, sp_size)),
            pltpu.SemaphoreType.REGULAR,
            pltpu.SemaphoreType.REGULAR,
        ],
        compiler_params=pltpu.CompilerParams(
            collective_id=0, has_side_effects=True
        ),
    )(
        head_decay_rate,
        next_write_strength,
        tokens,
        key_matrix,
        value_matrix,
        gate_matrix.T,
        extra_log_decay,
        next_token_query,
        next_token_key,
        next_token_value,
        read_norm_gain,
    )
    turned, read = pl.pallas_call(
        place_kernel,
        out_shape=tuple(jax.ShapeDtypeStruct(a.shape, a.dtype) for a in (turned, read)),
        in_specs=[vmem, vmem],
        out_specs=(anywhere, anywhere),
        scratch_shapes=[dma((2,))],
    )(*(pltpu.with_memory_space_constraint(a, pltpu.VMEM) for a in (turned, read)))
    return jnp.swapaxes(turned, 2, 3), read


def local(*arguments):
    tokens, key_matrix, value_matrix = arguments[:3]
    sequences, positions, _ = tokens.shape
    local_heads = arguments[4].shape[0]
    sp_size = lax.axis_size("sp")
    fits = (
        local_heads == sp_size
        and sp_size == 4
        and sequences == 2
        and 2 * local_heads == 8
        and lax.axis_size("tp") % CORES == 0
        and lax.axis_size("tp") > CORES
        and positions == key_matrix.shape[1] // local_heads
        and positions == value_matrix.shape[1] // local_heads
        and positions % 128 == 0
    )
    return local_fused(*arguments) if fits else local_general(*arguments)


def solution(mesh):
    in_specs = (
        P(None, "sp", "tp"),
        P(None, "tp"),
        P(None, "tp"),
        P(),
        P("tp"),
        P(None, "tp", "sp"),
        P(None, "tp"),
        P(None, "tp"),
        P(None, "tp", "sp"),
        P(None, "tp"),
        P("sp"),
    )
    out_specs = (P(None, "tp", None, "sp"), P(None, "tp", "sp"))
    return jax.shard_map(local, mesh=mesh, in_specs=in_specs, out_specs=out_specs, check_vma=False)
```

```python
import functools

import jax
import jax.numpy as jnp
from jax import lax
from jax.experimental import pallas as pl
from jax.experimental.pallas import tpu as pltpu
from jax.sharding import PartitionSpec as P

DV = 128
CORES = 2
MESH = pl.DeviceIdType.MESH


exact_mode = lax.Precision.HIGHEST
strength_offset = 5.0


def unit_rows(matrix):
    return matrix * lax.rsqrt(jnp.sum(matrix * matrix, axis=-1, keepdims=True) + 1e-06)


def nilpotent_inverse(mixing):
    extent = mixing.shape[-1]
    result = jnp.zeros_like(mixing) + jnp.eye(extent, dtype=jnp.float32)
    powered = -mixing
    covered = 1
    while covered < extent:
        product = lax.optimization_barrier(
            jnp.einsum("...ij,...jk->...ik", result, powered, precision=exact_mode)
        )
        result = result + product
        powered = jnp.einsum("...ij,...jk->...ik", powered, powered, precision=exact_mode)
        covered = covered * 2
    return result


def block_terms(unit_keys, values, decay_logarithm, strength):
    extent = unit_keys.shape[-2]
    lower = jnp.tril(jnp.ones((extent, extent), jnp.bool_))
    strict = jnp.tril(jnp.ones((extent, extent), jnp.bool_), -1)
    running = jnp.cumsum(decay_logarithm, axis=-1)
    spread = running[..., :, None] - running[..., None, :]
    within = jnp.where(lower, jnp.exp(jnp.where(lower, spread, 0.0)), 0.0)
    scaled = unit_keys * strength[..., None]
    mixing = jnp.where(
        strict,
        jnp.einsum("...id,...jd->...ij", scaled, unit_keys, precision=exact_mode) * within,
        0.0,
    )
    inverse = nilpotent_inverse(mixing)
    writes = jnp.einsum(
        "...ij,...je->...ie", inverse, values * strength[..., None], precision=exact_mode
    )
    erases = jnp.einsum(
        "...ij,...jd->...id", inverse, scaled * jnp.exp(running)[..., None], precision=exact_mode
    )
    final_log = running[..., -1]
    carried = unit_keys * jnp.exp(final_log[..., None] - running)[..., None]
    return (writes, erases, carried, final_log)


def split_blocks(array, block_count):
    shaped = array.reshape(
        array.shape[:2] + (block_count, array.shape[2] // block_count) + array.shape[3:]
    )
    return jnp.moveaxis(shaped, 2, 0)


def local_general(
    tokens,
    key_matrix,
    value_matrix,
    gate_matrix,
    head_decay_rate,
    extra_log_decay,
    next_token_query,
    next_token_key,
    next_token_value,
    next_write_strength,
    read_norm_gain,
):
    sequences, positions, _ = tokens.shape
    local_heads = head_decay_rate.shape[0]
    key_width = key_matrix.shape[1] // local_heads
    value_width = value_matrix.shape[1] // local_heads
    all_heads = gate_matrix.shape[1] // 2
    group_size = lax.axis_size("sp")
    column_share = value_width // group_size
    first_head = lax.axis_index("tp") * local_heads
    decay_cols = lax.dynamic_slice_in_dim(gate_matrix, first_head, local_heads, 1)
    strength_cols = lax.dynamic_slice_in_dim(gate_matrix, all_heads + first_head, local_heads, 1)
    gate_cols = jnp.concatenate([decay_cols, strength_cols], axis=1)
    row_count = sequences * positions
    incoming = lax.all_gather(tokens, "tp", axis=2, tiled=True)
    span_width = incoming.shape[2]
    flat_rows = incoming.reshape(row_count, span_width)
    products = lax.optimization_barrier(
        (
            jnp.dot(flat_rows, key_matrix, preferred_element_type=jnp.float32),
            jnp.dot(flat_rows, value_matrix, preferred_element_type=jnp.float32),
            jnp.dot(flat_rows, gate_cols, preferred_element_type=jnp.float32),
        )
    )
    key_sum = products[0]
    value_sum = products[1]
    gate_pre = products[2]
    key_float = lax.optimization_barrier(key_sum.astype(jnp.bfloat16)).astype(jnp.float32)
    value_float = lax.optimization_barrier(value_sum.astype(jnp.bfloat16)).astype(jnp.float32)
    unit_keys = unit_rows(
        key_float.reshape(sequences, positions, local_heads, key_width).transpose(0, 2, 1, 3)
    )
    values = value_float.reshape(sequences, positions, local_heads, value_width).transpose(
        0, 2, 1, 3
    )
    gate_projected = gate_pre.reshape(sequences, positions, 2 * local_heads).transpose(0, 2, 1)
    decay_logarithm = (
        -head_decay_rate[None, :, None] * jax.nn.softplus(gate_projected[:, :local_heads])
        + extra_log_decay
    )
    strength = jax.nn.sigmoid(gate_projected[:, local_heads:] - strength_offset)
    block_count = positions // min(64, positions)
    block_parts = block_terms(
        split_blocks(unit_keys, block_count),
        split_blocks(values, block_count),
        split_blocks(decay_logarithm, block_count),
        split_blocks(strength, block_count),
    )
    identity = jnp.zeros((sequences, local_heads, key_width, key_width), jnp.float32) + jnp.eye(
        key_width, dtype=jnp.float32
    )
    start_map = jnp.concatenate(
        [identity, jnp.zeros((sequences, local_heads, key_width, value_width), jnp.float32)],
        axis=-1,
    )

    def advance(current, block_part):
        writes, erases, carried, final_log = block_part
        padded = jnp.concatenate(
            [jnp.zeros(writes.shape[:-1] + (key_width,), jnp.float32), writes], axis=-1
        )
        removed = lax.optimization_barrier(
            jnp.einsum("shcd,shde->shce", erases, current, precision=exact_mode)
        )
        fresh = padded - removed
        added = lax.optimization_barrier(
            jnp.einsum("shcd,shce->shde", carried, fresh, precision=exact_mode)
        )
        current = current * jnp.exp(final_log)[..., None, None] + added
        return (current, None)

    local_map, _ = lax.scan(advance, start_map, block_parts)
    carry_map = local_map[..., :key_width]
    write_map = local_map[..., key_width:]
    carry_copies = jnp.broadcast_to(carry_map[None], (group_size,) + carry_map.shape)
    write_parts = jnp.moveaxis(
        write_map.reshape(sequences, local_heads, key_width, group_size, column_share), 3, 0
    )
    carries = lax.all_to_all(carry_copies, "sp", split_axis=0, concat_axis=0, tiled=True)
    write_cols = lax.all_to_all(write_parts, "sp", split_axis=0, concat_axis=0, tiled=True)

    def fold_step(current, block_map):
        moved = lax.optimization_barrier(
            jnp.einsum("shij,shje->shie", block_map[0], current, precision=exact_mode)
        )
        return (moved + block_map[1], None)

    begin_state = jnp.zeros(write_cols.shape[1:], jnp.float32)
    folded, _ = lax.scan(fold_step, begin_state, (carries, write_cols))
    query_rows = next_token_query.astype(jnp.float32).reshape(sequences, local_heads, key_width)
    unit_new = unit_rows(
        next_token_key.astype(jnp.float32).reshape(sequences, local_heads, key_width)
    )
    value_rows = next_token_value.astype(jnp.float32)
    key_read = jnp.einsum("shd,shde->she", unit_new, folded, precision=exact_mode)
    query_read = jnp.einsum("shd,shde->she", query_rows, folded, precision=exact_mode)
    intersection = jnp.sum(query_rows * unit_new, axis=-1)
    read_raw = query_read + (next_write_strength * intersection)[..., None] * (
        value_rows - key_read
    )
    square_total = lax.psum(jnp.sum(read_raw * read_raw, axis=-1, keepdims=True), "sp")
    first_read = read_raw * lax.rsqrt(square_total / DV + 1e-06) * read_norm_gain
    return (folded.astype(jnp.bfloat16), first_read.astype(jnp.bfloat16))


def short_dot(left, right, contract=((1,), (0,))):
    return lax.dot_general(
        left.astype(jnp.bfloat16),
        right.astype(jnp.bfloat16),
        (contract, ((), ())),
        preferred_element_type=jnp.float32,
    )


def three_terms(x):
    first = x.astype(jnp.bfloat16)
    rest = x - first.astype(jnp.float32)
    second = rest.astype(jnp.bfloat16)
    third = (rest - second.astype(jnp.float32)).astype(jnp.bfloat16)
    return first, second, third


def softplus(x):
    return jnp.maximum(x, 0.0) + jnp.log1p(jnp.exp(-jnp.abs(x)))


def grid_mask(rows, cols, rule):
    row = lax.broadcasted_iota(jnp.int32, (rows, cols), 0)
    col = lax.broadcasted_iota(jnp.int32, (rows, cols), 1)
    return rule(row, col)


def compose(late, early):
    late_map, late_write, late_keep = late
    early_map, early_write, early_keep = early
    width = early_map.shape[1]
    moved = short_dot(late_map, jnp.concatenate([early_map, early_write], axis=1))
    return (
        late_keep * early_map + early_keep * late_map - moved[:, :width],
        late_keep * early_write + late_write - moved[:, width:],
        late_keep * early_keep,
    )


def compose_write(late, early_write):
    late_map, late_write, late_keep = late
    return late_keep * early_write + late_write - short_dot(late_map, early_write)


def fused_kernel(
    sp_size,
    tp_size,
    rate_hbm,
    next_strength_hbm,
    tokens_ref,
    key_ref,
    value_ref,
    gate_hbm,
    extra_hbm,
    query_hbm,
    new_key_hbm,
    new_value_hbm,
    gain_hbm,
    state_ref,
    read_ref,
    rate_ref,
    next_strength_ref,
    gathered,
    key_w,
    value_w,
    gate_ref,
    gate_own,
    extra_ref,
    query_ref,
    new_key_ref,
    new_value_ref,
    gain_ref,
    key_acc,
    value_acc,
    gate_acc,
    key_out,
    key_in,
    value_out,
    value_in,
    side_out,
    side_in,
    state_out,
    row_out,
    row_in,
    load_sem,
    weight_sem,
    gather_recv,
    gather_send,
    swap_recv,
    swap_send,
    last_recv,
    last_send,
    above_sem,
    peers_sem,
):
    sequences, positions, depth = tokens_ref.shape
    local_heads = extra_ref.shape[1]
    key_width = key_acc.shape[1] // local_heads
    value_width = value_acc.shape[1] // local_heads
    share = value_width // sp_size
    all_heads = gate_ref.shape[0] // 2
    chips = tp_size // CORES
    me = lax.axis_index("sp")
    spot = lax.axis_index("tp")
    chip = spot // CORES
    core = spot % CORES
    partner = chip * CORES + (1 - core)
    half = positions // 2
    units = [(s, part * half, half) for s in range(sequences) for part in range(2)]
    last_unit = len(units) - 1
    batches = [(0, 0, positions, (0, 1)), (1, 0, half, (2,)), (1, half, half, (3,))]
    others = [sp_size - 1 - me, me + 1 - 2 * (me % 2), (me + 2) % sp_size]

    loads = [
        pltpu.make_async_copy(
            tokens_ref.at[s],
            gathered.at[spot, pl.ds(s * positions, positions)],
            load_sem.at[s],
        )
        for s in range(sequences)
    ]
    for load in loads:
        load.start()

    barrier = pltpu.get_barrier_semaphore()
    pl.semaphore_signal(barrier, inc=1, device_id={"tp": partner}, device_id_type=MESH)

    @pl.when(chip < chips - 1)
    def _():
        pl.semaphore_signal(barrier, inc=1, device_id={"tp": spot + CORES}, device_id_type=MESH)

    for other in range(1, sp_size):

        @pl.when(me < other)
        def _(other=other):
            pl.semaphore_signal(barrier, inc=1, device_id={"sp": other}, device_id_type=MESH)

    weights = [
        pltpu.make_async_copy(key_ref, key_w, weight_sem.at[0]),
        pltpu.make_async_copy(value_ref, value_w, weight_sem.at[1]),
        pltpu.make_async_copy(gate_hbm, gate_ref, weight_sem.at[2]),
        pltpu.make_async_copy(extra_hbm, extra_ref, weight_sem.at[3]),
        pltpu.make_async_copy(query_hbm, query_ref, weight_sem.at[4]),
        pltpu.make_async_copy(new_key_hbm, new_key_ref, weight_sem.at[5]),
        pltpu.make_async_copy(new_value_hbm, new_value_ref, weight_sem.at[6]),
        pltpu.make_async_copy(gain_hbm, gain_ref, weight_sem.at[7]),
        pltpu.make_async_copy(rate_hbm, rate_ref, weight_sem.at[8]),
        pltpu.make_async_copy(next_strength_hbm, next_strength_ref, weight_sem.at[9]),
    ]
    for weight in weights:
        weight.start()
    pl.semaphore_wait(barrier, jnp.where(chip > 0, 1, 0) + 1 + me)

    @pl.when(chip > 0)
    def _():
        pl.semaphore_signal(above_sem, inc=1, device_id={"tp": spot - CORES}, device_id_type=MESH)

    for other in range(sp_size - 1):

        @pl.when(other < me)
        def _(other=other):
            pl.semaphore_signal(peers_sem, inc=1, device_id={"sp": other}, device_id_type=MESH)

    def crossing(block, send, recv, axis, target):
        return pltpu.make_async_remote_copy(
            src_ref=block[0],
            dst_ref=block[1],
            send_sem=send,
            recv_sem=recv,
            device_id={axis: target},
            device_id_type=MESH,
        )

    def piece(origin, u, way, target, own=False):
        s, low, count = units[u]
        block = gathered.at[origin, pl.ds(s * positions + low, count)]
        kind = 2 * way + (u == last_unit) + (way == 2 and u == last_unit and own)
        return crossing(
            (block, block), gather_send.at[kind], gather_recv.at[origin, u], "tp", target
        )

    def settle(kind, blocks, count):
        block = gathered.at[pl.ds(0, blocks), pl.ds(0, count)]
        crossing(
            (block, block), gather_send.at[kind], gather_recv.at[0, 0], "tp", partner
        ).wait_send()

    for load in loads:
        load.wait()

    def hub(a_chip):
        return jnp.where((a_chip == 0) | (a_chip == chips - 1), 0, 1)

    for u in range(last_unit):

        @pl.when(chip > 0)
        def _(u=u):
            piece(spot, u, 1, spot - CORES).start()

    for u in [last_unit, *range(last_unit)]:
        piece(spot, u, 2, partner, own=True).start()

    @pl.when(chip < chips - 1)
    def _():
        pl.semaphore_wait(above_sem, 1)

    for u in range(last_unit):

        @pl.when(chip < chips - 1)
        def _(u=u):
            piece(spot, u, 0, spot + CORES).start()

    def send_last(way):
        onward = chip + (1 if way == 0 else -1)
        for c in range(CORES):
            piece(chip * CORES + c, last_unit, way, onward * CORES + hub(onward)).start()

    @pl.when(core == 1)
    def _():
        piece(partner, last_unit, 2, partner).wait_recv()

        @pl.when(chip == chips - 1)
        def _():
            send_last(1)

        @pl.when(chip == 0)
        def _():
            send_last(0)

    key_acc[...] = jnp.zeros_like(key_acc)
    value_acc[...] = jnp.zeros_like(value_acc)
    gate_acc[...] = jnp.zeros_like(gate_acc)
    side_out[...] = jnp.zeros_like(side_out)

    def add_in(rows, span, batch):
        s, low, count, parts = batches[batch]
        cut = slice(s * positions + low, s * positions + low + count)
        key_acc[cut] += jnp.dot(rows, key_w[span, :], preferred_element_type=jnp.float32)
        value_acc[cut] += jnp.dot(rows, value_w[span, :], preferred_element_type=jnp.float32)
        gates = lax.dot_general(
            gate_own[:, span],
            rows,
            (((1,), (1,)), ((), ())),
            preferred_element_type=jnp.float32,
        )
        gate_acc[s, :, low : low + count] += gates

    def take_one(block, batch):
        s, low, count, _ = batches[batch]
        span = pl.ds(pl.multiple_of(block * depth, depth), depth)
        add_in(gathered[block, s * positions + low : s * positions + low + count], span, batch)

    def take_chip(origin_chip, batch):
        s, low, count, _ = batches[batch]
        width = CORES * depth
        span = pl.ds(pl.multiple_of(origin_chip * width, width), width)
        rows = jnp.concatenate(
            [
                gathered[
                    origin_chip * CORES + c, s * positions + low : s * positions + low + count
                ]
                for c in range(CORES)
            ],
            axis=1,
        )
        add_in(rows, span, batch)

    first = spot * local_heads

    def prepare():
        for weight in weights:
            weight.wait()
        chooser = grid_mask(
            2 * local_heads,
            2 * all_heads,
            lambda r, c: c
            == jnp.where(r < local_heads, first + r, all_heads + first + r - local_heads),
        ).astype(jnp.float32)
        gate_own[...] = short_dot(chooser, gate_ref[...]).astype(jnp.bfloat16)
        placer = grid_mask(share, value_width, lambda r, c: c == me * share + r)
        for s in range(sequences):
            new_value = short_dot(new_value_ref[s], placer.astype(jnp.float32))
            for h in range(local_heads):
                side_out[h, s, 2:3, :] = new_value[h : h + 1, :]

    def own(batch):
        for u in batches[batch][3]:
            if u == last_unit:

                @pl.when(core == 0)
                def _(u=u):
                    piece(partner, u, 2, partner).wait_recv()

            else:
                piece(partner, u, 2, partner).wait_recv()
        take_chip(chip, batch)

    def relay(distance, u):
        lanes = range(CORES) if u == last_unit else [core]
        for lane in lanes:
            relay_lane(distance, u, lane)

    def relay_lane(distance, u, lane):
        for way, step in ((1, 1), (0, -1)):
            origin_chip = chip + step * distance
            origin = origin_chip * CORES + lane
            present = (origin_chip >= 0) & (origin_chip < chips)
            if u == last_unit:
                present = present & (core == hub(chip))
            onward = chip - step
            beyond = (onward >= 0) & (onward < chips)
            target = onward * CORES + (hub(onward) if u == last_unit else core)

            @pl.when(present)
            def _(way=way, origin_chip=origin_chip, origin=origin, target=target, beyond=beyond):
                piece(origin, u, way, partner).wait_recv()

                @pl.when(beyond)
                def _():
                    piece(origin, u, way, target).start()

                piece(origin, u, 2, partner).start()
                if u == 1:

                    @pl.when(
                        beyond & (core == 1) & (origin_chip == (0 if way == 0 else chips - 1))
                    )
                    def _():
                        send_last(way)

    def both_sides(distance, act):
        def one_side(side, carry):
            origin_chip = chip + (2 * side - 1) * distance

            @pl.when((origin_chip >= 0) & (origin_chip < chips))
            def _():
                act(origin_chip)

            return carry

        lax.fori_loop(0, 2, one_side, 0)

    def absorb(distance, batch):
        def act(origin_chip):
            for u in batches[batch][3]:
                if u == last_unit:

                    @pl.when(core != hub(chip))
                    def _(u=u):
                        for c in range(CORES):
                            piece(origin_chip * CORES + c, u, 2, partner).wait_recv()

                else:
                    piece(origin_chip * CORES + 1 - core, u, 2, partner).wait_recv()
            take_chip(origin_chip, batch)

        both_sides(distance, act)

    def absorb_last_lane(distance, lane):
        relay_lane(distance, last_unit, lane)

        def act(origin_chip):
            block = origin_chip * CORES + lane

            @pl.when(core != hub(chip))
            def _():
                piece(block, last_unit, 2, partner).wait_recv()

            take_one(block, len(batches) - 1)

        both_sides(distance, act)

    def swap(n, slot, target):
        s, low, count, _ = batches[slot]
        if n == 0:
            block = side_out.at[target, slot], side_in.at[me, slot]
        else:
            source, sink = ((key_out, key_in), (value_out, value_in))[n - 1]
            block = source.at[target, s, pl.ds(low, count)], sink.at[me, s, pl.ds(low, count)]
        return crossing(block, swap_send.at[n], swap_recv.at[n, s], "sp", target)

    def swapped(n, s):
        if n == 0:
            held = sum(batch[0] == s for batch in batches)
            block = side_in.at[pl.ds(0, sp_size - 1), pl.ds(s, held)]
        else:
            block = (key_in, value_in)[n - 1].at[pl.ds(0, sp_size - 1), s]
        crossing((block, block), swap_send.at[n], swap_recv.at[n, s], "sp", others[0]).wait_recv()

    def hand_out(slot):
        s, low, count, _ = batches[slot]
        cut = slice(s * positions + low, s * positions + low + count)
        gates = gate_acc[s, :, low : low + count]
        extra = extra_ref[s, :, low : low + count]
        for h in range(local_heads):
            side_out[h, slot, 0:1, low : low + count] = (
                -rate_ref[h] * softplus(gates[h : h + 1]) + extra[h : h + 1, :]
            )
            side_out[h, slot, 1:2, low : low + count] = jax.nn.sigmoid(
                gates[local_heads + h : local_heads + h + 1] - strength_offset
            )
        for other in others:
            swap(0, slot, other).start()
        for h in range(local_heads):
            key_out[h, s, low : low + count] = key_acc[
                cut, h * key_width : (h + 1) * key_width
            ].astype(jnp.bfloat16)
        for other in others:
            swap(1, slot, other).start()
        for h in range(local_heads):
            value_out[h, s, low : low + count] = value_acc[
                cut, h * value_width : (h + 1) * value_width
            ].astype(jnp.bfloat16)
        for other in others:
            swap(2, slot, other).start()
        side_in[me, slot] = side_out[me, slot]
        key_in[me, s, low : low + count] = key_out[me, s, low : low + count]
        value_in[me, s, low : low + count] = value_out[me, s, low : low + count]

    far = chips - 1
    last_batch = len(batches) - 1
    steps = {1: [(1, 0), (1, 1), (1, 2)]} if far > 1 else {}
    for distance in range(2, far):
        steps[distance] = [(distance, 0), (distance, 1), (distance, 2)]
    work = [(own, (0,)), (own, (1,)), (own, (2,))]
    prepared = False
    for distance in range(1, far):
        for event in steps[distance]:
            relay(*event)
            if not prepared:
                prepare()
                prepared = True
            if work:
                act, operands = work.pop(0)
                act(*operands)
            if event[1] == 1:
                work.insert(0, (absorb, (distance, 0)))
            if event[1] == 2:
                work.append((absorb, (distance, 1)))
    if not prepared:
        prepare()
    for act, operands in [w for w in work if w[0] is own]:
        act(*operands)
    work = [w for w in work if w[0] is absorb]
    relay(far, 0)
    for act, operands in [w for w in work if w[1][1] == 0]:
        act(*operands)
    work = [w for w in work if w[1][1] != 0]
    relay(far, 1)
    absorb(far, 0)

    @pl.when(me < sp_size - 1)
    def _():
        pl.semaphore_wait(peers_sem, sp_size - 1 - me)

    hand_out(0)
    if far > 1:
        relay(1, last_unit)
    for act, operands in work:
        act(*operands)
    relay(far, 2)
    if far > 1:
        absorb(1, last_batch)
    absorb(far, 1)
    hand_out(1)
    pending = None
    for distance in range(2, far):
        relay(distance, last_unit)
        if pending is not None:
            absorb(*pending)
        pending = (distance, last_batch)
    if pending is not None:
        absorb(*pending)
    for lane in range(CORES):
        absorb_last_lane(far, lane)
    hand_out(2)

    whole, part = last_unit * half, half
    settle(4, chips, whole)
    settle(6, 1, part)

    @pl.when(core == hub(chip))
    def _():
        settle(5, CORES * far, part)

    for c in range(chips):
        for way, sent in ((0, c + 1), (1, chips - c)):
            if sent < chips:

                @pl.when(chip == c)
                def _(way=way, sent=sent):
                    settle(2 * way, sent, whole)

                @pl.when((chip == c) & (core == 1))
                def _(way=way, sent=sent):
                    settle(2 * way + 1, CORES * sent, part)

    side_rows = side_in.shape[2]
    upto = grid_mask(positions, positions, lambda r, c: r <= c).astype(jnp.float32)
    down = jnp.concatenate(
        [
            grid_mask(positions, positions, lambda r, c: c <= r).astype(jnp.float32),
            grid_mask(positions, positions, lambda r, c: c == r).astype(jnp.float32),
        ],
        axis=0,
    )
    lanes = pl.ds(pl.multiple_of(me * key_width, key_width), key_width)
    queries = query_ref[:, lanes].astype(jnp.float32)
    new_keys = new_key_ref[:, lanes].astype(jnp.float32)
    new_keys = new_keys * lax.rsqrt(jnp.sum(new_keys * new_keys, axis=-1, keepdims=True) + 1e-06)
    meets = jnp.sum(queries * new_keys, axis=-1, keepdims=True)

    def block_maps(s, slots):
        count = positions
        eye = grid_mask(count, count, lambda r, c: r == c).astype(jnp.float32)
        lower = grid_mask(count, count, lambda r, c: r >= c)
        strict = grid_mask(count, count, lambda r, c: r > c)
        swapped(0, s)
        swapped(1, s)
        side = three_terms(
            sum(side_in[:, slot].reshape(sp_size * side_rows, positions) for slot in slots)
        )
        running_row = sum(short_dot(term, upto) for term in side)
        columns = sum(short_dot(down, term, ((1,), (1,))) for term in side)
        parts = []
        for b in range(sp_size):
            line = b * side_rows
            row = running_row[line : line + 1, :]
            col = columns[:positions, line : line + 1]
            strength = columns[positions:, line + 1 : line + 2]
            final_log = row[:, count - 1 : count]
            keys = key_in[b, s].astype(jnp.float32)
            keys = keys * lax.rsqrt(jnp.sum(keys * keys, axis=-1, keepdims=True) + 1e-06)
            within = jnp.where(lower, jnp.exp(jnp.where(lower, col - row, 0.0)), 0.0)
            scaled = keys * strength
            power = jnp.where(strict, -short_dot(scaled, keys, ((1,), (1,))) * within, 0.0)
            erased = scaled * jnp.exp(col)
            carried = (keys * jnp.exp(final_log - col)).T.astype(jnp.bfloat16)
            parts.append([eye + power, power, strength, erased, carried, jnp.exp(final_log)])
        for part in parts:
            part[1] = short_dot(part[1], part[1])
        covered = 2
        while covered < count:
            for part in parts:
                if covered * 2 < count:
                    both = short_dot(part[1], jnp.concatenate([part[0], part[1]], axis=1))
                    part[0] = part[0] + both[:, :count]
                    part[1] = both[:, count:]
                else:
                    part[0] = part[0] + short_dot(part[1], part[0])
            covered = covered * 2
        swapped(2, s)
        solved = []
        for b, part in enumerate(parts):
            values = value_in[b, s].astype(jnp.float32) * part[2]
            solved.append(short_dot(part[0], jnp.concatenate([part[3], values], axis=1)))
        maps = []
        for part, both in zip(parts, solved):
            both = short_dot(part[4], both)
            maps.append((both[:, :key_width], both[:, key_width:], part[5]))
        return maps

    def final(n, s, target):
        block = (
            (state_out.at[target, s], state_ref.at[s, me]),
            (row_out.at[target, s], row_in.at[me, s]),
        )[n]
        return crossing(block, last_send.at[n], last_recv.at[n], "sp", target)

    def finish(s, maps):
        while len(maps) > 2:
            maps = [compose(maps[i + 1], maps[i]) for i in range(0, len(maps), 2)]
        state = compose_write(maps[1], maps[0][1])
        wide = (8, key_width)
        first_row = grid_mask(*wide, lambda r, c: r == 0)
        probes = jnp.where(
            first_row,
            jnp.broadcast_to(queries[s : s + 1], wide),
            jnp.broadcast_to(new_keys[s : s + 1], wide),
        )
        probe_terms, state_terms = three_terms(probes)[:2], three_terms(state)[:2]
        reads = (
            short_dot(probe_terms[0], state_terms[0])
            + short_dot(probe_terms[0], state_terms[1])
            + short_dot(probe_terms[1], state_terms[0])
        )
        turned = state.T.astype(jnp.bfloat16)
        for j in range(sp_size):
            state_out[j, s] = turned[j * share : (j + 1) * share, :]
        for other in others:
            final(0, s, other).start()
        query_read, key_read = reads[0:1], reads[1:2]
        new_value = jnp.sum(side_in[:, s, 2, :], axis=0, keepdims=True)
        raw = query_read + (next_strength_ref[s, me] * meets[s : s + 1]) * (new_value - key_read)
        raw = raw * lax.rsqrt(jnp.sum(raw * raw, axis=-1, keepdims=True) / value_width + 1e-06)
        for j in range(sp_size):
            turn = j * share
            row_out[j, s, 0:1, :] = (
                jnp.concatenate([raw[:, turn:], raw[:, :turn]], axis=1) if j else raw
            )
        for other in others:
            final(1, s, other).start()
        state_ref[s, me] = state_out[me, s]
        row_in[me, s] = row_out[me, s]

    row_out[...] = jnp.zeros_like(row_out)
    finish(0, block_maps(0, (0,)))
    finish(1, block_maps(1, (1, 2)))

    peers = pl.ds(0, sp_size - 1)
    for n, sent in enumerate((side_out, key_out, value_out)):
        block = sent.at[peers]
        crossing((block, block), swap_send.at[n], swap_recv.at[n, 0], "sp", others[0]).wait_send()
    for n, sent in enumerate((state_out, row_out)):
        block = sent.at[peers]
        crossing((block, block), last_send.at[n], last_recv.at[n], "sp", others[0]).wait_send()
    block = row_in.at[peers]
    crossing((block, block), last_send.at[1], last_recv.at[1], "sp", others[0]).wait_recv()
    for s in range(sequences):
        rows = jnp.concatenate([row_in[i, s, 0:1, :share] for i in range(sp_size)], axis=0)
        read_ref[s] = (rows * gain_ref[...].reshape(1, share)).astype(jnp.bfloat16)
    block = state_ref.at[:, peers]
    crossing((block, block), last_send.at[0], last_recv.at[0], "sp", others[0]).wait_recv()


def place_kernel(state_ref, read_ref, state_hbm, read_hbm, sem):
    copies = [
        pltpu.make_async_copy(state_ref, state_hbm, sem.at[0]),
        pltpu.make_async_copy(read_ref, read_hbm, sem.at[1]),
    ]
    for copy in copies:
        copy.start()
    for copy in copies:
        copy.wait()


def local_fused(
    tokens,
    key_matrix,
    value_matrix,
    gate_matrix,
    head_decay_rate,
    extra_log_decay,
    next_token_query,
    next_token_key,
    next_token_value,
    next_write_strength,
    read_norm_gain,
):
    sequences, positions, depth = tokens.shape
    local_heads = head_decay_rate.shape[0]
    sp_size = lax.axis_size("sp")
    tp_size = lax.axis_size("tp")
    key_total = key_matrix.shape[1]
    value_total = value_matrix.shape[1]
    key_width = key_total // local_heads
    value_width = value_total // local_heads
    share = value_width // sp_size
    rows = sequences * positions
    units = 2 * sequences
    slots = sequences + 1
    vmem = pl.BlockSpec(memory_space=pltpu.VMEM)
    anywhere = pl.BlockSpec(memory_space=pl.ANY)
    dma = pltpu.SemaphoreType.DMA
    held = (sp_size, sequences, positions)
    turned, read = pl.pallas_call(
        functools.partial(fused_kernel, sp_size, tp_size),
        out_shape=(
            pltpu.VMEM((sequences, local_heads, share, key_width), jnp.bfloat16),
            pltpu.VMEM((sequences, local_heads, share), jnp.bfloat16),
        ),
        in_specs=[anywhere] * 11,
        out_specs=(vmem, vmem),
        scratch_shapes=[
            pltpu.SMEM(head_decay_rate.shape, jnp.float32),
            pltpu.SMEM(next_write_strength.shape, jnp.float32),
            pltpu.VMEM((tp_size, rows, depth), jnp.bfloat16),
            pltpu.VMEM(key_matrix.shape, jnp.bfloat16),
            pltpu.VMEM(value_matrix.shape, jnp.bfloat16),
            pltpu.VMEM(gate_matrix.shape[::-1], jnp.bfloat16),
            pltpu.VMEM((2 * local_heads, gate_matrix.shape[0]), jnp.bfloat16),
            pltpu.VMEM(extra_log_decay.shape, jnp.float32),
            pltpu.VMEM(next_token_query.shape, jnp.bfloat16),
            pltpu.VMEM(next_token_key.shape, jnp.bfloat16),
            pltpu.VMEM(next_token_value.shape, jnp.bfloat16),
            pltpu.VMEM(read_norm_gain.shape, jnp.float32),
            pltpu.VMEM((rows, key_total), jnp.float32),
            pltpu.VMEM((rows, value_total), jnp.float32),
            pltpu.VMEM((sequences, 2 * local_heads, positions), jnp.float32),
            pltpu.VMEM((*held, key_width), jnp.bfloat16),
            pltpu.VMEM((*held, key_width), jnp.bfloat16),
            pltpu.VMEM((*held, value_width), jnp.bfloat16),
            pltpu.VMEM((*held, value_width), jnp.bfloat16),
            pltpu.VMEM((sp_size, slots, 8, positions), jnp.float32),
            pltpu.VMEM((sp_size, slots, 8, positions), jnp.float32),
            pltpu.VMEM((sp_size, sequences, share, key_width), jnp.bfloat16),
            pltpu.VMEM((sp_size, sequences, 8, value_width), jnp.float32),
            pltpu.VMEM((sp_size, sequences, 8, value_width), jnp.float32),
            dma((sequences,)),
            dma((10,)),
            dma((tp_size, units)),
            dma((7,)),
            dma((3, sequences)),
            dma((3,)),
            dma((2,)),
            dma((2,)),
            pltpu.SemaphoreType.REGULAR,
            pltpu.SemaphoreType.REGULAR,
        ],
        compiler_params=pltpu.CompilerParams(
            collective_id=0, has_side_effects=True
        ),
    )(
        head_decay_rate,
        next_write_strength,
        tokens,
        key_matrix,
        value_matrix,
        gate_matrix.T,
        extra_log_decay,
        next_token_query,
        next_token_key,
        next_token_value,
        read_norm_gain,
    )
    turned, read = pl.pallas_call(
        place_kernel,
        out_shape=tuple(jax.ShapeDtypeStruct(a.shape, a.dtype) for a in (turned, read)),
        in_specs=[vmem, vmem],
        out_specs=(anywhere, anywhere),
        scratch_shapes=[dma((2,))],
    )(*(pltpu.with_memory_space_constraint(a, pltpu.VMEM) for a in (turned, read)))
    return jnp.swapaxes(turned, 2, 3), read


def local(*arguments):
    tokens, key_matrix, value_matrix = arguments[:3]
    sequences, positions, _ = tokens.shape
    local_heads = arguments[4].shape[0]
    sp_size = lax.axis_size("sp")
    fits = (
        local_heads == sp_size
        and sp_size == 4
        and sequences == 2
        and 2 * local_heads == 8
        and lax.axis_size("tp") % CORES == 0
        and lax.axis_size("tp") > CORES
        and positions == key_matrix.shape[1] // local_heads
        and positions == value_matrix.shape[1] // local_heads
        and positions % 128 == 0
    )
    return local_fused(*arguments) if fits else local_general(*arguments)


def solution(mesh):
    in_specs = (
        P(None, "sp", "tp"),
        P(None, "tp"),
        P(None, "tp"),
        P(),
        P("tp"),
        P(None, "tp", "sp"),
        P(None, "tp"),
        P(None, "tp"),
        P(None, "tp", "sp"),
        P(None, "tp"),
        P("sp"),
    )
    out_specs = (P(None, "tp", None, "sp"), P(None, "tp", "sp"))
    return jax.shard_map(local, mesh=mesh, in_specs=in_specs, out_specs=out_specs, check_vma=False)
```

```python
import functools

import jax
import jax.numpy as jnp
from jax import lax
from jax.experimental import pallas as pl
from jax.experimental.pallas import tpu as pltpu
from jax.sharding import PartitionSpec as P

DV = 128
CORES = 2
MESH = pl.DeviceIdType.MESH


exact_mode = lax.Precision.HIGHEST
strength_offset = 5.0


def unit_rows(matrix):
    return matrix * lax.rsqrt(jnp.sum(matrix * matrix, axis=-1, keepdims=True) + 1e-06)


def nilpotent_inverse(mixing):
    extent = mixing.shape[-1]
    result = jnp.zeros_like(mixing) + jnp.eye(extent, dtype=jnp.float32)
    powered = -mixing
    covered = 1
    while covered < extent:
        product = lax.optimization_barrier(
            jnp.einsum("...ij,...jk->...ik", result, powered, precision=exact_mode)
        )
        result = result + product
        powered = jnp.einsum("...ij,...jk->...ik", powered, powered, precision=exact_mode)
        covered = covered * 2
    return result


def block_terms(unit_keys, values, decay_logarithm, strength):
    extent = unit_keys.shape[-2]
    lower = jnp.tril(jnp.ones((extent, extent), jnp.bool_))
    strict = jnp.tril(jnp.ones((extent, extent), jnp.bool_), -1)
    running = jnp.cumsum(decay_logarithm, axis=-1)
    spread = running[..., :, None] - running[..., None, :]
    within = jnp.where(lower, jnp.exp(jnp.where(lower, spread, 0.0)), 0.0)
    scaled = unit_keys * strength[..., None]
    mixing = jnp.where(
        strict,
        jnp.einsum("...id,...jd->...ij", scaled, unit_keys, precision=exact_mode) * within,
        0.0,
    )
    inverse = nilpotent_inverse(mixing)
    writes = jnp.einsum(
        "...ij,...je->...ie", inverse, values * strength[..., None], precision=exact_mode
    )
    erases = jnp.einsum(
        "...ij,...jd->...id", inverse, scaled * jnp.exp(running)[..., None], precision=exact_mode
    )
    final_log = running[..., -1]
    carried = unit_keys * jnp.exp(final_log[..., None] - running)[..., None]
    return (writes, erases, carried, final_log)


def split_blocks(array, block_count):
    shaped = array.reshape(
        array.shape[:2] + (block_count, array.shape[2] // block_count) + array.shape[3:]
    )
    return jnp.moveaxis(shaped, 2, 0)


def local_general(
    tokens,
    key_matrix,
    value_matrix,
    gate_matrix,
    head_decay_rate,
    extra_log_decay,
    next_token_query,
    next_token_key,
    next_token_value,
    next_write_strength,
    read_norm_gain,
):
    sequences, positions, _ = tokens.shape
    local_heads = head_decay_rate.shape[0]
    key_width = key_matrix.shape[1] // local_heads
    value_width = value_matrix.shape[1] // local_heads
    all_heads = gate_matrix.shape[1] // 2
    group_size = lax.axis_size("sp")
    column_share = value_width // group_size
    first_head = lax.axis_index("tp") * local_heads
    decay_cols = lax.dynamic_slice_in_dim(gate_matrix, first_head, local_heads, 1)
    strength_cols = lax.dynamic_slice_in_dim(gate_matrix, all_heads + first_head, local_heads, 1)
    gate_cols = jnp.concatenate([decay_cols, strength_cols], axis=1)
    row_count = sequences * positions
    incoming = lax.all_gather(tokens, "tp", axis=2, tiled=True)
    span_width = incoming.shape[2]
    flat_rows = incoming.reshape(row_count, span_width)
    products = lax.optimization_barrier(
        (
            jnp.dot(flat_rows, key_matrix, preferred_element_type=jnp.float32),
            jnp.dot(flat_rows, value_matrix, preferred_element_type=jnp.float32),
            jnp.dot(flat_rows, gate_cols, preferred_element_type=jnp.float32),
        )
    )
    key_sum = products[0]
    value_sum = products[1]
    gate_pre = products[2]
    key_float = lax.optimization_barrier(key_sum.astype(jnp.bfloat16)).astype(jnp.float32)
    value_float = lax.optimization_barrier(value_sum.astype(jnp.bfloat16)).astype(jnp.float32)
    unit_keys = unit_rows(
        key_float.reshape(sequences, positions, local_heads, key_width).transpose(0, 2, 1, 3)
    )
    values = value_float.reshape(sequences, positions, local_heads, value_width).transpose(
        0, 2, 1, 3
    )
    gate_projected = gate_pre.reshape(sequences, positions, 2 * local_heads).transpose(0, 2, 1)
    decay_logarithm = (
        -head_decay_rate[None, :, None] * jax.nn.softplus(gate_projected[:, :local_heads])
        + extra_log_decay
    )
    strength = jax.nn.sigmoid(gate_projected[:, local_heads:] - strength_offset)
    block_count = positions // min(64, positions)
    block_parts = block_terms(
        split_blocks(unit_keys, block_count),
        split_blocks(values, block_count),
        split_blocks(decay_logarithm, block_count),
        split_blocks(strength, block_count),
    )
    identity = jnp.zeros((sequences, local_heads, key_width, key_width), jnp.float32) + jnp.eye(
        key_width, dtype=jnp.float32
    )
    start_map = jnp.concatenate(
        [identity, jnp.zeros((sequences, local_heads, key_width, value_width), jnp.float32)],
        axis=-1,
    )

    def advance(current, block_part):
        writes, erases, carried, final_log = block_part
        padded = jnp.concatenate(
            [jnp.zeros(writes.shape[:-1] + (key_width,), jnp.float32), writes], axis=-1
        )
        removed = lax.optimization_barrier(
            jnp.einsum("shcd,shde->shce", erases, current, precision=exact_mode)
        )
        fresh = padded - removed
        added = lax.optimization_barrier(
            jnp.einsum("shcd,shce->shde", carried, fresh, precision=exact_mode)
        )
        current = current * jnp.exp(final_log)[..., None, None] + added
        return (current, None)

    local_map, _ = lax.scan(advance, start_map, block_parts)
    carry_map = local_map[..., :key_width]
    write_map = local_map[..., key_width:]
    carry_copies = jnp.broadcast_to(carry_map[None], (group_size,) + carry_map.shape)
    write_parts = jnp.moveaxis(
        write_map.reshape(sequences, local_heads, key_width, group_size, column_share), 3, 0
    )
    carries = lax.all_to_all(carry_copies, "sp", split_axis=0, concat_axis=0, tiled=True)
    write_cols = lax.all_to_all(write_parts, "sp", split_axis=0, concat_axis=0, tiled=True)

    def fold_step(current, block_map):
        moved = lax.optimization_barrier(
            jnp.einsum("shij,shje->shie", block_map[0], current, precision=exact_mode)
        )
        return (moved + block_map[1], None)

    begin_state = jnp.zeros(write_cols.shape[1:], jnp.float32)
    folded, _ = lax.scan(fold_step, begin_state, (carries, write_cols))
    query_rows = next_token_query.astype(jnp.float32).reshape(sequences, local_heads, key_width)
    unit_new = unit_rows(
        next_token_key.astype(jnp.float32).reshape(sequences, local_heads, key_width)
    )
    value_rows = next_token_value.astype(jnp.float32)
    key_read = jnp.einsum("shd,shde->she", unit_new, folded, precision=exact_mode)
    query_read = jnp.einsum("shd,shde->she", query_rows, folded, precision=exact_mode)
    intersection = jnp.sum(query_rows * unit_new, axis=-1)
    read_raw = query_read + (next_write_strength * intersection)[..., None] * (
        value_rows - key_read
    )
    square_total = lax.psum(jnp.sum(read_raw * read_raw, axis=-1, keepdims=True), "sp")
    first_read = read_raw * lax.rsqrt(square_total / DV + 1e-06) * read_norm_gain
    return (folded.astype(jnp.bfloat16), first_read.astype(jnp.bfloat16))


def short_dot(left, right, contract=((1,), (0,))):
    return lax.dot_general(
        left.astype(jnp.bfloat16),
        right.astype(jnp.bfloat16),
        (contract, ((), ())),
        preferred_element_type=jnp.float32,
    )


def three_terms(x):
    first = x.astype(jnp.bfloat16)
    rest = x - first.astype(jnp.float32)
    second = rest.astype(jnp.bfloat16)
    third = (rest - second.astype(jnp.float32)).astype(jnp.bfloat16)
    return first, second, third


def close_dot(left, right):
    left, right = three_terms(left)[:2], three_terms(right)[:2]
    return (
        short_dot(left[0], right[0]) + short_dot(left[0], right[1]) + short_dot(left[1], right[0])
    )


def softplus(x):
    return jnp.maximum(x, 0.0) + jnp.log1p(jnp.exp(-jnp.abs(x)))


def grid_mask(rows, cols, rule):
    row = lax.broadcasted_iota(jnp.int32, (rows, cols), 0)
    col = lax.broadcasted_iota(jnp.int32, (rows, cols), 1)
    return rule(row, col)


def compose(late, early):
    late_map, late_write, late_keep = late
    early_map, early_write, early_keep = early
    width = early_map.shape[1]
    moved = short_dot(late_map, jnp.concatenate([early_map, early_write], axis=1))
    return (
        late_keep * early_map + early_keep * late_map - moved[:, :width],
        late_keep * early_write + late_write - moved[:, width:],
        late_keep * early_keep,
    )


def compose_write(late, early_write):
    late_map, late_write, late_keep = late
    return late_keep * early_write + late_write - short_dot(late_map, early_write)


def fused_kernel(
    sp_size,
    tp_size,
    rate_hbm,
    next_strength_hbm,
    tokens_ref,
    key_ref,
    value_ref,
    gate_hbm,
    extra_hbm,
    query_hbm,
    new_key_hbm,
    new_value_hbm,
    gain_hbm,
    state_ref,
    read_ref,
    rate_ref,
    next_strength_ref,
    gathered,
    key_w,
    value_w,
    gate_ref,
    gate_own,
    extra_ref,
    query_ref,
    new_key_ref,
    new_value_ref,
    gain_ref,
    key_acc,
    value_acc,
    gate_acc,
    key_out,
    key_in,
    value_out,
    value_in,
    side_out,
    side_in,
    state_out,
    row_out,
    row_in,
    load_sem,
    weight_sem,
    gather_recv,
    gather_send,
    swap_recv,
    swap_send,
    last_recv,
    last_send,
    above_sem,
    peers_sem,
):
    sequences, positions, depth = tokens_ref.shape
    local_heads = extra_ref.shape[1]
    key_width = key_acc.shape[1] // local_heads
    value_width = value_acc.shape[1] // local_heads
    share = value_width // sp_size
    all_heads = gate_ref.shape[0] // 2
    chips = tp_size // CORES
    me = lax.axis_index("sp")
    spot = lax.axis_index("tp")
    chip = spot // CORES
    core = spot % CORES
    partner = chip * CORES + (1 - core)
    half = positions // 2
    units = [(s, part * half, half) for s in range(sequences) for part in range(2)]
    last_unit = len(units) - 1
    batches = [(0, 0, positions, (0, 1)), (1, 0, half, (2,)), (1, half, half, (3,))]
    others = [sp_size - 1 - me, me + 1 - 2 * (me % 2), (me + 2) % sp_size]

    loads = [
        pltpu.make_async_copy(
            tokens_ref.at[s],
            gathered.at[spot, pl.ds(s * positions, positions)],
            load_sem.at[s],
        )
        for s in range(sequences)
    ]
    for load in loads:
        load.start()

    barrier = pltpu.get_barrier_semaphore()
    pl.semaphore_signal(barrier, inc=1, device_id={"tp": partner}, device_id_type=MESH)

    @pl.when(chip < chips - 1)
    def _():
        pl.semaphore_signal(barrier, inc=1, device_id={"tp": spot + CORES}, device_id_type=MESH)

    for other in range(1, sp_size):

        @pl.when(me < other)
        def _(other=other):
            pl.semaphore_signal(barrier, inc=1, device_id={"sp": other}, device_id_type=MESH)

    weights = [
        pltpu.make_async_copy(key_ref, key_w, weight_sem.at[0]),
        pltpu.make_async_copy(value_ref, value_w, weight_sem.at[1]),
        pltpu.make_async_copy(gate_hbm, gate_ref, weight_sem.at[2]),
        pltpu.make_async_copy(extra_hbm, extra_ref, weight_sem.at[3]),
        pltpu.make_async_copy(query_hbm, query_ref, weight_sem.at[4]),
        pltpu.make_async_copy(new_key_hbm, new_key_ref, weight_sem.at[5]),
        pltpu.make_async_copy(new_value_hbm, new_value_ref, weight_sem.at[6]),
        pltpu.make_async_copy(gain_hbm, gain_ref, weight_sem.at[7]),
        pltpu.make_async_copy(rate_hbm, rate_ref, weight_sem.at[8]),
        pltpu.make_async_copy(next_strength_hbm, next_strength_ref, weight_sem.at[9]),
    ]
    for weight in weights:
        weight.start()
    pl.semaphore_wait(barrier, jnp.where(chip > 0, 1, 0) + 1 + me)

    @pl.when(chip > 0)
    def _():
        pl.semaphore_signal(above_sem, inc=1, device_id={"tp": spot - CORES}, device_id_type=MESH)

    for other in range(sp_size - 1):

        @pl.when(other < me)
        def _(other=other):
            pl.semaphore_signal(peers_sem, inc=1, device_id={"sp": other}, device_id_type=MESH)

    def crossing(block, send, recv, axis, target):
        return pltpu.make_async_remote_copy(
            src_ref=block[0],
            dst_ref=block[1],
            send_sem=send,
            recv_sem=recv,
            device_id={axis: target},
            device_id_type=MESH,
        )

    def piece(origin, u, way, target, own=False):
        s, low, count = units[u]
        block = gathered.at[origin, pl.ds(s * positions + low, count)]
        kind = 2 * way + (u == last_unit) + (way == 2 and u == last_unit and own)
        return crossing(
            (block, block), gather_send.at[kind], gather_recv.at[origin, u], "tp", target
        )

    def settle(kind, blocks, count):
        block = gathered.at[pl.ds(0, blocks), pl.ds(0, count)]
        crossing(
            (block, block), gather_send.at[kind], gather_recv.at[0, 0], "tp", partner
        ).wait_send()

    for load in loads:
        load.wait()

    def hub(a_chip):
        return jnp.where((a_chip == 0) | (a_chip == chips - 1), 0, 1)

    for u in range(last_unit):

        @pl.when(chip > 0)
        def _(u=u):
            piece(spot, u, 1, spot - CORES).start()

    for u in [last_unit, *range(last_unit)]:
        piece(spot, u, 2, partner, own=True).start()

    @pl.when(chip < chips - 1)
    def _():
        pl.semaphore_wait(above_sem, 1)

    for u in range(last_unit):

        @pl.when(chip < chips - 1)
        def _(u=u):
            piece(spot, u, 0, spot + CORES).start()

    def send_last(way):
        onward = chip + (1 if way == 0 else -1)
        for c in range(CORES):
            piece(chip * CORES + c, last_unit, way, onward * CORES + hub(onward)).start()

    @pl.when(core == 1)
    def _():
        piece(partner, last_unit, 2, partner).wait_recv()

        @pl.when(chip == chips - 1)
        def _():
            send_last(1)

        @pl.when(chip == 0)
        def _():
            send_last(0)

    key_acc[...] = jnp.zeros_like(key_acc)
    value_acc[...] = jnp.zeros_like(value_acc)
    gate_acc[...] = jnp.zeros_like(gate_acc)
    side_out[...] = jnp.zeros_like(side_out)

    def add_in(rows, span, batch):
        s, low, count, parts = batches[batch]
        cut = slice(s * positions + low, s * positions + low + count)
        key_acc[cut] += jnp.dot(rows, key_w[span, :], preferred_element_type=jnp.float32)
        value_acc[cut] += jnp.dot(rows, value_w[span, :], preferred_element_type=jnp.float32)
        gates = lax.dot_general(
            gate_own[:, span],
            rows,
            (((1,), (1,)), ((), ())),
            preferred_element_type=jnp.float32,
        )
        gate_acc[s, :, low : low + count] += gates

    def take_one(block, batch):
        s, low, count, _ = batches[batch]
        span = pl.ds(pl.multiple_of(block * depth, depth), depth)
        add_in(gathered[block, s * positions + low : s * positions + low + count], span, batch)

    def take_chip(origin_chip, batch):
        s, low, count, _ = batches[batch]
        width = CORES * depth
        span = pl.ds(pl.multiple_of(origin_chip * width, width), width)
        rows = jnp.concatenate(
            [
                gathered[
                    origin_chip * CORES + c, s * positions + low : s * positions + low + count
                ]
                for c in range(CORES)
            ],
            axis=1,
        )
        add_in(rows, span, batch)

    first = spot * local_heads

    def prepare():
        for weight in weights:
            weight.wait()
        chooser = grid_mask(
            2 * local_heads,
            2 * all_heads,
            lambda r, c: c
            == jnp.where(r < local_heads, first + r, all_heads + first + r - local_heads),
        ).astype(jnp.float32)
        gate_own[...] = short_dot(chooser, gate_ref[...]).astype(jnp.bfloat16)
        placer = grid_mask(share, value_width, lambda r, c: c == me * share + r)
        for s in range(sequences):
            new_value = short_dot(new_value_ref[s], placer.astype(jnp.float32))
            for h in range(local_heads):
                side_out[h, s, 2:3, :] = new_value[h : h + 1, :]

    def own(batch):
        for u in batches[batch][3]:
            if u == last_unit:

                @pl.when(core == 0)
                def _(u=u):
                    piece(partner, u, 2, partner).wait_recv()

            else:
                piece(partner, u, 2, partner).wait_recv()
        take_chip(chip, batch)

    def relay(distance, u):
        lanes = range(CORES) if u == last_unit else [core]
        for lane in lanes:
            relay_lane(distance, u, lane)

    def relay_lane(distance, u, lane):
        for way, step in ((1, 1), (0, -1)):
            origin_chip = chip + step * distance
            origin = origin_chip * CORES + lane
            present = (origin_chip >= 0) & (origin_chip < chips)
            if u == last_unit:
                present = present & (core == hub(chip))
            onward = chip - step
            beyond = (onward >= 0) & (onward < chips)
            target = onward * CORES + (hub(onward) if u == last_unit else core)

            @pl.when(present)
            def _(way=way, origin_chip=origin_chip, origin=origin, target=target, beyond=beyond):
                piece(origin, u, way, partner).wait_recv()

                @pl.when(beyond)
                def _():
                    piece(origin, u, way, target).start()

                piece(origin, u, 2, partner).start()
                if u == 1:

                    @pl.when(
                        beyond & (core == 1) & (origin_chip == (0 if way == 0 else chips - 1))
                    )
                    def _():
                        send_last(way)

    def both_sides(distance, act):
        def one_side(side, carry):
            origin_chip = chip + (2 * side - 1) * distance

            @pl.when((origin_chip >= 0) & (origin_chip < chips))
            def _():
                act(origin_chip)

            return carry

        lax.fori_loop(0, 2, one_side, 0)

    def absorb(distance, batch):
        def act(origin_chip):
            for u in batches[batch][3]:
                if u == last_unit:

                    @pl.when(core != hub(chip))
                    def _(u=u):
                        for c in range(CORES):
                            piece(origin_chip * CORES + c, u, 2, partner).wait_recv()

                else:
                    piece(origin_chip * CORES + 1 - core, u, 2, partner).wait_recv()
            take_chip(origin_chip, batch)

        both_sides(distance, act)

    def absorb_last_lane(distance, lane):
        relay_lane(distance, last_unit, lane)

        def act(origin_chip):
            block = origin_chip * CORES + lane

            @pl.when(core != hub(chip))
            def _():
                piece(block, last_unit, 2, partner).wait_recv()

            take_one(block, len(batches) - 1)

        both_sides(distance, act)

    def swap(n, slot, target):
        s, low, count, _ = batches[slot]
        if n == 0:
            block = side_out.at[target, slot], side_in.at[me, slot]
        else:
            source, sink = ((key_out, key_in), (value_out, value_in))[n - 1]
            block = source.at[target, s, pl.ds(low, count)], sink.at[me, s, pl.ds(low, count)]
        return crossing(block, swap_send.at[n], swap_recv.at[n, s], "sp", target)

    def swapped(n, s):
        if n == 0:
            held = sum(batch[0] == s for batch in batches)
            block = side_in.at[pl.ds(0, sp_size - 1), pl.ds(s, held)]
        else:
            block = (key_in, value_in)[n - 1].at[pl.ds(0, sp_size - 1), s]
        crossing((block, block), swap_send.at[n], swap_recv.at[n, s], "sp", others[0]).wait_recv()

    def hand_out(slot):
        s, low, count, _ = batches[slot]
        cut = slice(s * positions + low, s * positions + low + count)
        gates = gate_acc[s, :, low : low + count]
        extra = extra_ref[s, :, low : low + count]
        for h in range(local_heads):
            side_out[h, slot, 0:1, low : low + count] = (
                -rate_ref[h] * softplus(gates[h : h + 1]) + extra[h : h + 1, :]
            )
            side_out[h, slot, 1:2, low : low + count] = jax.nn.sigmoid(
                gates[local_heads + h : local_heads + h + 1] - strength_offset
            )
        for other in others:
            swap(0, slot, other).start()
        for h in range(local_heads):
            key_out[h, s, low : low + count] = key_acc[
                cut, h * key_width : (h + 1) * key_width
            ].astype(jnp.bfloat16)
        for other in others:
            swap(1, slot, other).start()
        for h in range(local_heads):
            value_out[h, s, low : low + count] = value_acc[
                cut, h * value_width : (h + 1) * value_width
            ].astype(jnp.bfloat16)
        for other in others:
            swap(2, slot, other).start()
        side_in[me, slot] = side_out[me, slot]
        key_in[me, s, low : low + count] = key_out[me, s, low : low + count]
        value_in[me, s, low : low + count] = value_out[me, s, low : low + count]

    far = chips - 1
    last_batch = len(batches) - 1
    steps = {1: [(1, 0), (1, 1), (1, 2)]} if far > 1 else {}
    for distance in range(2, far):
        steps[distance] = [(distance, 0), (distance, 1), (distance, 2)]
    work = [(own, (0,)), (own, (1,)), (own, (2,))]
    prepared = False
    for distance in range(1, far):
        for event in steps[distance]:
            relay(*event)
            if not prepared:
                prepare()
                prepared = True
            if work:
                act, operands = work.pop(0)
                act(*operands)
            if event[1] == 1:
                work.insert(0, (absorb, (distance, 0)))
            if event[1] == 2:
                work.append((absorb, (distance, 1)))
    if not prepared:
        prepare()
    for act, operands in [w for w in work if w[0] is own]:
        act(*operands)
    work = [w for w in work if w[0] is absorb]
    relay(far, 0)
    for act, operands in [w for w in work if w[1][1] == 0]:
        act(*operands)
    work = [w for w in work if w[1][1] != 0]
    relay(far, 1)
    absorb(far, 0)

    @pl.when(me < sp_size - 1)
    def _():
        pl.semaphore_wait(peers_sem, sp_size - 1 - me)

    hand_out(0)
    if far > 1:
        relay(1, last_unit)
    for act, operands in work:
        act(*operands)
    relay(far, 2)
    if far > 1:
        absorb(1, last_batch)
    absorb(far, 1)
    hand_out(1)
    pending = None
    for distance in range(2, far):
        relay(distance, last_unit)
        if pending is not None:
            absorb(*pending)
        pending = (distance, last_batch)
    if pending is not None:
        absorb(*pending)
    for lane in range(CORES):
        absorb_last_lane(far, lane)
    hand_out(2)

    whole, part = last_unit * half, half
    settle(4, chips, whole)
    settle(6, 1, part)

    @pl.when(core == hub(chip))
    def _():
        settle(5, CORES * far, part)

    for c in range(chips):
        for way, sent in ((0, c + 1), (1, chips - c)):
            if sent < chips:

                @pl.when(chip == c)
                def _(way=way, sent=sent):
                    settle(2 * way, sent, whole)

                @pl.when((chip == c) & (core == 1))
                def _(way=way, sent=sent):
                    settle(2 * way + 1, CORES * sent, part)

    side_rows = side_in.shape[2]
    upto = grid_mask(positions, positions, lambda r, c: r <= c).astype(jnp.float32)
    down = grid_mask(positions, positions, lambda r, c: c <= r).astype(jnp.float32)
    lanes = pl.ds(pl.multiple_of(me * key_width, key_width), key_width)
    queries = query_ref[:, lanes].astype(jnp.float32)
    new_keys = new_key_ref[:, lanes].astype(jnp.float32)
    new_keys = new_keys * lax.rsqrt(jnp.sum(new_keys * new_keys, axis=-1, keepdims=True) + 1e-06)
    meets = jnp.sum(queries * new_keys, axis=-1, keepdims=True)
    weight_of_new = [next_strength_ref[s, me] * meets[s : s + 1] for s in range(sequences)]
    probes = [queries[s : s + 1] - weight_of_new[s] * new_keys[s : s + 1] for s in range(sequences)]

    def block_maps(s, slots):
        count = positions
        eye = grid_mask(count, count, lambda r, c: r == c).astype(jnp.float32)
        strict = grid_mask(count, count, lambda r, c: r > c)
        swapped(0, s)
        swapped(1, s)
        side = sum(side_in[:, slot].reshape(sp_size * side_rows, positions) for slot in slots)
        terms = three_terms(side)
        rows = sum(short_dot(term, upto) for term in terms)
        columns = sum(short_dot(down, term, ((1,), (1,))) for term in terms)
        parts = []
        for b in range(sp_size):
            line = b * side_rows
            row = rows[line : line + 1, :]
            strength = side[line + 1 : line + 2, :]
            col = jnp.broadcast_to(columns[:, line : line + 1], (count, count))
            final_log = row[:, count - 1 : count]
            keys = key_in[b, s].astype(jnp.float32)
            keys = keys * lax.rsqrt(jnp.sum(keys * keys, axis=-1, keepdims=True) + 1e-06)
            within = jnp.exp(jnp.where(strict, col - row, 0.0)) * -strength
            power = jnp.where(strict, short_dot(keys, keys, ((1,), (1,))) * within, 0.0)
            erased = (keys * jnp.exp(col)).astype(jnp.bfloat16)
            carried = (keys.T * (jnp.exp(final_log - row) * strength)).astype(jnp.bfloat16)
            parts.append([eye + power, power, erased, carried, jnp.exp(final_log)])
        for part in parts:
            part[1] = short_dot(part[1], part[1])
        covered = 2
        while covered < count:
            for part in parts:
                if covered * 2 < count:
                    both = short_dot(part[1], jnp.concatenate([part[0], part[1]], axis=1))
                    part[0] = part[0] + both[:, :count]
                    part[1] = both[:, count:]
                else:
                    part[0] = part[0] + short_dot(part[1], part[0])
            covered = covered * 2
        swapped(2, s)
        solved = []
        for b, part in enumerate(parts):
            sources = jnp.concatenate([part[2], value_in[b, s]], axis=1)
            solved.append(short_dot(part[0], sources))
        maps = []
        for part, both in zip(parts, solved):
            both = short_dot(part[3], both)
            maps.append((both[:, :key_width], both[:, key_width:], part[4]))
        return maps

    def final(n, s, target):
        block = (
            (state_out.at[target, s], state_ref.at[s, me]),
            (row_out.at[target, s], row_in.at[me, s]),
        )[n]
        return crossing(block, last_send.at[n], last_recv.at[n], "sp", target)

    def finish(s, maps):
        while len(maps) > 2:
            maps = [compose(maps[i + 1], maps[i]) for i in range(0, len(maps), 2)]
        (_, first_write, _), (late_map, late_write, late_keep) = maps
        state = compose_write(maps[1], first_write)
        probe = jnp.broadcast_to(probes[s], (8, key_width))
        passed = close_dot(probe, jnp.concatenate([late_write, late_map], axis=1))
        onto_first = late_keep * probe - passed[:, value_width:]
        raw = close_dot(onto_first, first_write) + passed[:, :value_width]
        turned = state.T.astype(jnp.bfloat16)
        for j in range(sp_size):
            state_out[j, s] = turned[j * share : (j + 1) * share, :]
        for other in others:
            final(0, s, other).start()
        new_value = jnp.sum(side_in[:, s, 2, :], axis=0, keepdims=True)
        raw = raw[0:1] + weight_of_new[s] * new_value
        raw = raw * lax.rsqrt(jnp.sum(raw * raw, axis=-1, keepdims=True) / value_width + 1e-06)
        for j in range(sp_size):
            turn = j * share
            row_out[j, s, 0:1, :] = (
                jnp.concatenate([raw[:, turn:], raw[:, :turn]], axis=1) if j else raw
            )
        for other in others:
            final(1, s, other).start()
        state_ref[s, me] = state_out[me, s]
        row_in[me, s] = row_out[me, s]

    row_out[...] = jnp.zeros_like(row_out)
    finish(0, block_maps(0, (0,)))
    finish(1, block_maps(1, (1, 2)))

    peers = pl.ds(0, sp_size - 1)
    for n, sent in enumerate((side_out, key_out, value_out)):
        block = sent.at[peers]
        crossing((block, block), swap_send.at[n], swap_recv.at[n, 0], "sp", others[0]).wait_send()
    for n, sent in enumerate((state_out, row_out)):
        block = sent.at[peers]
        crossing((block, block), last_send.at[n], last_recv.at[n], "sp", others[0]).wait_send()
    block = row_in.at[peers]
    crossing((block, block), last_send.at[1], last_recv.at[1], "sp", others[0]).wait_recv()
    for s in range(sequences):
        rows = jnp.concatenate([row_in[i, s, 0:1, :share] for i in range(sp_size)], axis=0)
        read_ref[s] = (rows * gain_ref[...].reshape(1, share)).astype(jnp.bfloat16)
    block = state_ref.at[:, peers]
    crossing((block, block), last_send.at[0], last_recv.at[0], "sp", others[0]).wait_recv()


def place_kernel(state_ref, read_ref, state_hbm, read_hbm, sem):
    copies = [
        pltpu.make_async_copy(state_ref, state_hbm, sem.at[0]),
        pltpu.make_async_copy(read_ref, read_hbm, sem.at[1]),
    ]
    for copy in copies:
        copy.start()
    for copy in copies:
        copy.wait()


def local_fused(
    tokens,
    key_matrix,
    value_matrix,
    gate_matrix,
    head_decay_rate,
    extra_log_decay,
    next_token_query,
    next_token_key,
    next_token_value,
    next_write_strength,
    read_norm_gain,
):
    sequences, positions, depth = tokens.shape
    local_heads = head_decay_rate.shape[0]
    sp_size = lax.axis_size("sp")
    tp_size = lax.axis_size("tp")
    key_total = key_matrix.shape[1]
    value_total = value_matrix.shape[1]
    key_width = key_total // local_heads
    value_width = value_total // local_heads
    share = value_width // sp_size
    rows = sequences * positions
    units = 2 * sequences
    slots = sequences + 1
    vmem = pl.BlockSpec(memory_space=pltpu.VMEM)
    anywhere = pl.BlockSpec(memory_space=pl.ANY)
    dma = pltpu.SemaphoreType.DMA
    held = (sp_size, sequences, positions)
    turned, read = pl.pallas_call(
        functools.partial(fused_kernel, sp_size, tp_size),
        out_shape=(
            pltpu.VMEM((sequences, local_heads, share, key_width), jnp.bfloat16),
            pltpu.VMEM((sequences, local_heads, share), jnp.bfloat16),
        ),
        in_specs=[anywhere] * 11,
        out_specs=(vmem, vmem),
        scratch_shapes=[
            pltpu.SMEM(head_decay_rate.shape, jnp.float32),
            pltpu.SMEM(next_write_strength.shape, jnp.float32),
            pltpu.VMEM((tp_size, rows, depth), jnp.bfloat16),
            pltpu.VMEM(key_matrix.shape, jnp.bfloat16),
            pltpu.VMEM(value_matrix.shape, jnp.bfloat16),
            pltpu.VMEM(gate_matrix.shape[::-1], jnp.bfloat16),
            pltpu.VMEM((2 * local_heads, gate_matrix.shape[0]), jnp.bfloat16),
            pltpu.VMEM(extra_log_decay.shape, jnp.float32),
            pltpu.VMEM(next_token_query.shape, jnp.bfloat16),
            pltpu.VMEM(next_token_key.shape, jnp.bfloat16),
            pltpu.VMEM(next_token_value.shape, jnp.bfloat16),
            pltpu.VMEM(read_norm_gain.shape, jnp.float32),
            pltpu.VMEM((rows, key_total), jnp.float32),
            pltpu.VMEM((rows, value_total), jnp.float32),
            pltpu.VMEM((sequences, 2 * local_heads, positions), jnp.float32),
            pltpu.VMEM((*held, key_width), jnp.bfloat16),
            pltpu.VMEM((*held, key_width), jnp.bfloat16),
            pltpu.VMEM((*held, value_width), jnp.bfloat16),
            pltpu.VMEM((*held, value_width), jnp.bfloat16),
            pltpu.VMEM((sp_size, slots, 8, positions), jnp.float32),
            pltpu.VMEM((sp_size, slots, 8, positions), jnp.float32),
            pltpu.VMEM((sp_size, sequences, share, key_width), jnp.bfloat16),
            pltpu.VMEM((sp_size, sequences, 8, value_width), jnp.float32),
            pltpu.VMEM((sp_size, sequences, 8, value_width), jnp.float32),
            dma((sequences,)),
            dma((10,)),
            dma((tp_size, units)),
            dma((7,)),
            dma((3, sequences)),
            dma((3,)),
            dma((2,)),
            dma((2,)),
            pltpu.SemaphoreType.REGULAR,
            pltpu.SemaphoreType.REGULAR,
        ],
        compiler_params=pltpu.CompilerParams(
            collective_id=0, has_side_effects=True
        ),
    )(
        head_decay_rate,
        next_write_strength,
        tokens,
        key_matrix,
        value_matrix,
        gate_matrix.T,
        extra_log_decay,
        next_token_query,
        next_token_key,
        next_token_value,
        read_norm_gain,
    )
    turned, read = pl.pallas_call(
        place_kernel,
        out_shape=tuple(jax.ShapeDtypeStruct(a.shape, a.dtype) for a in (turned, read)),
        in_specs=[vmem, vmem],
        out_specs=(anywhere, anywhere),
        scratch_shapes=[dma((2,))],
    )(*(pltpu.with_memory_space_constraint(a, pltpu.VMEM) for a in (turned, read)))
    return jnp.swapaxes(turned, 2, 3), read


def local(*arguments):
    tokens, key_matrix, value_matrix = arguments[:3]
    sequences, positions, _ = tokens.shape
    local_heads = arguments[4].shape[0]
    sp_size = lax.axis_size("sp")
    fits = (
        local_heads == sp_size
        and sp_size == 4
        and sequences == 2
        and 2 * local_heads == 8
        and lax.axis_size("tp") % CORES == 0
        and lax.axis_size("tp") > CORES
        and positions == key_matrix.shape[1] // local_heads
        and positions == value_matrix.shape[1] // local_heads
        and positions % 128 == 0
    )
    return local_fused(*arguments) if fits else local_general(*arguments)


def solution(mesh):
    in_specs = (
        P(None, "sp", "tp"),
        P(None, "tp"),
        P(None, "tp"),
        P(),
        P("tp"),
        P(None, "tp", "sp"),
        P(None, "tp"),
        P(None, "tp"),
        P(None, "tp", "sp"),
        P(None, "tp"),
        P("sp"),
    )
    out_specs = (P(None, "tp", None, "sp"), P(None, "tp", "sp"))
    return jax.shard_map(local, mesh=mesh, in_specs=in_specs, out_specs=out_specs, check_vma=False)
```

```python
import functools

import jax
import jax.numpy as jnp
from jax import lax
from jax.experimental import pallas as pl
from jax.experimental.pallas import tpu as pltpu
from jax.sharding import PartitionSpec as P

DV = 128
CORES = 2
MESH = pl.DeviceIdType.MESH


exact_mode = lax.Precision.HIGHEST
strength_offset = 5.0


def unit_rows(matrix):
    return matrix * lax.rsqrt(jnp.sum(matrix * matrix, axis=-1, keepdims=True) + 1e-06)


def nilpotent_inverse(mixing):
    extent = mixing.shape[-1]
    result = jnp.zeros_like(mixing) + jnp.eye(extent, dtype=jnp.float32)
    powered = -mixing
    covered = 1
    while covered < extent:
        product = lax.optimization_barrier(
            jnp.einsum("...ij,...jk->...ik", result, powered, precision=exact_mode)
        )
        result = result + product
        powered = jnp.einsum("...ij,...jk->...ik", powered, powered, precision=exact_mode)
        covered = covered * 2
    return result


def block_terms(unit_keys, values, decay_logarithm, strength):
    extent = unit_keys.shape[-2]
    lower = jnp.tril(jnp.ones((extent, extent), jnp.bool_))
    strict = jnp.tril(jnp.ones((extent, extent), jnp.bool_), -1)
    running = jnp.cumsum(decay_logarithm, axis=-1)
    spread = running[..., :, None] - running[..., None, :]
    within = jnp.where(lower, jnp.exp(jnp.where(lower, spread, 0.0)), 0.0)
    scaled = unit_keys * strength[..., None]
    mixing = jnp.where(
        strict,
        jnp.einsum("...id,...jd->...ij", scaled, unit_keys, precision=exact_mode) * within,
        0.0,
    )
    inverse = nilpotent_inverse(mixing)
    writes = jnp.einsum(
        "...ij,...je->...ie", inverse, values * strength[..., None], precision=exact_mode
    )
    erases = jnp.einsum(
        "...ij,...jd->...id", inverse, scaled * jnp.exp(running)[..., None], precision=exact_mode
    )
    final_log = running[..., -1]
    carried = unit_keys * jnp.exp(final_log[..., None] - running)[..., None]
    return (writes, erases, carried, final_log)


def split_blocks(array, block_count):
    shaped = array.reshape(
        array.shape[:2] + (block_count, array.shape[2] // block_count) + array.shape[3:]
    )
    return jnp.moveaxis(shaped, 2, 0)


def local_general(
    tokens,
    key_matrix,
    value_matrix,
    gate_matrix,
    head_decay_rate,
    extra_log_decay,
    next_token_query,
    next_token_key,
    next_token_value,
    next_write_strength,
    read_norm_gain,
):
    sequences, positions, _ = tokens.shape
    local_heads = head_decay_rate.shape[0]
    key_width = key_matrix.shape[1] // local_heads
    value_width = value_matrix.shape[1] // local_heads
    all_heads = gate_matrix.shape[1] // 2
    group_size = lax.axis_size("sp")
    column_share = value_width // group_size
    first_head = lax.axis_index("tp") * local_heads
    decay_cols = lax.dynamic_slice_in_dim(gate_matrix, first_head, local_heads, 1)
    strength_cols = lax.dynamic_slice_in_dim(gate_matrix, all_heads + first_head, local_heads, 1)
    gate_cols = jnp.concatenate([decay_cols, strength_cols], axis=1)
    row_count = sequences * positions
    incoming = lax.all_gather(tokens, "tp", axis=2, tiled=True)
    span_width = incoming.shape[2]
    flat_rows = incoming.reshape(row_count, span_width)
    products = lax.optimization_barrier(
        (
            jnp.dot(flat_rows, key_matrix, preferred_element_type=jnp.float32),
            jnp.dot(flat_rows, value_matrix, preferred_element_type=jnp.float32),
            jnp.dot(flat_rows, gate_cols, preferred_element_type=jnp.float32),
        )
    )
    key_sum = products[0]
    value_sum = products[1]
    gate_pre = products[2]
    key_float = lax.optimization_barrier(key_sum.astype(jnp.bfloat16)).astype(jnp.float32)
    value_float = lax.optimization_barrier(value_sum.astype(jnp.bfloat16)).astype(jnp.float32)
    unit_keys = unit_rows(
        key_float.reshape(sequences, positions, local_heads, key_width).transpose(0, 2, 1, 3)
    )
    values = value_float.reshape(sequences, positions, local_heads, value_width).transpose(
        0, 2, 1, 3
    )
    gate_projected = gate_pre.reshape(sequences, positions, 2 * local_heads).transpose(0, 2, 1)
    decay_logarithm = (
        -head_decay_rate[None, :, None] * jax.nn.softplus(gate_projected[:, :local_heads])
        + extra_log_decay
    )
    strength = jax.nn.sigmoid(gate_projected[:, local_heads:] - strength_offset)
    block_count = positions // min(64, positions)
    block_parts = block_terms(
        split_blocks(unit_keys, block_count),
        split_blocks(values, block_count),
        split_blocks(decay_logarithm, block_count),
        split_blocks(strength, block_count),
    )
    identity = jnp.zeros((sequences, local_heads, key_width, key_width), jnp.float32) + jnp.eye(
        key_width, dtype=jnp.float32
    )
    start_map = jnp.concatenate(
        [identity, jnp.zeros((sequences, local_heads, key_width, value_width), jnp.float32)],
        axis=-1,
    )

    def advance(current, block_part):
        writes, erases, carried, final_log = block_part
        padded = jnp.concatenate(
            [jnp.zeros(writes.shape[:-1] + (key_width,), jnp.float32), writes], axis=-1
        )
        removed = lax.optimization_barrier(
            jnp.einsum("shcd,shde->shce", erases, current, precision=exact_mode)
        )
        fresh = padded - removed
        added = lax.optimization_barrier(
            jnp.einsum("shcd,shce->shde", carried, fresh, precision=exact_mode)
        )
        current = current * jnp.exp(final_log)[..., None, None] + added
        return (current, None)

    local_map, _ = lax.scan(advance, start_map, block_parts)
    carry_map = local_map[..., :key_width]
    write_map = local_map[..., key_width:]
    carry_copies = jnp.broadcast_to(carry_map[None], (group_size,) + carry_map.shape)
    write_parts = jnp.moveaxis(
        write_map.reshape(sequences, local_heads, key_width, group_size, column_share), 3, 0
    )
    carries = lax.all_to_all(carry_copies, "sp", split_axis=0, concat_axis=0, tiled=True)
    write_cols = lax.all_to_all(write_parts, "sp", split_axis=0, concat_axis=0, tiled=True)

    def fold_step(current, block_map):
        moved = lax.optimization_barrier(
            jnp.einsum("shij,shje->shie", block_map[0], current, precision=exact_mode)
        )
        return (moved + block_map[1], None)

    begin_state = jnp.zeros(write_cols.shape[1:], jnp.float32)
    folded, _ = lax.scan(fold_step, begin_state, (carries, write_cols))
    query_rows = next_token_query.astype(jnp.float32).reshape(sequences, local_heads, key_width)
    unit_new = unit_rows(
        next_token_key.astype(jnp.float32).reshape(sequences, local_heads, key_width)
    )
    value_rows = next_token_value.astype(jnp.float32)
    key_read = jnp.einsum("shd,shde->she", unit_new, folded, precision=exact_mode)
    query_read = jnp.einsum("shd,shde->she", query_rows, folded, precision=exact_mode)
    intersection = jnp.sum(query_rows * unit_new, axis=-1)
    read_raw = query_read + (next_write_strength * intersection)[..., None] * (
        value_rows - key_read
    )
    square_total = lax.psum(jnp.sum(read_raw * read_raw, axis=-1, keepdims=True), "sp")
    first_read = read_raw * lax.rsqrt(square_total / DV + 1e-06) * read_norm_gain
    return (folded.astype(jnp.bfloat16), first_read.astype(jnp.bfloat16))


def short_dot(left, right, contract=((1,), (0,))):
    return lax.dot_general(
        left.astype(jnp.bfloat16),
        right.astype(jnp.bfloat16),
        (contract, ((), ())),
        preferred_element_type=jnp.float32,
    )


def three_terms(x):
    first = x.astype(jnp.bfloat16)
    rest = x - first.astype(jnp.float32)
    second = rest.astype(jnp.bfloat16)
    third = (rest - second.astype(jnp.float32)).astype(jnp.bfloat16)
    return first, second, third


def close_dot(left, right):
    left, right = three_terms(left)[:2], three_terms(right)[:2]
    return (
        short_dot(left[0], right[0]) + short_dot(left[0], right[1]) + short_dot(left[1], right[0])
    )


def softplus(x):
    return jnp.maximum(x, 0.0) + jnp.log1p(jnp.exp(-jnp.abs(x)))


def grid_mask(rows, cols, rule):
    row = lax.broadcasted_iota(jnp.int32, (rows, cols), 0)
    col = lax.broadcasted_iota(jnp.int32, (rows, cols), 1)
    return rule(row, col)


def compose(late, early):
    late_map, late_write, late_keep = late
    early_map, early_write, early_keep = early
    width = early_map.shape[1]
    moved = short_dot(late_map, jnp.concatenate([early_map, early_write], axis=1))
    return (
        late_keep * early_map + early_keep * late_map - moved[:, :width],
        late_keep * early_write + late_write - moved[:, width:],
        late_keep * early_keep,
    )


def compose_write(late, early_write):
    late_map, late_write, late_keep = late
    return late_keep * early_write + late_write - short_dot(late_map, early_write)


def fused_kernel(
    sp_size,
    tp_size,
    rate_hbm,
    next_strength_hbm,
    tokens_ref,
    key_ref,
    value_ref,
    gate_hbm,
    extra_hbm,
    query_hbm,
    new_key_hbm,
    new_value_hbm,
    gain_hbm,
    state_ref,
    read_ref,
    rate_ref,
    next_strength_ref,
    gathered,
    key_w,
    value_w,
    gate_ref,
    gate_own,
    extra_ref,
    query_ref,
    new_key_ref,
    new_value_ref,
    gain_ref,
    key_acc,
    value_acc,
    gate_acc,
    key_out,
    key_in,
    value_out,
    value_in,
    side_out,
    side_in,
    state_out,
    row_out,
    row_in,
    load_sem,
    weight_sem,
    gather_recv,
    gather_send,
    swap_recv,
    swap_send,
    last_recv,
    last_send,
    above_sem,
    peers_sem,
):
    sequences, positions, depth = tokens_ref.shape
    local_heads = extra_ref.shape[1]
    key_width = key_acc.shape[1] // local_heads
    value_width = value_acc.shape[1] // local_heads
    share = value_width // sp_size
    all_heads = gate_ref.shape[0] // 2
    chips = tp_size // CORES
    me = lax.axis_index("sp")
    spot = lax.axis_index("tp")
    chip = spot // CORES
    core = spot % CORES
    partner = chip * CORES + (1 - core)
    half = positions // 2
    units = [(s, part * half, half) for s in range(sequences) for part in range(2)]
    last_unit = len(units) - 1
    batches = [(0, 0, positions, (0, 1)), (1, 0, half, (2,)), (1, half, half, (3,))]
    others = [sp_size - 1 - me, me + 1 - 2 * (me % 2), (me + 2) % sp_size]

    loads = [
        pltpu.make_async_copy(
            tokens_ref.at[s],
            gathered.at[spot, pl.ds(s * positions, positions)],
            load_sem.at[s],
        )
        for s in range(sequences)
    ]
    for load in loads:
        load.start()

    barrier = pltpu.get_barrier_semaphore()
    pl.semaphore_signal(barrier, inc=1, device_id={"tp": partner}, device_id_type=MESH)

    @pl.when(chip < chips - 1)
    def _():
        pl.semaphore_signal(barrier, inc=1, device_id={"tp": spot + CORES}, device_id_type=MESH)

    for other in range(1, sp_size):

        @pl.when(me < other)
        def _(other=other):
            pl.semaphore_signal(barrier, inc=1, device_id={"sp": other}, device_id_type=MESH)

    weights = [
        pltpu.make_async_copy(key_ref, key_w, weight_sem.at[0]),
        pltpu.make_async_copy(value_ref, value_w, weight_sem.at[1]),
        pltpu.make_async_copy(gate_hbm, gate_ref, weight_sem.at[2]),
        pltpu.make_async_copy(extra_hbm, extra_ref, weight_sem.at[3]),
        pltpu.make_async_copy(query_hbm, query_ref, weight_sem.at[4]),
        pltpu.make_async_copy(new_key_hbm, new_key_ref, weight_sem.at[5]),
        pltpu.make_async_copy(new_value_hbm, new_value_ref, weight_sem.at[6]),
        pltpu.make_async_copy(gain_hbm, gain_ref, weight_sem.at[7]),
        pltpu.make_async_copy(rate_hbm, rate_ref, weight_sem.at[8]),
        pltpu.make_async_copy(next_strength_hbm, next_strength_ref, weight_sem.at[9]),
    ]
    for weight in weights:
        weight.start()
    pl.semaphore_wait(barrier, jnp.where(chip > 0, 1, 0) + 1 + me)

    @pl.when(chip > 0)
    def _():
        pl.semaphore_signal(above_sem, inc=1, device_id={"tp": spot - CORES}, device_id_type=MESH)

    for other in range(sp_size - 1):

        @pl.when(other < me)
        def _(other=other):
            pl.semaphore_signal(peers_sem, inc=1, device_id={"sp": other}, device_id_type=MESH)

    def crossing(block, send, recv, axis, target):
        return pltpu.make_async_remote_copy(
            src_ref=block[0],
            dst_ref=block[1],
            send_sem=send,
            recv_sem=recv,
            device_id={axis: target},
            device_id_type=MESH,
        )

    def piece(origin, u, way, target, own=False):
        s, low, count = units[u]
        block = gathered.at[origin, pl.ds(s * positions + low, count)]
        kind = 2 * way + (u == last_unit) + (way == 2 and u == last_unit and own)
        return crossing(
            (block, block), gather_send.at[kind], gather_recv.at[origin, u], "tp", target
        )

    def settle(kind, blocks, count):
        block = gathered.at[pl.ds(0, blocks), pl.ds(0, count)]
        crossing(
            (block, block), gather_send.at[kind], gather_recv.at[0, 0], "tp", partner
        ).wait_send()

    for load in loads:
        load.wait()

    def hub(a_chip):
        return jnp.where((a_chip == 0) | (a_chip == chips - 1), 0, 1)

    for u in range(last_unit):

        @pl.when(chip > 0)
        def _(u=u):
            piece(spot, u, 1, spot - CORES).start()

    for u in [last_unit, *range(last_unit)]:
        piece(spot, u, 2, partner, own=True).start()

    @pl.when(chip < chips - 1)
    def _():
        pl.semaphore_wait(above_sem, 1)

    for u in range(last_unit):

        @pl.when(chip < chips - 1)
        def _(u=u):
            piece(spot, u, 0, spot + CORES).start()

    def send_last(way):
        onward = chip + (1 if way == 0 else -1)
        for c in range(CORES):
            piece(chip * CORES + c, last_unit, way, onward * CORES + hub(onward)).start()

    @pl.when(core == 1)
    def _():
        piece(partner, last_unit, 2, partner).wait_recv()

        @pl.when(chip == chips - 1)
        def _():
            send_last(1)

        @pl.when(chip == 0)
        def _():
            send_last(0)

    key_acc[...] = jnp.zeros_like(key_acc)
    value_acc[...] = jnp.zeros_like(value_acc)
    gate_acc[...] = jnp.zeros_like(gate_acc)
    side_out[...] = jnp.zeros_like(side_out)

    def add_in(rows, span, batch):
        s, low, count, parts = batches[batch]
        cut = slice(s * positions + low, s * positions + low + count)
        key_acc[cut] += jnp.dot(rows, key_w[span, :], preferred_element_type=jnp.float32)
        value_acc[cut] += jnp.dot(rows, value_w[span, :], preferred_element_type=jnp.float32)
        gates = lax.dot_general(
            gate_own[:, span],
            rows,
            (((1,), (1,)), ((), ())),
            preferred_element_type=jnp.float32,
        )
        gate_acc[s, :, low : low + count] += gates

    def take_one(block, batch):
        s, low, count, _ = batches[batch]
        span = pl.ds(pl.multiple_of(block * depth, depth), depth)
        add_in(gathered[block, s * positions + low : s * positions + low + count], span, batch)

    def take_chip(origin_chip, batch):
        s, low, count, _ = batches[batch]
        width = CORES * depth
        span = pl.ds(pl.multiple_of(origin_chip * width, width), width)
        rows = jnp.concatenate(
            [
                gathered[
                    origin_chip * CORES + c, s * positions + low : s * positions + low + count
                ]
                for c in range(CORES)
            ],
            axis=1,
        )
        add_in(rows, span, batch)

    first = spot * local_heads

    def prepare():
        for weight in weights:
            weight.wait()
        chooser = grid_mask(
            2 * local_heads,
            2 * all_heads,
            lambda r, c: c
            == jnp.where(r < local_heads, first + r, all_heads + first + r - local_heads),
        ).astype(jnp.float32)
        gate_own[...] = short_dot(chooser, gate_ref[...]).astype(jnp.bfloat16)
        placer = grid_mask(share, value_width, lambda r, c: c == me * share + r)
        for s in range(sequences):
            new_value = short_dot(new_value_ref[s], placer.astype(jnp.float32))
            for h in range(local_heads):
                side_out[h, s, 0, 2:3, :] = new_value[h : h + 1, :]

    def own(batch):
        for u in batches[batch][3]:
            if u == last_unit:

                @pl.when(core == 0)
                def _(u=u):
                    piece(partner, u, 2, partner).wait_recv()

            else:
                piece(partner, u, 2, partner).wait_recv()
        take_chip(chip, batch)

    def relay(distance, u):
        lanes = range(CORES) if u == last_unit else [core]
        for lane in lanes:
            relay_lane(distance, u, lane)

    def relay_lane(distance, u, lane):
        for way, step in ((1, 1), (0, -1)):
            origin_chip = chip + step * distance
            origin = origin_chip * CORES + lane
            present = (origin_chip >= 0) & (origin_chip < chips)
            if u == last_unit:
                present = present & (core == hub(chip))
            onward = chip - step
            beyond = (onward >= 0) & (onward < chips)
            target = onward * CORES + (hub(onward) if u == last_unit else core)

            @pl.when(present)
            def _(way=way, origin_chip=origin_chip, origin=origin, target=target, beyond=beyond):
                piece(origin, u, way, partner).wait_recv()

                @pl.when(beyond)
                def _():
                    piece(origin, u, way, target).start()

                piece(origin, u, 2, partner).start()
                if u == 1:

                    @pl.when(
                        beyond & (core == 1) & (origin_chip == (0 if way == 0 else chips - 1))
                    )
                    def _():
                        send_last(way)

    def both_sides(distance, act):
        def one_side(side, carry):
            origin_chip = chip + (2 * side - 1) * distance

            @pl.when((origin_chip >= 0) & (origin_chip < chips))
            def _():
                act(origin_chip)

            return carry

        lax.fori_loop(0, 2, one_side, 0)

    def absorb(distance, batch):
        def act(origin_chip):
            for u in batches[batch][3]:
                if u == last_unit:

                    @pl.when(core != hub(chip))
                    def _(u=u):
                        for c in range(CORES):
                            piece(origin_chip * CORES + c, u, 2, partner).wait_recv()

                else:
                    piece(origin_chip * CORES + 1 - core, u, 2, partner).wait_recv()
            take_chip(origin_chip, batch)

        both_sides(distance, act)

    def absorb_last_lane(distance, lane):
        relay_lane(distance, last_unit, lane)

        def act(origin_chip):
            block = origin_chip * CORES + lane

            @pl.when(core != hub(chip))
            def _():
                piece(block, last_unit, 2, partner).wait_recv()

            take_one(block, len(batches) - 1)

        both_sides(distance, act)

    def swap(n, slot, target):
        s, low, count, _ = batches[slot]
        if n == 0:
            block = (
                (side_out.at[target, s], side_in.at[me, s])
                if slot == 0
                else (side_out.at[target, s, slot - 1], side_in.at[me, s, slot - 1])
            )
        else:
            source, sink = ((key_out, key_in), (value_out, value_in))[n - 1]
            block = source.at[target, s, pl.ds(low, count)], sink.at[me, s, pl.ds(low, count)]
        return crossing(block, swap_send.at[n], swap_recv.at[n, s], "sp", target)

    def swapped(n, s):
        if n == 0:
            block = side_in.at[pl.ds(0, sp_size - 1), s]
        else:
            block = (key_in, value_in)[n - 1].at[pl.ds(0, sp_size - 1), s]
        crossing((block, block), swap_send.at[n], swap_recv.at[n, s], "sp", others[0]).wait_recv()

    def hand_out(slot):
        s, low, count, _ = batches[slot]
        cut = slice(s * positions + low, s * positions + low + count)
        part = max(slot - 1, 0)
        gates = gate_acc[s, :, low : low + count]
        extra = extra_ref[s, :, low : low + count]
        for h in range(local_heads):
            side_out[h, s, part, 0:1, low : low + count] = (
                -rate_ref[h] * softplus(gates[h : h + 1]) + extra[h : h + 1, :]
            )
            side_out[h, s, part, 1:2, low : low + count] = jax.nn.sigmoid(
                gates[local_heads + h : local_heads + h + 1] - strength_offset
            )
        for other in others:
            swap(0, slot, other).start()
        for h in range(local_heads):
            key_out[h, s, low : low + count] = key_acc[
                cut, h * key_width : (h + 1) * key_width
            ].astype(jnp.bfloat16)
        for other in others:
            swap(1, slot, other).start()
        for h in range(local_heads):
            value_out[h, s, low : low + count] = value_acc[
                cut, h * value_width : (h + 1) * value_width
            ].astype(jnp.bfloat16)
        for other in others:
            swap(2, slot, other).start()
        if slot == 0:
            side_in[me, s] = side_out[me, s]
        else:
            side_in[me, s, part] = side_out[me, s, part]
        key_in[me, s, low : low + count] = key_out[me, s, low : low + count]
        value_in[me, s, low : low + count] = value_out[me, s, low : low + count]

    far = chips - 1
    last_batch = len(batches) - 1
    steps = {1: [(1, 0), (1, 1), (1, 2)]} if far > 1 else {}
    for distance in range(2, far):
        steps[distance] = [(distance, 0), (distance, 1), (distance, 2)]
    work = [(own, (0,)), (own, (1,)), (own, (2,))]
    prepared = False
    for distance in range(1, far):
        for event in steps[distance]:
            relay(*event)
            if not prepared:
                prepare()
                prepared = True
            if work:
                act, operands = work.pop(0)
                act(*operands)
            if event[1] == 1:
                work.insert(0, (absorb, (distance, 0)))
            if event[1] == 2:
                work.append((absorb, (distance, 1)))
    if not prepared:
        prepare()
    for act, operands in [w for w in work if w[0] is own]:
        act(*operands)
    work = [w for w in work if w[0] is absorb]
    relay(far, 0)
    for act, operands in [w for w in work if w[1][1] == 0]:
        act(*operands)
    work = [w for w in work if w[1][1] != 0]
    relay(far, 1)
    absorb(far, 0)

    @pl.when(me < sp_size - 1)
    def _():
        pl.semaphore_wait(peers_sem, sp_size - 1 - me)

    hand_out(0)
    if far > 1:
        relay(1, last_unit)
    for act, operands in work:
        act(*operands)
    relay(far, 2)
    if far > 1:
        absorb(1, last_batch)
    absorb(far, 1)
    hand_out(1)
    pending = None
    for distance in range(2, far):
        relay(distance, last_unit)
        if pending is not None:
            absorb(*pending)
        pending = (distance, last_batch)
    if pending is not None:
        absorb(*pending)
    for lane in range(CORES):
        absorb_last_lane(far, lane)
    hand_out(2)

    side_rows = side_in.shape[3]
    upto = grid_mask(positions, positions, lambda r, c: r <= c).astype(jnp.float32)
    down = grid_mask(positions, positions, lambda r, c: c <= r).astype(jnp.float32)
    lanes = pl.ds(pl.multiple_of(me * key_width, key_width), key_width)
    queries = query_ref[:, lanes].astype(jnp.float32)
    new_keys = new_key_ref[:, lanes].astype(jnp.float32)
    new_keys = new_keys * lax.rsqrt(jnp.sum(new_keys * new_keys, axis=-1, keepdims=True) + 1e-06)
    meets = jnp.sum(queries * new_keys, axis=-1, keepdims=True)
    weight_of_new = [next_strength_ref[s, me] * meets[s : s + 1] for s in range(sequences)]
    probes = [queries[s : s + 1] - weight_of_new[s] * new_keys[s : s + 1] for s in range(sequences)]

    def block_maps(s):
        count = positions
        eye = grid_mask(count, count, lambda r, c: r == c).astype(jnp.float32)
        strict = grid_mask(count, count, lambda r, c: r > c)
        swapped(0, s)
        swapped(1, s)
        side = jnp.concatenate(
            [side_in[b, s, 0] + side_in[b, s, 1] for b in range(sp_size)], axis=0
        )
        new_value = sum(side[b * side_rows + 2 : b * side_rows + 3] for b in range(sp_size))
        terms = three_terms(side)
        rows = sum(short_dot(term, upto) for term in terms)
        columns = sum(short_dot(down, term, ((1,), (1,))) for term in terms)
        parts = []
        for b in range(sp_size):
            line = b * side_rows
            row = rows[line : line + 1, :]
            strength = side[line + 1 : line + 2, :]
            col = jnp.broadcast_to(columns[:, line : line + 1], (count, count))
            final_log = row[:, count - 1 : count]
            keys = key_in[b, s].astype(jnp.float32)
            keys = keys * lax.rsqrt(jnp.sum(keys * keys, axis=-1, keepdims=True) + 1e-06)
            within = jnp.exp(jnp.where(strict, col - row, 0.0)) * -strength
            power = jnp.where(strict, short_dot(keys, keys, ((1,), (1,))) * within, 0.0)
            erased = (keys * jnp.exp(col)).astype(jnp.bfloat16)
            carried = (keys.T * (jnp.exp(final_log - row) * strength)).astype(jnp.bfloat16)
            parts.append([eye + power, power, erased, carried, jnp.exp(final_log)])
        for part in parts:
            part[1] = short_dot(part[1], part[1])
        covered = 2
        while covered < count:
            for part in parts:
                if covered * 2 < count:
                    both = short_dot(part[1], jnp.concatenate([part[0], part[1]], axis=1))
                    part[0] = part[0] + both[:, :count]
                    part[1] = both[:, count:]
                else:
                    part[0] = part[0] + short_dot(part[1], part[0])
            covered = covered * 2
        swapped(2, s)
        solved = []
        for b, part in enumerate(parts):
            sources = jnp.concatenate([part[2], value_in[b, s]], axis=1)
            solved.append(short_dot(part[0], sources))
        maps = []
        for part, both in zip(parts, solved):
            both = short_dot(part[3], both)
            maps.append((both[:, :key_width], both[:, key_width:], part[4]))
        return maps, new_value

    def final(n, s, target):
        block = (
            (state_out.at[target, s], state_ref.at[s, me]),
            (row_out.at[target, s], row_in.at[me, s]),
        )[n]
        return crossing(block, last_send.at[n], last_recv.at[n], "sp", target)

    def finish(s, maps, new_value):
        while len(maps) > 2:
            maps = [compose(maps[i + 1], maps[i]) for i in range(0, len(maps), 2)]
        (_, first_write, _), (late_map, late_write, late_keep) = maps
        state = compose_write(maps[1], first_write)
        probe = jnp.where(s == 0, probes[0], probes[1])
        probe = jnp.broadcast_to(probe, (8, key_width))
        new_weight = jnp.where(s == 0, weight_of_new[0], weight_of_new[1])
        passed = close_dot(probe, jnp.concatenate([late_write, late_map], axis=1))
        onto_first = late_keep * probe - passed[:, value_width:]
        raw = close_dot(onto_first, first_write) + passed[:, :value_width]
        turned = state.T.astype(jnp.bfloat16)
        for j in range(sp_size):
            state_out[j, s] = turned[j * share : (j + 1) * share, :]
        for other in others:
            final(0, s, other).start()
        raw = raw[0:1] + new_weight * new_value
        raw = raw * lax.rsqrt(jnp.sum(raw * raw, axis=-1, keepdims=True) / value_width + 1e-06)
        for j in range(sp_size):
            turn = j * share
            row_out[j, s, 0:1, :] = (
                jnp.concatenate([raw[:, turn:], raw[:, :turn]], axis=1) if j else raw
            )
        for other in others:
            final(1, s, other).start()
        state_ref[s, me] = state_out[me, s]
        row_in[me, s] = row_out[me, s]

    row_out[...] = jnp.zeros_like(row_out)

    def solve(s, carry):
        finish(s, *block_maps(s))
        return carry

    lax.fori_loop(0, sequences, solve, 0)

    whole, part = last_unit * half, half
    settle(4, chips, whole)
    settle(6, 1, part)

    @pl.when(core == hub(chip))
    def _():
        settle(5, CORES * far, part)

    for c in range(chips):
        for way, sent in ((0, c + 1), (1, chips - c)):
            if sent < chips:

                @pl.when(chip == c)
                def _(way=way, sent=sent):
                    settle(2 * way, sent, whole)

                @pl.when((chip == c) & (core == 1))
                def _(way=way, sent=sent):
                    settle(2 * way + 1, CORES * sent, part)

    peers = pl.ds(0, sp_size - 1)
    for n, sent in enumerate((side_out, key_out, value_out)):
        block = sent.at[peers]
        crossing((block, block), swap_send.at[n], swap_recv.at[n, 0], "sp", others[0]).wait_send()
    for n, sent in enumerate((state_out, row_out)):
        block = sent.at[peers]
        crossing((block, block), last_send.at[n], last_recv.at[n], "sp", others[0]).wait_send()
    block = row_in.at[peers]
    crossing((block, block), last_send.at[1], last_recv.at[1], "sp", others[0]).wait_recv()
    for s in range(sequences):
        rows = jnp.concatenate([row_in[i, s, 0:1, :share] for i in range(sp_size)], axis=0)
        read_ref[s] = (rows * gain_ref[...].reshape(1, share)).astype(jnp.bfloat16)
    block = state_ref.at[:, peers]
    crossing((block, block), last_send.at[0], last_recv.at[0], "sp", others[0]).wait_recv()


def place_kernel(state_ref, read_ref, state_hbm, read_hbm, sem):
    copies = [
        pltpu.make_async_copy(state_ref, state_hbm, sem.at[0]),
        pltpu.make_async_copy(read_ref, read_hbm, sem.at[1]),
    ]
    for copy in copies:
        copy.start()
    for copy in copies:
        copy.wait()


def local_fused(
    tokens,
    key_matrix,
    value_matrix,
    gate_matrix,
    head_decay_rate,
    extra_log_decay,
    next_token_query,
    next_token_key,
    next_token_value,
    next_write_strength,
    read_norm_gain,
):
    sequences, positions, depth = tokens.shape
    local_heads = head_decay_rate.shape[0]
    sp_size = lax.axis_size("sp")
    tp_size = lax.axis_size("tp")
    key_total = key_matrix.shape[1]
    value_total = value_matrix.shape[1]
    key_width = key_total // local_heads
    value_width = value_total // local_heads
    share = value_width // sp_size
    rows = sequences * positions
    units = 2 * sequences
    vmem = pl.BlockSpec(memory_space=pltpu.VMEM)
    anywhere = pl.BlockSpec(memory_space=pl.ANY)
    dma = pltpu.SemaphoreType.DMA
    held = (sp_size, sequences, positions)
    turned, read = pl.pallas_call(
        functools.partial(fused_kernel, sp_size, tp_size),
        out_shape=(
            pltpu.VMEM((sequences, local_heads, share, key_width), jnp.bfloat16),
            pltpu.VMEM((sequences, local_heads, share), jnp.bfloat16),
        ),
        in_specs=[anywhere] * 11,
        out_specs=(vmem, vmem),
        scratch_shapes=[
            pltpu.SMEM(head_decay_rate.shape, jnp.float32),
            pltpu.SMEM(next_write_strength.shape, jnp.float32),
            pltpu.VMEM((tp_size, rows, depth), jnp.bfloat16),
            pltpu.VMEM(key_matrix.shape, jnp.bfloat16),
            pltpu.VMEM(value_matrix.shape, jnp.bfloat16),
            pltpu.VMEM(gate_matrix.shape[::-1], jnp.bfloat16),
            pltpu.VMEM((2 * local_heads, gate_matrix.shape[0]), jnp.bfloat16),
            pltpu.VMEM(extra_log_decay.shape, jnp.float32),
            pltpu.VMEM(next_token_query.shape, jnp.bfloat16),
            pltpu.VMEM(next_token_key.shape, jnp.bfloat16),
            pltpu.VMEM(next_token_value.shape, jnp.bfloat16),
            pltpu.VMEM(read_norm_gain.shape, jnp.float32),
            pltpu.VMEM((rows, key_total), jnp.float32),
            pltpu.VMEM((rows, value_total), jnp.float32),
            pltpu.VMEM((sequences, 2 * local_heads, positions), jnp.float32),
            pltpu.VMEM((*held, key_width), jnp.bfloat16),
            pltpu.VMEM((*held, key_width), jnp.bfloat16),
            pltpu.VMEM((*held, value_width), jnp.bfloat16),
            pltpu.VMEM((*held, value_width), jnp.bfloat16),
            pltpu.VMEM((sp_size, sequences, 2, 8, positions), jnp.float32),
            pltpu.VMEM((sp_size, sequences, 2, 8, positions), jnp.float32),
            pltpu.VMEM((sp_size, sequences, share, key_width), jnp.bfloat16),
            pltpu.VMEM((sp_size, sequences, 8, value_width), jnp.float32),
            pltpu.VMEM((sp_size, sequences, 8, value_width), jnp.float32),
            dma((sequences,)),
            dma((10,)),
            dma((tp_size, units)),
            dma((7,)),
            dma((3, sequences)),
            dma((3,)),
            dma((2,)),
            dma((2,)),
            pltpu.SemaphoreType.REGULAR,
            pltpu.SemaphoreType.REGULAR,
        ],
        compiler_params=pltpu.CompilerParams(
            collective_id=0, has_side_effects=True
        ),
    )(
        head_decay_rate,
        next_write_strength,
        tokens,
        key_matrix,
        value_matrix,
        gate_matrix.T,
        extra_log_decay,
        next_token_query,
        next_token_key,
        next_token_value,
        read_norm_gain,
    )
    turned, read = pl.pallas_call(
        place_kernel,
        out_shape=tuple(jax.ShapeDtypeStruct(a.shape, a.dtype) for a in (turned, read)),
        in_specs=[vmem, vmem],
        out_specs=(anywhere, anywhere),
        scratch_shapes=[dma((2,))],
    )(*(pltpu.with_memory_space_constraint(a, pltpu.VMEM) for a in (turned, read)))
    return jnp.swapaxes(turned, 2, 3), read


def local(*arguments):
    tokens, key_matrix, value_matrix = arguments[:3]
    sequences, positions, _ = tokens.shape
    local_heads = arguments[4].shape[0]
    sp_size = lax.axis_size("sp")
    fits = (
        local_heads == sp_size
        and sp_size == 4
        and sequences == 2
        and 2 * local_heads == 8
        and lax.axis_size("tp") % CORES == 0
        and lax.axis_size("tp") > CORES
        and positions == key_matrix.shape[1] // local_heads
        and positions == value_matrix.shape[1] // local_heads
        and positions % 128 == 0
    )
    return local_fused(*arguments) if fits else local_general(*arguments)


def solution(mesh):
    in_specs = (
        P(None, "sp", "tp"),
        P(None, "tp"),
        P(None, "tp"),
        P(),
        P("tp"),
        P(None, "tp", "sp"),
        P(None, "tp"),
        P(None, "tp"),
        P(None, "tp", "sp"),
        P(None, "tp"),
        P("sp"),
    )
    out_specs = (P(None, "tp", None, "sp"), P(None, "tp", "sp"))
    return jax.shard_map(local, mesh=mesh, in_specs=in_specs, out_specs=out_specs, check_vma=False)
```

```python
import functools

import jax
import jax.numpy as jnp
from jax import lax
from jax.experimental import pallas as pl
from jax.experimental.pallas import tpu as pltpu
from jax.sharding import PartitionSpec as P

DV = 128
CORES = 2
MESH = pl.DeviceIdType.MESH


exact_mode = lax.Precision.HIGHEST
strength_offset = 5.0


def unit_rows(matrix):
    return matrix * lax.rsqrt(jnp.sum(matrix * matrix, axis=-1, keepdims=True) + 1e-06)


def nilpotent_inverse(mixing):
    extent = mixing.shape[-1]
    result = jnp.zeros_like(mixing) + jnp.eye(extent, dtype=jnp.float32)
    powered = -mixing
    covered = 1
    while covered < extent:
        product = lax.optimization_barrier(
            jnp.einsum("...ij,...jk->...ik", result, powered, precision=exact_mode)
        )
        result = result + product
        powered = jnp.einsum("...ij,...jk->...ik", powered, powered, precision=exact_mode)
        covered = covered * 2
    return result


def block_terms(unit_keys, values, decay_logarithm, strength):
    extent = unit_keys.shape[-2]
    lower = jnp.tril(jnp.ones((extent, extent), jnp.bool_))
    strict = jnp.tril(jnp.ones((extent, extent), jnp.bool_), -1)
    running = jnp.cumsum(decay_logarithm, axis=-1)
    spread = running[..., :, None] - running[..., None, :]
    within = jnp.where(lower, jnp.exp(jnp.where(lower, spread, 0.0)), 0.0)
    scaled = unit_keys * strength[..., None]
    mixing = jnp.where(
        strict,
        jnp.einsum("...id,...jd->...ij", scaled, unit_keys, precision=exact_mode) * within,
        0.0,
    )
    inverse = nilpotent_inverse(mixing)
    writes = jnp.einsum(
        "...ij,...je->...ie", inverse, values * strength[..., None], precision=exact_mode
    )
    erases = jnp.einsum(
        "...ij,...jd->...id", inverse, scaled * jnp.exp(running)[..., None], precision=exact_mode
    )
    final_log = running[..., -1]
    carried = unit_keys * jnp.exp(final_log[..., None] - running)[..., None]
    return (writes, erases, carried, final_log)


def split_blocks(array, block_count):
    shaped = array.reshape(
        array.shape[:2] + (block_count, array.shape[2] // block_count) + array.shape[3:]
    )
    return jnp.moveaxis(shaped, 2, 0)


def local_general(
    tokens,
    key_matrix,
    value_matrix,
    gate_matrix,
    head_decay_rate,
    extra_log_decay,
    next_token_query,
    next_token_key,
    next_token_value,
    next_write_strength,
    read_norm_gain,
):
    sequences, positions, _ = tokens.shape
    local_heads = head_decay_rate.shape[0]
    key_width = key_matrix.shape[1] // local_heads
    value_width = value_matrix.shape[1] // local_heads
    all_heads = gate_matrix.shape[1] // 2
    group_size = lax.axis_size("sp")
    column_share = value_width // group_size
    first_head = lax.axis_index("tp") * local_heads
    decay_cols = lax.dynamic_slice_in_dim(gate_matrix, first_head, local_heads, 1)
    strength_cols = lax.dynamic_slice_in_dim(gate_matrix, all_heads + first_head, local_heads, 1)
    gate_cols = jnp.concatenate([decay_cols, strength_cols], axis=1)
    row_count = sequences * positions
    incoming = lax.all_gather(tokens, "tp", axis=2, tiled=True)
    span_width = incoming.shape[2]
    flat_rows = incoming.reshape(row_count, span_width)
    products = lax.optimization_barrier(
        (
            jnp.dot(flat_rows, key_matrix, preferred_element_type=jnp.float32),
            jnp.dot(flat_rows, value_matrix, preferred_element_type=jnp.float32),
            jnp.dot(flat_rows, gate_cols, preferred_element_type=jnp.float32),
        )
    )
    key_sum = products[0]
    value_sum = products[1]
    gate_pre = products[2]
    key_float = lax.optimization_barrier(key_sum.astype(jnp.bfloat16)).astype(jnp.float32)
    value_float = lax.optimization_barrier(value_sum.astype(jnp.bfloat16)).astype(jnp.float32)
    unit_keys = unit_rows(
        key_float.reshape(sequences, positions, local_heads, key_width).transpose(0, 2, 1, 3)
    )
    values = value_float.reshape(sequences, positions, local_heads, value_width).transpose(
        0, 2, 1, 3
    )
    gate_projected = gate_pre.reshape(sequences, positions, 2 * local_heads).transpose(0, 2, 1)
    decay_logarithm = (
        -head_decay_rate[None, :, None] * jax.nn.softplus(gate_projected[:, :local_heads])
        + extra_log_decay
    )
    strength = jax.nn.sigmoid(gate_projected[:, local_heads:] - strength_offset)
    block_count = positions // min(64, positions)
    block_parts = block_terms(
        split_blocks(unit_keys, block_count),
        split_blocks(values, block_count),
        split_blocks(decay_logarithm, block_count),
        split_blocks(strength, block_count),
    )
    identity = jnp.zeros((sequences, local_heads, key_width, key_width), jnp.float32) + jnp.eye(
        key_width, dtype=jnp.float32
    )
    start_map = jnp.concatenate(
        [identity, jnp.zeros((sequences, local_heads, key_width, value_width), jnp.float32)],
        axis=-1,
    )

    def advance(current, block_part):
        writes, erases, carried, final_log = block_part
        padded = jnp.concatenate(
            [jnp.zeros(writes.shape[:-1] + (key_width,), jnp.float32), writes], axis=-1
        )
        removed = lax.optimization_barrier(
            jnp.einsum("shcd,shde->shce", erases, current, precision=exact_mode)
        )
        fresh = padded - removed
        added = lax.optimization_barrier(
            jnp.einsum("shcd,shce->shde", carried, fresh, precision=exact_mode)
        )
        current = current * jnp.exp(final_log)[..., None, None] + added
        return (current, None)

    local_map, _ = lax.scan(advance, start_map, block_parts)
    carry_map = local_map[..., :key_width]
    write_map = local_map[..., key_width:]
    carry_copies = jnp.broadcast_to(carry_map[None], (group_size,) + carry_map.shape)
    write_parts = jnp.moveaxis(
        write_map.reshape(sequences, local_heads, key_width, group_size, column_share), 3, 0
    )
    carries = lax.all_to_all(carry_copies, "sp", split_axis=0, concat_axis=0, tiled=True)
    write_cols = lax.all_to_all(write_parts, "sp", split_axis=0, concat_axis=0, tiled=True)

    def fold_step(current, block_map):
        moved = lax.optimization_barrier(
            jnp.einsum("shij,shje->shie", block_map[0], current, precision=exact_mode)
        )
        return (moved + block_map[1], None)

    begin_state = jnp.zeros(write_cols.shape[1:], jnp.float32)
    folded, _ = lax.scan(fold_step, begin_state, (carries, write_cols))
    query_rows = next_token_query.astype(jnp.float32).reshape(sequences, local_heads, key_width)
    unit_new = unit_rows(
        next_token_key.astype(jnp.float32).reshape(sequences, local_heads, key_width)
    )
    value_rows = next_token_value.astype(jnp.float32)
    key_read = jnp.einsum("shd,shde->she", unit_new, folded, precision=exact_mode)
    query_read = jnp.einsum("shd,shde->she", query_rows, folded, precision=exact_mode)
    intersection = jnp.sum(query_rows * unit_new, axis=-1)
    read_raw = query_read + (next_write_strength * intersection)[..., None] * (
        value_rows - key_read
    )
    square_total = lax.psum(jnp.sum(read_raw * read_raw, axis=-1, keepdims=True), "sp")
    first_read = read_raw * lax.rsqrt(square_total / DV + 1e-06) * read_norm_gain
    return (folded.astype(jnp.bfloat16), first_read.astype(jnp.bfloat16))


def short_dot(left, right, contract=((1,), (0,))):
    return lax.dot_general(
        left.astype(jnp.bfloat16),
        right.astype(jnp.bfloat16),
        (contract, ((), ())),
        preferred_element_type=jnp.float32,
    )


def three_terms(x):
    first = x.astype(jnp.bfloat16)
    rest = x - first.astype(jnp.float32)
    second = rest.astype(jnp.bfloat16)
    third = (rest - second.astype(jnp.float32)).astype(jnp.bfloat16)
    return first, second, third


def close_dot(left, right):
    left, right = three_terms(left)[:2], three_terms(right)[:2]
    return (
        short_dot(left[0], right[0]) + short_dot(left[0], right[1]) + short_dot(left[1], right[0])
    )


def softplus(x):
    return jnp.maximum(x, 0.0) + jnp.log1p(jnp.exp(-jnp.abs(x)))


def grid_mask(rows, cols, rule):
    row = lax.broadcasted_iota(jnp.int32, (rows, cols), 0)
    col = lax.broadcasted_iota(jnp.int32, (rows, cols), 1)
    return rule(row, col)


def compose(late, early):
    late_map, late_write, late_keep = late
    early_map, early_write, early_keep = early
    width = early_map.shape[1]
    moved = short_dot(late_map, jnp.concatenate([early_map, early_write], axis=1))
    return (
        late_keep * early_map + early_keep * late_map - moved[:, :width],
        late_keep * early_write + late_write - moved[:, width:],
        late_keep * early_keep,
    )


def compose_write(late, early_write):
    late_map, late_write, late_keep = late
    return late_keep * early_write + late_write - short_dot(late_map, early_write)


def fused_kernel(
    sp_size,
    tp_size,
    rate_hbm,
    next_strength_hbm,
    tokens_ref,
    key_ref,
    value_ref,
    gate_hbm,
    extra_hbm,
    query_hbm,
    new_key_hbm,
    new_value_hbm,
    gain_hbm,
    state_ref,
    read_ref,
    rate_ref,
    next_strength_ref,
    gathered,
    key_w,
    value_w,
    gate_ref,
    gate_own,
    extra_ref,
    query_ref,
    new_key_ref,
    new_value_ref,
    gain_ref,
    key_acc,
    value_acc,
    gate_acc,
    key_out,
    key_in,
    value_out,
    value_in,
    side_out,
    side_in,
    state_out,
    row_out,
    row_in,
    load_sem,
    weight_sem,
    gather_recv,
    gather_send,
    swap_recv,
    swap_send,
    last_recv,
    last_send,
    above_sem,
    peers_sem,
):
    sequences, positions, depth = tokens_ref.shape
    local_heads = extra_ref.shape[1]
    key_width = key_acc.shape[1] // local_heads
    value_width = value_acc.shape[1] // local_heads
    share = value_width // sp_size
    all_heads = gate_ref.shape[0] // 2
    chips = tp_size // CORES
    me = lax.axis_index("sp")
    spot = lax.axis_index("tp")
    chip = spot // CORES
    core = spot % CORES
    partner = chip * CORES + (1 - core)
    half = positions // 2
    units = [(s, part * half, half) for s in range(sequences) for part in range(2)]
    last_unit = len(units) - 1
    batches = [(0, 0, positions, (0, 1)), (1, 0, half, (2,)), (1, half, half, (3,))]
    others = [sp_size - 1 - me, me + 1 - 2 * (me % 2), (me + 2) % sp_size]

    loads = [
        pltpu.make_async_copy(
            tokens_ref.at[s],
            gathered.at[spot, pl.ds(s * positions, positions)],
            load_sem.at[s],
        )
        for s in range(sequences)
    ]
    for load in loads:
        load.start()

    barrier = pltpu.get_barrier_semaphore()
    pl.semaphore_signal(barrier, inc=1, device_id={"tp": partner}, device_id_type=MESH)

    @pl.when(chip < chips - 1)
    def _():
        pl.semaphore_signal(barrier, inc=1, device_id={"tp": spot + CORES}, device_id_type=MESH)

    for other in range(1, sp_size):

        @pl.when(me < other)
        def _(other=other):
            pl.semaphore_signal(barrier, inc=1, device_id={"sp": other}, device_id_type=MESH)

    weights = [
        pltpu.make_async_copy(key_ref, key_w, weight_sem.at[0]),
        pltpu.make_async_copy(value_ref, value_w, weight_sem.at[1]),
        pltpu.make_async_copy(gate_hbm, gate_ref, weight_sem.at[2]),
        pltpu.make_async_copy(extra_hbm, extra_ref, weight_sem.at[3]),
        pltpu.make_async_copy(query_hbm, query_ref, weight_sem.at[4]),
        pltpu.make_async_copy(new_key_hbm, new_key_ref, weight_sem.at[5]),
        pltpu.make_async_copy(new_value_hbm, new_value_ref, weight_sem.at[6]),
        pltpu.make_async_copy(gain_hbm, gain_ref, weight_sem.at[7]),
        pltpu.make_async_copy(rate_hbm, rate_ref, weight_sem.at[8]),
        pltpu.make_async_copy(next_strength_hbm, next_strength_ref, weight_sem.at[9]),
    ]
    for weight in weights:
        weight.start()
    pl.semaphore_wait(barrier, jnp.where(chip > 0, 1, 0) + 1 + me)

    @pl.when(chip > 0)
    def _():
        pl.semaphore_signal(above_sem, inc=1, device_id={"tp": spot - CORES}, device_id_type=MESH)

    for other in range(sp_size - 1):

        @pl.when(other < me)
        def _(other=other):
            pl.semaphore_signal(peers_sem, inc=1, device_id={"sp": other}, device_id_type=MESH)

    def crossing(block, send, recv, axis, target):
        return pltpu.make_async_remote_copy(
            src_ref=block[0],
            dst_ref=block[1],
            send_sem=send,
            recv_sem=recv,
            device_id={axis: target},
            device_id_type=MESH,
        )

    def piece(origin, u, way, target, own=False):
        s, low, count = units[u]
        block = gathered.at[origin, pl.ds(s * positions + low, count)]
        kind = 2 * way + (u == last_unit) + (way == 2 and u == last_unit and own)
        return crossing(
            (block, block), gather_send.at[kind], gather_recv.at[origin, u], "tp", target
        )

    def settle(kind, blocks, count):
        block = gathered.at[pl.ds(0, blocks), pl.ds(0, count)]
        crossing(
            (block, block), gather_send.at[kind], gather_recv.at[0, 0], "tp", partner
        ).wait_send()

    for load in loads:
        load.wait()

    def hub(a_chip):
        return jnp.where((a_chip == 0) | (a_chip == chips - 1), 0, 1)

    for u in range(last_unit):

        @pl.when(chip > 0)
        def _(u=u):
            piece(spot, u, 1, spot - CORES).start()

    for u in [last_unit, *range(last_unit)]:
        piece(spot, u, 2, partner, own=True).start()

    @pl.when(chip < chips - 1)
    def _():
        pl.semaphore_wait(above_sem, 1)

    for u in range(last_unit):

        @pl.when(chip < chips - 1)
        def _(u=u):
            piece(spot, u, 0, spot + CORES).start()

    def send_last(way):
        onward = chip + (1 if way == 0 else -1)
        for c in range(CORES):
            piece(chip * CORES + c, last_unit, way, onward * CORES + hub(onward)).start()

    @pl.when(core == 1)
    def _():
        piece(partner, last_unit, 2, partner).wait_recv()

        @pl.when(chip == chips - 1)
        def _():
            send_last(1)

        @pl.when(chip == 0)
        def _():
            send_last(0)

    key_acc[...] = jnp.zeros_like(key_acc)
    value_acc[...] = jnp.zeros_like(value_acc)
    gate_acc[...] = jnp.zeros_like(gate_acc)
    side_out[...] = jnp.zeros_like(side_out)

    def add_in(rows, span, batch, keys=True, values=True):
        s, low, count, parts = batches[batch]
        cut = slice(s * positions + low, s * positions + low + count)
        if values:
            value_acc[cut] += jnp.dot(rows, value_w[span, :], preferred_element_type=jnp.float32)
        if not keys:
            return
        key_acc[cut] += jnp.dot(rows, key_w[span, :], preferred_element_type=jnp.float32)
        gates = lax.dot_general(
            gate_own[:, span],
            rows,
            (((1,), (1,)), ((), ())),
            preferred_element_type=jnp.float32,
        )
        gate_acc[s, :, low : low + count] += gates

    def take_one(block, batch, **kinds):
        s, low, count, _ = batches[batch]
        span = pl.ds(pl.multiple_of(block * depth, depth), depth)
        add_in(gathered[block, s * positions + low : s * positions + low + count], span, batch, **kinds)

    def take_chip(origin_chip, batch):
        s, low, count, _ = batches[batch]
        width = CORES * depth
        span = pl.ds(pl.multiple_of(origin_chip * width, width), width)
        rows = jnp.concatenate(
            [
                gathered[
                    origin_chip * CORES + c, s * positions + low : s * positions + low + count
                ]
                for c in range(CORES)
            ],
            axis=1,
        )
        add_in(rows, span, batch)

    first = spot * local_heads

    def prepare():
        for weight in weights:
            weight.wait()
        chooser = grid_mask(
            2 * local_heads,
            2 * all_heads,
            lambda r, c: c
            == jnp.where(r < local_heads, first + r, all_heads + first + r - local_heads),
        ).astype(jnp.float32)
        gate_own[...] = short_dot(chooser, gate_ref[...]).astype(jnp.bfloat16)
        placer = grid_mask(share, value_width, lambda r, c: c == me * share + r)
        for s in range(sequences):
            new_value = short_dot(new_value_ref[s], placer.astype(jnp.float32))
            for h in range(local_heads):
                side_out[h, s, 0, 2:3, :] = new_value[h : h + 1, :]

    def own(batch):
        for u in batches[batch][3]:
            if u == last_unit:

                @pl.when(core == 0)
                def _(u=u):
                    piece(partner, u, 2, partner).wait_recv()

            else:
                piece(partner, u, 2, partner).wait_recv()
        take_chip(chip, batch)

    def relay(distance, u):
        lanes = range(CORES) if u == last_unit else [core]
        for lane in lanes:
            relay_lane(distance, u, lane)

    def relay_lane(distance, u, lane):
        for way, step in ((1, 1), (0, -1)):
            origin_chip = chip + step * distance
            origin = origin_chip * CORES + lane
            present = (origin_chip >= 0) & (origin_chip < chips)
            if u == last_unit:
                present = present & (core == hub(chip))
            onward = chip - step
            beyond = (onward >= 0) & (onward < chips)
            target = onward * CORES + (hub(onward) if u == last_unit else core)

            @pl.when(present)
            def _(way=way, origin_chip=origin_chip, origin=origin, target=target, beyond=beyond):
                piece(origin, u, way, partner).wait_recv()

                @pl.when(beyond)
                def _():
                    piece(origin, u, way, target).start()

                piece(origin, u, 2, partner).start()
                if u == 1:

                    @pl.when(
                        beyond & (core == 1) & (origin_chip == (0 if way == 0 else chips - 1))
                    )
                    def _():
                        send_last(way)

    def both_sides(distance, act):
        def one_side(side, carry):
            origin_chip = chip + (2 * side - 1) * distance

            @pl.when((origin_chip >= 0) & (origin_chip < chips))
            def _():
                act(origin_chip)

            return carry

        lax.fori_loop(0, 2, one_side, 0)

    def absorb(distance, batch):
        def act(origin_chip):
            for u in batches[batch][3]:
                if u == last_unit:

                    @pl.when(core != hub(chip))
                    def _(u=u):
                        for c in range(CORES):
                            piece(origin_chip * CORES + c, u, 2, partner).wait_recv()

                else:
                    piece(origin_chip * CORES + 1 - core, u, 2, partner).wait_recv()
            take_chip(origin_chip, batch)

        both_sides(distance, act)

    def absorb_last_lane(distance, lane):
        relay_lane(distance, last_unit, lane)

        def act(origin_chip):
            block = origin_chip * CORES + lane

            @pl.when(core != hub(chip))
            def _():
                piece(block, last_unit, 2, partner).wait_recv()

            take_one(block, len(batches) - 1, values=lane < CORES - 1)

        both_sides(distance, act)

    def absorb_last_values(distance):
        def act(origin_chip):
            take_one(origin_chip * CORES + CORES - 1, len(batches) - 1, keys=False)

        both_sides(distance, act)

    def swap(n, slot, target):
        s, low, count, _ = batches[slot]
        if n == 0:
            block = (
                (side_out.at[target, s], side_in.at[me, s])
                if slot == 0
                else (side_out.at[target, s, slot - 1], side_in.at[me, s, slot - 1])
            )
        else:
            source, sink = ((key_out, key_in), (value_out, value_in))[n - 1]
            block = source.at[target, s, pl.ds(low, count)], sink.at[me, s, pl.ds(low, count)]
        return crossing(block, swap_send.at[n], swap_recv.at[n, s], "sp", target)

    def swapped(n, s):
        if n == 0:
            block = side_in.at[pl.ds(0, sp_size - 1), s]
        else:
            block = (key_in, value_in)[n - 1].at[pl.ds(0, sp_size - 1), s]
        crossing((block, block), swap_send.at[n], swap_recv.at[n, s], "sp", others[0]).wait_recv()

    def hand_out(slot, before_values=None):
        s, low, count, _ = batches[slot]
        cut = slice(s * positions + low, s * positions + low + count)
        part = max(slot - 1, 0)
        gates = gate_acc[s, :, low : low + count]
        extra = extra_ref[s, :, low : low + count]
        for h in range(local_heads):
            side_out[h, s, part, 0:1, low : low + count] = (
                -rate_ref[h] * softplus(gates[h : h + 1]) + extra[h : h + 1, :]
            )
            side_out[h, s, part, 1:2, low : low + count] = jax.nn.sigmoid(
                gates[local_heads + h : local_heads + h + 1] - strength_offset
            )
        for other in others:
            swap(0, slot, other).start()
        for h in range(local_heads):
            key_out[h, s, low : low + count] = key_acc[
                cut, h * key_width : (h + 1) * key_width
            ].astype(jnp.bfloat16)
        for other in others:
            swap(1, slot, other).start()
        if before_values is not None:
            before_values()
        for h in range(local_heads):
            value_out[h, s, low : low + count] = value_acc[
                cut, h * value_width : (h + 1) * value_width
            ].astype(jnp.bfloat16)
        for other in others:
            swap(2, slot, other).start()
        if slot == 0:
            side_in[me, s] = side_out[me, s]
        else:
            side_in[me, s, part] = side_out[me, s, part]
        key_in[me, s, low : low + count] = key_out[me, s, low : low + count]
        value_in[me, s, low : low + count] = value_out[me, s, low : low + count]

    far = chips - 1
    last_batch = len(batches) - 1
    steps = {1: [(1, 0), (1, 1), (1, 2)]} if far > 1 else {}
    for distance in range(2, far):
        steps[distance] = [(distance, 0), (distance, 1), (distance, 2)]
    work = [(own, (0,)), (own, (1,)), (own, (2,))]
    prepared = False
    for distance in range(1, far):
        for event in steps[distance]:
            relay(*event)
            if not prepared:
                prepare()
                prepared = True
            if work:
                act, operands = work.pop(0)
                act(*operands)
            if event[1] == 1:
                work.insert(0, (absorb, (distance, 0)))
            if event[1] == 2:
                work.append((absorb, (distance, 1)))
    if not prepared:
        prepare()
    for act, operands in [w for w in work if w[0] is own]:
        act(*operands)
    work = [w for w in work if w[0] is absorb]
    relay(far, 0)
    for act, operands in [w for w in work if w[1][1] == 0]:
        act(*operands)
    work = [w for w in work if w[1][1] != 0]
    relay(far, 1)
    absorb(far, 0)

    @pl.when(me < sp_size - 1)
    def _():
        pl.semaphore_wait(peers_sem, sp_size - 1 - me)

    hand_out(0)
    if far > 1:
        relay(1, last_unit)
    for act, operands in work:
        act(*operands)
    relay(far, 2)
    if far > 1:
        absorb(1, last_batch)
    absorb(far, 1)
    hand_out(1)
    pending = None
    for distance in range(2, far):
        relay(distance, last_unit)
        if pending is not None:
            absorb(*pending)
        pending = (distance, last_batch)
    if pending is not None:
        absorb(*pending)
    for lane in range(CORES):
        absorb_last_lane(far, lane)
    hand_out(2, lambda: absorb_last_values(far))

    side_rows = side_in.shape[3]
    upto = grid_mask(positions, positions, lambda r, c: r <= c).astype(jnp.float32)
    down = grid_mask(positions, positions, lambda r, c: c <= r).astype(jnp.float32)
    lanes = pl.ds(pl.multiple_of(me * key_width, key_width), key_width)
    queries = query_ref[:, lanes].astype(jnp.float32)
    new_keys = new_key_ref[:, lanes].astype(jnp.float32)
    new_keys = new_keys * lax.rsqrt(jnp.sum(new_keys * new_keys, axis=-1, keepdims=True) + 1e-06)
    meets = jnp.sum(queries * new_keys, axis=-1, keepdims=True)
    weight_of_new = [next_strength_ref[s, me] * meets[s : s + 1] for s in range(sequences)]
    probes = [queries[s : s + 1] - weight_of_new[s] * new_keys[s : s + 1] for s in range(sequences)]

    def block_maps(s):
        count = positions
        eye = grid_mask(count, count, lambda r, c: r == c).astype(jnp.float32)
        strict = grid_mask(count, count, lambda r, c: r > c)
        swapped(0, s)
        swapped(1, s)
        side = jnp.concatenate(
            [side_in[b, s, 0] + side_in[b, s, 1] for b in range(sp_size)], axis=0
        )
        new_value = sum(side[b * side_rows + 2 : b * side_rows + 3] for b in range(sp_size))
        terms = three_terms(side)
        rows = sum(short_dot(term, upto) for term in terms)
        columns = sum(short_dot(down, term, ((1,), (1,))) for term in terms)
        parts = []
        for b in range(sp_size):
            line = b * side_rows
            row = rows[line : line + 1, :]
            strength = side[line + 1 : line + 2, :]
            col = jnp.broadcast_to(columns[:, line : line + 1], (count, count))
            final_log = row[:, count - 1 : count]
            keys = key_in[b, s].astype(jnp.float32)
            keys = keys * lax.rsqrt(jnp.sum(keys * keys, axis=-1, keepdims=True) + 1e-06)
            within = jnp.exp(jnp.where(strict, col - row, 0.0)) * -strength
            power = jnp.where(strict, short_dot(keys, keys, ((1,), (1,))) * within, 0.0)
            erased = (keys * jnp.exp(col)).astype(jnp.bfloat16)
            carried = (keys.T * (jnp.exp(final_log - row) * strength)).astype(jnp.bfloat16)
            parts.append([eye + power, power, erased, carried, jnp.exp(final_log)])
        for part in parts:
            part[1] = short_dot(part[1], part[1])
        covered = 2
        while covered < count:
            for part in parts:
                if covered * 2 < count:
                    both = short_dot(part[1], jnp.concatenate([part[0], part[1]], axis=1))
                    part[0] = part[0] + both[:, :count]
                    part[1] = both[:, count:]
                else:
                    part[0] = part[0] + short_dot(part[1], part[0])
            covered = covered * 2
        swapped(2, s)
        solved = []
        for b, part in enumerate(parts):
            sources = jnp.concatenate([part[2], value_in[b, s]], axis=1)
            solved.append(short_dot(part[0], sources))
        maps = []
        for part, both in zip(parts, solved):
            both = short_dot(part[3], both)
            maps.append((both[:, :key_width], both[:, key_width:], part[4]))
        return maps, new_value

    def final(n, s, target):
        block = (
            (state_out.at[target, s], state_ref.at[s, me]),
            (row_out.at[target, s], row_in.at[me, s]),
        )[n]
        return crossing(block, last_send.at[n], last_recv.at[n], "sp", target)

    def finish(s, maps, new_value):
        while len(maps) > 2:
            maps = [compose(maps[i + 1], maps[i]) for i in range(0, len(maps), 2)]
        (_, first_write, _), (late_map, late_write, late_keep) = maps
        state = compose_write(maps[1], first_write)
        probe = jnp.where(s == 0, probes[0], probes[1])
        probe = jnp.broadcast_to(probe, (8, key_width))
        new_weight = jnp.where(s == 0, weight_of_new[0], weight_of_new[1])
        passed = close_dot(probe, jnp.concatenate([late_write, late_map], axis=1))
        onto_first = late_keep * probe - passed[:, value_width:]
        raw = close_dot(onto_first, first_write) + passed[:, :value_width]
        turned = state.T.astype(jnp.bfloat16)
        for j in range(sp_size):
            state_out[j, s] = turned[j * share : (j + 1) * share, :]
        for other in others:
            final(0, s, other).start()
        raw = raw[0:1] + new_weight * new_value
        raw = raw * lax.rsqrt(jnp.sum(raw * raw, axis=-1, keepdims=True) / value_width + 1e-06)
        for j in range(sp_size):
            turn = j * share
            row_out[j, s, 0:1, :] = (
                jnp.concatenate([raw[:, turn:], raw[:, :turn]], axis=1) if j else raw
            )
        for other in others:
            final(1, s, other).start()
        state_ref[s, me] = state_out[me, s]
        row_in[me, s] = row_out[me, s]

    row_out[...] = jnp.zeros_like(row_out)

    def solve(s, carry):
        finish(s, *block_maps(s))
        return carry

    lax.fori_loop(0, sequences, solve, 0)

    whole, part = last_unit * half, half
    settle(4, chips, whole)
    settle(6, 1, part)

    @pl.when(core == hub(chip))
    def _():
        settle(5, CORES * far, part)

    for c in range(chips):
        for way, sent in ((0, c + 1), (1, chips - c)):
            if sent < chips:

                @pl.when(chip == c)
                def _(way=way, sent=sent):
                    settle(2 * way, sent, whole)

                @pl.when((chip == c) & (core == 1))
                def _(way=way, sent=sent):
                    settle(2 * way + 1, CORES * sent, part)

    peers = pl.ds(0, sp_size - 1)
    for n, sent in enumerate((side_out, key_out, value_out)):
        block = sent.at[peers]
        crossing((block, block), swap_send.at[n], swap_recv.at[n, 0], "sp", others[0]).wait_send()
    for n, sent in enumerate((state_out, row_out)):
        block = sent.at[peers]
        crossing((block, block), last_send.at[n], last_recv.at[n], "sp", others[0]).wait_send()
    block = row_in.at[peers]
    crossing((block, block), last_send.at[1], last_recv.at[1], "sp", others[0]).wait_recv()
    for s in range(sequences):
        rows = jnp.concatenate([row_in[i, s, 0:1, :share] for i in range(sp_size)], axis=0)
        read_ref[s] = (rows * gain_ref[...].reshape(1, share)).astype(jnp.bfloat16)
    block = state_ref.at[:, peers]
    crossing((block, block), last_send.at[0], last_recv.at[0], "sp", others[0]).wait_recv()


def place_kernel(state_ref, read_ref, state_hbm, read_hbm, sem):
    copies = [
        pltpu.make_async_copy(state_ref, state_hbm, sem.at[0]),
        pltpu.make_async_copy(read_ref, read_hbm, sem.at[1]),
    ]
    for copy in copies:
        copy.start()
    for copy in copies:
        copy.wait()


def local_fused(
    tokens,
    key_matrix,
    value_matrix,
    gate_matrix,
    head_decay_rate,
    extra_log_decay,
    next_token_query,
    next_token_key,
    next_token_value,
    next_write_strength,
    read_norm_gain,
):
    sequences, positions, depth = tokens.shape
    local_heads = head_decay_rate.shape[0]
    sp_size = lax.axis_size("sp")
    tp_size = lax.axis_size("tp")
    key_total = key_matrix.shape[1]
    value_total = value_matrix.shape[1]
    key_width = key_total // local_heads
    value_width = value_total // local_heads
    share = value_width // sp_size
    rows = sequences * positions
    units = 2 * sequences
    vmem = pl.BlockSpec(memory_space=pltpu.VMEM)
    anywhere = pl.BlockSpec(memory_space=pl.ANY)
    dma = pltpu.SemaphoreType.DMA
    held = (sp_size, sequences, positions)
    turned, read = pl.pallas_call(
        functools.partial(fused_kernel, sp_size, tp_size),
        out_shape=(
            pltpu.VMEM((sequences, local_heads, share, key_width), jnp.bfloat16),
            pltpu.VMEM((sequences, local_heads, share), jnp.bfloat16),
        ),
        in_specs=[anywhere] * 11,
        out_specs=(vmem, vmem),
        scratch_shapes=[
            pltpu.SMEM(head_decay_rate.shape, jnp.float32),
            pltpu.SMEM(next_write_strength.shape, jnp.float32),
            pltpu.VMEM((tp_size, rows, depth), jnp.bfloat16),
            pltpu.VMEM(key_matrix.shape, jnp.bfloat16),
            pltpu.VMEM(value_matrix.shape, jnp.bfloat16),
            pltpu.VMEM(gate_matrix.shape[::-1], jnp.bfloat16),
            pltpu.VMEM((2 * local_heads, gate_matrix.shape[0]), jnp.bfloat16),
            pltpu.VMEM(extra_log_decay.shape, jnp.float32),
            pltpu.VMEM(next_token_query.shape, jnp.bfloat16),
            pltpu.VMEM(next_token_key.shape, jnp.bfloat16),
            pltpu.VMEM(next_token_value.shape, jnp.bfloat16),
            pltpu.VMEM(read_norm_gain.shape, jnp.float32),
            pltpu.VMEM((rows, key_total), jnp.float32),
            pltpu.VMEM((rows, value_total), jnp.float32),
            pltpu.VMEM((sequences, 2 * local_heads, positions), jnp.float32),
            pltpu.VMEM((*held, key_width), jnp.bfloat16),
            pltpu.VMEM((*held, key_width), jnp.bfloat16),
            pltpu.VMEM((*held, value_width), jnp.bfloat16),
            pltpu.VMEM((*held, value_width), jnp.bfloat16),
            pltpu.VMEM((sp_size, sequences, 2, 8, positions), jnp.float32),
            pltpu.VMEM((sp_size, sequences, 2, 8, positions), jnp.float32),
            pltpu.VMEM((sp_size, sequences, share, key_width), jnp.bfloat16),
            pltpu.VMEM((sp_size, sequences, 8, value_width), jnp.float32),
            pltpu.VMEM((sp_size, sequences, 8, value_width), jnp.float32),
            dma((sequences,)),
            dma((10,)),
            dma((tp_size, units)),
            dma((7,)),
            dma((3, sequences)),
            dma((3,)),
            dma((2,)),
            dma((2,)),
            pltpu.SemaphoreType.REGULAR,
            pltpu.SemaphoreType.REGULAR,
        ],
        compiler_params=pltpu.CompilerParams(
            collective_id=0, has_side_effects=True
        ),
    )(
        head_decay_rate,
        next_write_strength,
        tokens,
        key_matrix,
        value_matrix,
        gate_matrix.T,
        extra_log_decay,
        next_token_query,
        next_token_key,
        next_token_value,
        read_norm_gain,
    )
    turned, read = pl.pallas_call(
        place_kernel,
        out_shape=tuple(jax.ShapeDtypeStruct(a.shape, a.dtype) for a in (turned, read)),
        in_specs=[vmem, vmem],
        out_specs=(anywhere, anywhere),
        scratch_shapes=[dma((2,))],
    )(*(pltpu.with_memory_space_constraint(a, pltpu.VMEM) for a in (turned, read)))
    return jnp.swapaxes(turned, 2, 3), read


def local(*arguments):
    tokens, key_matrix, value_matrix = arguments[:3]
    sequences, positions, _ = tokens.shape
    local_heads = arguments[4].shape[0]
    sp_size = lax.axis_size("sp")
    fits = (
        local_heads == sp_size
        and sp_size == 4
        and sequences == 2
        and 2 * local_heads == 8
        and lax.axis_size("tp") % CORES == 0
        and lax.axis_size("tp") > CORES
        and positions == key_matrix.shape[1] // local_heads
        and positions == value_matrix.shape[1] // local_heads
        and positions % 128 == 0
    )
    return local_fused(*arguments) if fits else local_general(*arguments)


def solution(mesh):
    in_specs = (
        P(None, "sp", "tp"),
        P(None, "tp"),
        P(None, "tp"),
        P(),
        P("tp"),
        P(None, "tp", "sp"),
        P(None, "tp"),
        P(None, "tp"),
        P(None, "tp", "sp"),
        P(None, "tp"),
        P("sp"),
    )
    out_specs = (P(None, "tp", None, "sp"), P(None, "tp", "sp"))
    return jax.shard_map(local, mesh=mesh, in_specs=in_specs, out_specs=out_specs, check_vma=False)
```
